128 devices in a mesh: sp: 16 (over z, y), tp: 8 (over x, core).
Axes of the slice: x: 4, y: 4, z: 4, core: 2. Of those that a mesh axis runs over, the one named last changes fastest.
Arguments:
- queries: bfloat16 [16384, 1024], P('sp', 'tp'), may hold values from -6 to 6
- keys: bfloat16 [16384, 1024], P('sp', 'tp'), may hold values from -6 to 6
- values: bfloat16 [16384, 1024], P('sp', 'tp'), may hold values from -6 to 6
- cum_gates: float32 [16384, 16], P('sp', 'tp'), may hold values from -2050 to 0, as said below
- doc_ids: int32 [16384], P('sp'), may hold values from 0 to 1, never falling along the last dimension, each value on 1 to 12288 neighbouring positions
- residual: bfloat16 [16384, 2048], P('sp', 'tp'), may hold values from -100 to 100
- w_out: bfloat16 [1024, 2048], P('tp'), may hold values from -0.1875 to 0.1875
- norm_gain: bfloat16 [2048], P('tp'), may hold values from 0.099609375 to 1.8984375
- w_up: bfloat16 [2048, 8192], P('sp', 'tp'), may hold values from -0.125 to 0.125
- w_down: bfloat16 [8192, 2048], P('tp', 'sp'), may hold values from -0.0625 to 0.0625
Outputs:
- output: bfloat16 [16384, 2048], P('sp', 'tp')
The draws below stay inside these ranges and needn't reach their ends.
Inputs may be any that keep to these rules, and one draw needn't show every extreme that they name: `cum_gates`: along positions each head's values never rise. `doc_ids`: document numbers never fall along positions; a document holds 1 to three quarters of 16384 positions.
All inputs are finite; a program needn't handle non-finite values.
Results may differ from the reference program's by a relative error of at most 0.015.
Values may be sent and summed in bfloat16 or wider, within the bound.
A program may use at most 128 MiB of HBM per device.

```python
import math
import jax
import jax.numpy as jnp
import numpy as np
from jax import lax

D = 2048
HEAD_COUNT = 16
HD = 64
FF = 8192
TOK_DEV = 1024
TOKEN_COUNT = 16384
N_TP = 8


def draw_queries(key, part):
    shape_all = (TOKEN_COUNT, HEAD_COUNT * HD)
    drawn = jnp.clip(jax.random.normal(jax.random.fold_in(key, 11), shape_all, jnp.float32), -6.0, 6.0)
    return drawn.astype(jnp.bfloat16)


def draw_keys(key, part):
    shape_all = (TOKEN_COUNT, HEAD_COUNT * HD)
    drawn = jnp.clip(jax.random.normal(jax.random.fold_in(key, 13), shape_all, jnp.float32), -6.0, 6.0)
    return drawn.astype(jnp.bfloat16)


def draw_values(key, part):
    block_count = TOKEN_COUNT // TOK_DEV
    cols_all = HEAD_COUNT * HD
    block_means = jnp.clip(jax.random.normal(jax.random.fold_in(key, 21), (block_count, 1, cols_all), jnp.float32), -2.0, 2.0)
    draw_noise = jnp.clip(jax.random.normal(jax.random.fold_in(key, 23), (block_count, TOK_DEV, cols_all), jnp.float32), -4.6, 4.6)
    mean_weight = 0.7
    drawn = jnp.clip(draw_noise + mean_weight * block_means, -6.0, 6.0)
    return drawn.reshape(TOKEN_COUNT, cols_all).astype(jnp.bfloat16)


def draw_cum_gates(key, part):
    head_rank = jax.random.permutation(jax.random.fold_in(key, 31), HEAD_COUNT)
    fast_count = HEAD_COUNT // 2
    pos_factor = jax.random.uniform(jax.random.fold_in(key, 33), (TOKEN_COUNT, HEAD_COUNT), jnp.float32, 0.3, 1.7)
    fast_heads = head_rank < fast_count
    fast_rate = jnp.exp(jax.random.uniform(jax.random.fold_in(key, 34), (HEAD_COUNT,), jnp.float32, jnp.log(1.0 / 100.0), jnp.log(1.0 / 30.0)))
    slow_rate = jnp.exp(jax.random.uniform(jax.random.fold_in(key, 35), (HEAD_COUNT,), jnp.float32, jnp.log(0.1), jnp.log(0.4))) / TOKEN_COUNT
    head_rate = jnp.where(fast_heads, fast_rate, slow_rate)
    block_factor = jnp.exp(jax.random.uniform(jax.random.fold_in(key, 36), (TOKEN_COUNT // TOK_DEV,), jnp.float32, jnp.log(0.5), jnp.log(2.0)))
    block_factor = jnp.repeat(block_factor, TOK_DEV)
    gate_logarithm = -head_rate[None, :] * block_factor[:, None] * pos_factor
    spike_positions = jax.random.randint(jax.random.fold_in(key, 37), (2, HEAD_COUNT), 0, TOKEN_COUNT)
    spike_penalty = jnp.log(jax.random.uniform(jax.random.fold_in(key, 38), (2, HEAD_COUNT), jnp.float32, 0.5, 0.8))
    spike_matches = jnp.arange(TOKEN_COUNT, dtype=jnp.int32)[:, None, None] == spike_positions[None]
    gate_logarithm = gate_logarithm + jnp.sum(jnp.where(spike_matches, spike_penalty[None], 0.0), axis=1)
    return jnp.cumsum(gate_logarithm, axis=0).astype(jnp.float32)


def draw_residual(key, part):
    col_frac = jnp.arange(D, dtype=jnp.float32) / D
    col_low, col_span, row_low, row_high = (0.3, 10.0, 0.6, 1.6)
    jitter = jax.random.uniform(jax.random.fold_in(key, 41), (D,), jnp.float32, 0.7, 1.3)
    col_scale = col_low * col_span ** col_frac * jitter
    row_scale = jnp.exp(jax.random.uniform(jax.random.fold_in(key, 42), (TOKEN_COUNT, 1), jnp.float32, jnp.log(row_low), jnp.log(row_high)))
    drawn = jnp.clip(jax.random.normal(jax.random.fold_in(key, 43), (TOKEN_COUNT, D), jnp.float32), -6.0, 6.0)
    return (drawn * col_scale[None, :] * row_scale).astype(jnp.bfloat16)


def shard_levels(stream_key, dims, split, smallest, top_value):
    gain, own = 1.0, jax.random.fold_in(stream_key, 6)
    for position, shards_of in split:
        draws = jnp.exp(jax.random.uniform(jax.random.fold_in(own, position), (shards_of,), jnp.float32, smallest / len(split), top_value / len(split)))
        gain = gain * jnp.repeat(draws, dims[position] // shards_of).reshape([-1 if axis == position else 1 for axis in range(len(dims))])
    return gain


def profile(number_of, total, bound, slope):
    portions = [(1 << 20) // math.isqrt(standing ** slope) + 1 for standing in range(2, number_of + 1)]
    spare, holding = total - bound - (number_of - 1), [1] * (number_of - 1)
    while spare > 0:
        movable = [i for i in range(number_of - 1) if holding[i] < bound]
        whole, left = sum([portions[i] for i in movable]), spare
        for i in movable:
            addition = min(bound - holding[i], max(1, left * portions[i] // whole), spare)
            holding[i] = holding[i] + addition
            spare = spare - addition
    return np.array([bound] + holding)


def uneven(stream_key, count, total, bound, lean):
    if count == 2:
        one = jax.random.randint(stream_key, (), max(1, total - bound), min(bound, total - 1) + 1)
        return jnp.stack([one, total - one])
    tallies = jnp.asarray(profile(count, total, bound, lean), jnp.int32)
    pairs = (count - 1) // 2
    giver, receiver = tallies[1:1 + 2 * pairs:2], tallies[2:2 + 2 * pairs:2]
    slack = jnp.minimum(giver - 1, bound - receiver)
    passed = jax.random.randint(jax.random.fold_in(stream_key, 1), (pairs,), 0, 1 << 20) % (slack + 1)
    tallies = tallies.at[1:1 + 2 * pairs:2].set(giver - passed).at[2:2 + 2 * pairs:2].set(receiver + passed)
    return tallies[jax.random.permutation(jax.random.fold_in(stream_key, 2), count)]


def scatter_about(stream_key, extent, scale, bound, shards=(), kind=jnp.bfloat16):
    result = scale * jax.random.normal(stream_key, extent, jnp.float32)
    if shards:
        result = result * shard_levels(stream_key, extent, shards, -0.22, 0.18)
    return jnp.clip(result, -bound, bound).astype(kind)


def setup_inputs(seed: int = 0) -> dict:
    streams_of = jax.random.split(jax.random.key(seed), 11)
    queries = draw_queries(jax.random.fold_in(streams_of[10], 71), 0)
    keys = draw_keys(jax.random.fold_in(streams_of[10], 71), 0)
    values = draw_values(jax.random.fold_in(streams_of[10], 71), 0)
    cum_gates = draw_cum_gates(jax.random.fold_in(streams_of[10], 71), 0)
    doc_ids = jnp.searchsorted(jnp.cumsum(uneven(streams_of[4], 2, TOKEN_COUNT, TOKEN_COUNT * 3 // 4, 0)), jnp.arange(TOKEN_COUNT), side="right").astype(jnp.int32)
    residual = draw_residual(jax.random.fold_in(streams_of[10], 71), 0)
    w_out = scatter_about(streams_of[6], (HEAD_COUNT * HD, D), (HEAD_COUNT * HD) ** -0.5, 0.1875, ((0, 8),))
    norm_gain = jnp.clip(1.0 + 0.18 * jax.random.normal(streams_of[7], (D,), jnp.float32), 0.099609375, 1.8984375).astype(jnp.bfloat16)
    w_up = scatter_about(streams_of[8], (D, FF), D ** -0.5, 0.125, ((0, 16), (1, 8)))
    w_down = scatter_about(streams_of[9], (FF, D), FF ** -0.5, 0.0625, ((0, 8), (1, 16)))
    return dict(queries=queries, keys=keys, values=values, cum_gates=cum_gates, doc_ids=doc_ids, residual=residual, w_out=w_out, norm_gain=norm_gain, w_up=w_up, w_down=w_down)


eps = 1e-06

def rounded_back(value):
    return lax.optimization_barrier(value.astype(jnp.bfloat16)).astype(jnp.float32)

def reference(queries, keys, values, cum_gates, doc_ids, residual, w_out, norm_gain, w_up, w_down):
    seq_total = queries.shape[0]
    head_cols = queries.shape[1]
    head_count = head_cols // HD
    q_block = math.gcd(seq_total, 128)
    score_scale = HD ** (-0.5)
    keys_wide = keys.astype(jnp.float32).reshape(seq_total, head_count, HD)
    values_wide = values.astype(jnp.float32).reshape(seq_total, head_count, HD)
    gates_t = jnp.transpose(cum_gates)
    key_pos = jnp.arange(seq_total, dtype=jnp.int32)

    def attend_block(block_index):
        row_start = (block_index * q_block).astype(jnp.int32)
        q_rows = lax.dynamic_slice_in_dim(queries, row_start, q_block, 0).astype(jnp.float32)
        q_rows = q_rows.reshape(q_block, head_count, HD)
        gate_rows = lax.dynamic_slice_in_dim(gates_t, row_start, q_block, 1)
        doc_rows = lax.dynamic_slice_in_dim(doc_ids, row_start, q_block, 0)
        q_pos = row_start + jnp.arange(q_block, dtype=jnp.int32)
        scores = jnp.einsum('qhd,khd->hqk', q_rows, keys_wide) * score_scale
        scores = scores + gate_rows[:, :, None] - gates_t[:, None, :]
        visible = ((key_pos[None, :] <= q_pos[:, None]) & (doc_ids[None, :] == doc_rows[:, None]))[None]
        row_top = lax.optimization_barrier(jnp.max(jnp.where(visible, scores, -jnp.inf), axis=-1))
        weights = jnp.where(visible, jnp.exp(scores - row_top[..., None]), 0.0)
        weight_sum = lax.optimization_barrier(jnp.sum(weights, axis=-1))
        rounded = rounded_back(weights)
        summed = jnp.einsum('hqk,khd->qhd', rounded, values_wide)
        attended = summed / jnp.transpose(weight_sum)[:, :, None]
        return attended.reshape(q_block, head_cols).astype(jnp.bfloat16)
    attended = lax.map(attend_block, jnp.arange(seq_total // q_block, dtype=jnp.int32))
    attended = attended.reshape(seq_total, head_cols)
    group_cols = head_cols // N_TP
    head_mixed = jnp.zeros((seq_total, D), jnp.float32)
    for group_index in range(N_TP):
        low_col = group_index * group_cols
        partial_term = jnp.dot(attended[:, low_col:low_col + group_cols], w_out[low_col:low_col + group_cols], preferred_element_type=jnp.float32)
        head_mixed = head_mixed + rounded_back(partial_term)
    middle = (residual.astype(jnp.float32) + head_mixed).astype(jnp.bfloat16)
    middle_wide = lax.optimization_barrier(middle).astype(jnp.float32)
    mean_square = lax.optimization_barrier(jnp.mean(middle_wide * middle_wide, axis=-1, keepdims=True))
    normed = (middle_wide * lax.rsqrt(mean_square + eps) * norm_gain.astype(jnp.float32)).astype(jnp.bfloat16)
    up_proj = jnp.dot(normed, w_up, preferred_element_type=jnp.float32)
    hidden = jnp.square(jax.nn.relu(up_proj)).astype(jnp.bfloat16)
    unit_cols = FF // N_TP
    feed = jnp.zeros((seq_total, D), jnp.float32)
    for group_index in range(N_TP):
        low_unit = group_index * unit_cols
        partial_term = jnp.dot(hidden[:, low_unit:low_unit + unit_cols], w_down[low_unit:low_unit + unit_cols], preferred_element_type=jnp.float32)
        feed = feed + rounded_back(partial_term)
    return (middle_wide + feed).astype(jnp.bfloat16)
```

```python
import functools

import jax
import jax.numpy as jnp
from jax import lax
from jax.experimental import pallas as pl
from jax.experimental.pallas import tpu as pltpu
from jax.sharding import PartitionSpec as P

D = 2048
HD = 64
T = 1024
HALF = 512
ITEM = 576
eps = 1e-06
far_below = -1e30
BIG = 8192.0
MESH = pl.DeviceIdType.MESH
BF = jnp.bfloat16
F32 = jnp.float32
VM = pl.BlockSpec(memory_space=pltpu.VMEM)
HB = pl.BlockSpec(memory_space=pl.ANY)
DMA = pltpu.SemaphoreType.DMA


def sds(shape, dtype):
    return jax.ShapeDtypeStruct(shape, dtype)


def place():
    sp, tp = lax.axis_index("sp"), lax.axis_index("tp")
    return lax.div(sp, 4), lax.rem(sp, 4), lax.div(tp, 2), lax.rem(tp, 2)


def dev(z, y, x, c):
    return (z * 4 + y, x * 2 + c)


def send(src, dst, ssem, rsem, device):
    return pltpu.make_async_remote_copy(
        src_ref=src, dst_ref=dst, send_sem=ssem, recv_sem=rsem, device_id=device, device_id_type=MESH
    )


def up(v, k):
    return lax.rem(v + k, 4)


def pack_kernel(q_ref, k_ref, v_ref, g_ref, d_ref, qt_ref, kv_ref):
    qt = (q_ref[...].astype(F32) * (HD ** -0.5)).T.astype(BF)
    qt_ref[0] = qt[:HD]
    qt_ref[1] = qt[HD:]
    k_lo, k_hi = k_ref[:HALF].astype(F32), k_ref[HALF:].astype(F32)
    first = lax.broadcasted_iota(jnp.int32, (HALF, 128), 1) < HD
    kv_ref[0, 0, :HALF] = jnp.where(first, k_lo, pltpu.roll(k_hi, HD, 1)).astype(BF)
    kv_ref[0, 1, :HALF] = jnp.where(first, pltpu.roll(k_lo, HD, 1), k_hi).astype(BF)
    vt = v_ref[...].astype(F32).T.astype(BF)
    row = lax.broadcasted_iota(jnp.int32, (8, T), 0)
    doc0 = 1.0 - d_ref[...].astype(F32)
    for j in range(2):
        kv_ref[0, j, HALF:] = jnp.zeros((64, 128), BF)
        g = g_ref[j:j + 1, :]
        hi = g.astype(BF).astype(F32)
        mid = (g - hi).astype(BF).astype(F32)
        lo = (g - hi) - mid
        aux = jnp.where(row == 0, hi, jnp.where(row == 1, mid, jnp.where(row == 2, lo, jnp.where(row == 3, doc0, 0.0))))
        for n in range(8):
            kv_ref[1, j, n * 64:(n + 1) * 64] = vt[j * HD:(j + 1) * HD, n * 128:(n + 1) * 128]
        for n in range(4):
            two = jnp.concatenate([aux[:, (2 * n) * 128:(2 * n + 1) * 128], aux[:, (2 * n + 1) * 128:(2 * n + 2) * 128]], axis=0)
            kv_ref[1, j, HALF + n * 16:HALF + (n + 1) * 16] = two.astype(BF)


def pack(q, k, v, g, d):
    return pl.pallas_call(
        pack_kernel,
        out_shape=(sds((2, HD, T), BF), sds((2, 2, ITEM, 128), BF)),
        in_specs=[VM] * 5,
        out_specs=(VM, VM),
        name="pack",
    )(q, k, v, g, d)


def exchange_kernel(
    qt, kv, wo, res, gain, qin, kvall, woall, resin, gainall,
    qs, qr, ks, rr, s_sib, r_sib, s_r, s_l,
    wl, w_sib, wr_sib, w_s_r, w_s_l, w_r, es, er, gs, gr,
):
    z, y, x, c = place()
    sp, tp = z * 4 + y, x * 2 + c
    sib = dev(z, y, x, 1 - c)
    yp, ym, y2 = up(y, 1), up(y, 3), up(y, 2)
    xp, xm, x2 = up(x, 1), up(x, 3), up(x, 2)

    def guarded(is_self, local, remote):
        @pl.when(is_self)
        def _():
            local.start()

        @pl.when(jnp.logical_not(is_self))
        def _():
            remote.start()

    pending = []
    for j in range(2):
        zt = 2 * c + j
        for t in range(2):
            mine = (zt == z) & (c == t)
            src, dst = kv.at[t, j], kvall.at[t, sp]
            remote = send(src, dst, ks.at[2 * t + j], rr.at[sp], dev(zt, y, x, t))
            guarded(mine, pltpu.make_async_copy(src, dst, rr.at[sp]), remote)
            pending.append((mine, remote))
    for j in range(2):
        zt = 2 * c + j
        for hf in range(2):
            ct = lax.rem(hf + z, 2)
            mine = (zt == z) & (ct == c)
            src, dst = qt.at[j, :, pl.ds(hf * HALF, HALF)], qin.at[z]
            remote = send(src, dst, qs.at[2 * j + hf], qr.at[z], dev(zt, y, x, ct))
            guarded(mine, pltpu.make_async_copy(src, dst, qr.at[z]), remote)
            pending.append((mine, remote))

    done = []

    def wrows(xs, half):
        return pl.ds((2 * xs + c) * 128 + half * 64, 64)

    def go(copy):
        copy.start()
        done.append(copy)

    own_w = []
    for half in range(2):
        src, dst = wo.at[pl.ds(half * 64, 64)], woall.at[wrows(x, half)]
        n = 2 * x + half
        loc = pltpu.make_async_copy(src, dst, wl.at[half])
        loc.start()
        own_w.append(loc)
        go(send(src, dst, w_s_r.at[n], w_r.at[n], dev(z, y, xp, c)))
        go(send(src, dst, w_s_l.at[n], w_r.at[n], dev(z, y, xm, c)))
        go(send(src, dst, w_sib.at[n], wr_sib.at[n], sib))

    own_e = pltpu.make_async_copy(res.at[pl.ds(pl.multiple_of(tp * 128, 128), 128)],
                                  resin.at[:, pl.ds(pl.multiple_of(tp * 256, 256), 256)], er.at[tp])
    own_e.start()
    own_g = pltpu.make_async_copy(gain, gainall.at[:, pl.ds(pl.multiple_of(tp * 256, 256), 256)], gr.at[tp])
    own_g.start()
    for k in range(1, 8):
        to = lax.rem(tp + k, 8)
        cols = pl.ds(pl.multiple_of(tp * 256, 256), 256)
        go(send(res.at[pl.ds(pl.multiple_of(to * 128, 128), 128)], resin.at[:, cols], es.at[k], er.at[tp], (sp, to)))
        go(send(gain, gainall.at[:, cols], gs.at[k], gr.at[tp], (sp, to)))

    def arrived(b):
        send(kvall.at[c, b], kvall.at[c, b], s_sib.at[b], rr.at[b], sib).wait_recv()
        go(send(kvall.at[c, b], kvall.at[c, b], s_sib.at[b], r_sib.at[b], sib))

    def right(b):
        go(send(kvall.at[c, b], kvall.at[c, b], s_r.at[b], rr.at[b], dev(z, yp, x, c)))

    def left(b):
        go(send(kvall.at[c, b], kvall.at[c, b], s_l.at[b], rr.at[b], dev(z, ym, x, c)))

    zs = [z, up(z, 1), up(z, 3), up(z, 2)]

    def near(r):
        b = zs[r] * 4 + y
        arrived(b)
        right(b)
        left(b)

    def next_to(r):
        b = zs[r] * 4 + ym
        arrived(b)
        if r in (0, 2):
            right(b)
        b = zs[r] * 4 + yp
        arrived(b)
        if r in (1, 3):
            left(b)

    def w_arrived(xs, half):
        rows, n = wrows(xs, half), 2 * xs + half
        send(woall.at[rows], woall.at[rows], w_sib.at[n], w_r.at[n], sib).wait_recv()
        go(send(woall.at[rows], woall.at[rows], w_sib.at[n], wr_sib.at[n], sib))

    def w_next(half):
        w_arrived(xm, half)
        w_arrived(xp, half)
        if half == 0:
            rows, n = wrows(xm, 0), 2 * xm
            go(send(woall.at[rows], woall.at[rows], w_s_r.at[n], w_r.at[n], dev(z, y, xp, c)))
        else:
            rows, n = wrows(xp, 1), 2 * xp + 1
            go(send(woall.at[rows], woall.at[rows], w_s_l.at[n], w_r.at[n], dev(z, y, xm, c)))

    near(0)
    near(1)
    near(2)
    next_to(0)
    w_next(0)
    near(3)
    next_to(1)
    next_to(2)
    w_next(1)
    next_to(3)
    for r in range(4):
        arrived(zs[r] * 4 + y2)
    w_arrived(x2, 0)
    w_arrived(x2, 1)

    for b in range(16):
        send(kvall.at[1 - c, b], kvall.at[1 - c, b], s_sib.at[b], r_sib.at[b], sib).wait_recv()
    for n in range(8):
        rows = pl.ds((2 * (n // 2) + (1 - c)) * 128 + (n % 2) * 64, 64)
        send(woall.at[rows], woall.at[rows], w_sib.at[n], wr_sib.at[n], sib).wait_recv()
    for i in range(4):
        send(qin.at[i], qin.at[i], qs.at[0], qr.at[i], sib).wait_recv()
    for n in range(8):
        cols = pl.ds(n * 256, 256)
        send(resin.at[:, cols], resin.at[:, cols], es.at[0], er.at[n], sib).wait_recv()
        send(gainall.at[:, cols], gainall.at[:, cols], gs.at[0], gr.at[n], sib).wait_recv()
    for loc in own_w:
        loc.wait()
    for mine, remote in pending:
        @pl.when(jnp.logical_not(mine))
        def _():
            remote.wait_send()
    for copy in done:
        copy.wait_send()


def exchange(qt, kv, wo, res, gain):
    return pl.pallas_call(
        exchange_kernel,
        out_shape=(
            sds((4, HD, HALF), BF),
            sds((2, 16, ITEM, 128), BF),
            sds((1024, D), BF),
            sds((128, D), BF),
            sds((8, D), F32),
        ),
        in_specs=[VM] * 5,
        out_specs=(HB,) * 5,
        scratch_shapes=[
            DMA((4,)), DMA((4,)), DMA((4,)), DMA((16,)), DMA((16,)), DMA((16,)), DMA((16,)), DMA((16,)),
            DMA((2,)), DMA((8,)), DMA((8,)), DMA((8,)), DMA((8,)), DMA((8,)),
            DMA((8,)), DMA((8,)), DMA((8,)), DMA((8,)),
        ],
        compiler_params=pltpu.CompilerParams(has_side_effects=True),
        cost_estimate=pl.CostEstimate(flops=20_000_000_000, bytes_accessed=16_000_000, transcendentals=0),
        name="exchange",
    )(qt, kv, wo, res, gain)


def attend_kernel(q_ref, kv_ref, o_ref, pieces, gmat, w_ref, acc, top):
    z, y, x, c = place()
    ones = jnp.ones((16, HALF), BF)
    count = jnp.zeros((1, 128), F32)
    for b in range(16):
        for n in range(8):
            a = kv_ref[1, b, HALF + n * 8:HALF + (n + 1) * 8, :].astype(F32)
            count = count + a[3:4]
            hf, at = n // 4, (n % 4) * 128
            pieces[b * 8 + hf * 4:b * 8 + hf * 4 + 4, at:at + 128] = a[:4]
    docs0 = jnp.sum(count).astype(jnp.int32)
    gmat[...] = pieces[...].T.astype(BF)
    unit_of_row = lax.broadcasted_iota(jnp.int32, (128, HALF), 0) // 4
    piece_of_row = lax.broadcasted_iota(jnp.int32, (128, HALF), 0) % 4

    for i in range(4):
        hq = 2 * (4 * i + y) + lax.rem(c + i, 2)
        q = q_ref[i]
        none = jnp.zeros_like(q)
        q_pos = hq * HALF + lax.broadcasted_iota(jnp.int32, (1, HALF), 1)
        doc1 = jnp.where(q_pos >= docs0, -BIG, 0.0)
        w_ref[...] = jnp.where(piece_of_row == 3, doc1, -1.0)
        acc[...] = jnp.zeros_like(acc)
        top[...] = jnp.full_like(top, far_below)

        def unit(u, masked):
            b, hf = lax.div(u, 2), lax.rem(u, 2)
            lhs = jnp.concatenate([kv_ref[0, b, :HALF, :], gmat[...]], axis=1)
            sel = jnp.where(unit_of_row == u, w_ref[...], 0.0).astype(BF)
            first = hf == 0
            rhs = jnp.concatenate([jnp.where(first, q, none), jnp.where(first, none, q), sel], axis=0)
            s = jnp.dot(lhs, rhs, preferred_element_type=F32)
            if masked:
                key = lax.broadcasted_iota(jnp.int32, (HALF, HALF), 0)
                s = jnp.where(key <= lax.broadcasted_iota(jnp.int32, (HALF, HALF), 1), s, far_below)
            m_old = top[...]
            m_new = jnp.maximum(m_old, jnp.max(s, axis=0, keepdims=True))
            p = jnp.exp(s - m_new).astype(BF)
            shrink = jnp.exp(m_old - m_new)
            top[...] = m_new
            vt = jnp.concatenate(
                [kv_ref[1, b, pl.ds(pl.multiple_of(hf * 256 + n * 64, 64), 64), :] for n in range(4)], axis=1
            )
            vt = jnp.concatenate([vt, ones], axis=0)
            acc[...] = acc[...] * shrink + jnp.dot(vt, p, preferred_element_type=F32)

        start = jnp.where(hq * HALF >= docs0, lax.div(docs0, HALF), 0)

        def step(u, carry):
            unit(u, False)
            return carry

        lax.fori_loop(start, hq, step, 0)
        unit(hq, True)
        total = acc[...]
        o_ref[i] = (total[:HD] / total[HD:HD + 1]).astype(BF)


def attend(q, kv):
    return pl.pallas_call(
        attend_kernel,
        out_shape=sds((4, HD, HALF), BF),
        in_specs=[VM, VM],
        out_specs=VM,
        scratch_shapes=[
            pltpu.VMEM((128, HALF), F32),
            pltpu.VMEM((HALF, 128), BF),
            pltpu.VMEM((128, HALF), F32),
            pltpu.VMEM((80, HALF), F32),
            pltpu.VMEM((1, HALF), F32),
        ],
        compiler_params=pltpu.CompilerParams(vmem_limit_bytes=40 * 1024 * 1024),
        cost_estimate=pl.CostEstimate(flops=20_000_000_000, bytes_accessed=8_000_000, transcendentals=0),
        name="attend",
    )(q, kv)


def mix_kernel(
    att, wo_any, res, mid, a_in, wo, own, w_sem, a_s, a_r, o_l, m_sib, mr_sib, m_s_r, m_s_l, m_r
):
    z, y, x, c = place()
    sp, tp = z * 4 + y, x * 2 + c
    sib = dev(z, y, x, 1 - c)
    xp, xm, x2 = up(x, 1), up(x, 3), up(x, 2)
    head = 4 * x + z
    w_copy = pltpu.make_async_copy(wo_any, wo, w_sem.at[0])
    w_copy.start()
    pending = []
    for i in range(4):
        hf = lax.rem(c + i, 2)
        for k in range(4):
            to = 4 * hf + k
            mine = (z == i) & (to == tp)
            src = att.at[i, :, pl.ds(k * 128, 128)]
            dst = a_in.at[pl.ds(pl.multiple_of(head * HD, HD), HD)]
            local = pltpu.make_async_copy(src, dst, a_r.at[head])
            remote = send(src, dst, a_s.at[4 * i + k], a_r.at[head], (i * 4 + y, to))

            @pl.when(mine)
            def _():
                local.start()

            @pl.when(jnp.logical_not(mine))
            def _():
                remote.start()

            pending.append((mine, remote))
    for h in range(16):
        rows = pl.ds(h * HD, HD)
        send(a_in.at[rows], a_in.at[rows], a_s.at[0], a_r.at[h], sib).wait_recv()
    w_copy.wait()
    a = a_in[...].astype(F32).T.astype(BF)
    for n in range(4):
        cols = slice(n * 512, (n + 1) * 512)
        mixed = jnp.dot(a, wo[:, cols], preferred_element_type=F32)
        own[:, cols] = (res[:, cols].astype(F32) + mixed).astype(BF)

    done = []

    def go(copy):
        copy.start()
        done.append(copy)

    def rows_of(xs, cc, half):
        return pl.ds((2 * xs + cc) * 128 + half * 64, 64)

    locals_ = []
    for half in range(2):
        src, dst = own.at[pl.ds(half * 64, 64)], mid.at[rows_of(x, c, half)]
        n = 2 * x + half
        go(send(src, dst, m_s_r.at[n], m_r.at[n], dev(z, y, xp, c)))
        go(send(src, dst, m_s_l.at[n], m_r.at[n], dev(z, y, xm, c)))
        go(send(src, dst, m_sib.at[n], mr_sib.at[n], sib))
        loc = pltpu.make_async_copy(src, dst, o_l.at[half])
        loc.start()
        locals_.append(loc)

    def arrived(xs, half):
        rows, n = rows_of(xs, c, half), 2 * xs + half
        send(mid.at[rows], mid.at[rows], m_sib.at[n], m_r.at[n], sib).wait_recv()
        return rows, n

    def to_sib(rows, n):
        go(send(mid.at[rows], mid.at[rows], m_sib.at[n], mr_sib.at[n], sib))

    rows, n = arrived(xm, 0)
    go(send(mid.at[rows], mid.at[rows], m_s_r.at[n], m_r.at[n], dev(z, y, xp, c)))
    to_sib(rows, n)
    to_sib(*arrived(xp, 0))
    rows, n = arrived(xp, 1)
    go(send(mid.at[rows], mid.at[rows], m_s_l.at[n], m_r.at[n], dev(z, y, xm, c)))
    to_sib(rows, n)
    to_sib(*arrived(xm, 1))
    to_sib(*arrived(x2, 0))
    to_sib(*arrived(x2, 1))
    for n in range(8):
        rows = rows_of(n // 2, 1 - c, n % 2)
        send(mid.at[rows], mid.at[rows], m_sib.at[n], mr_sib.at[n], sib).wait_recv()
    for loc in locals_:
        loc.wait()
    for mine, remote in pending:
        @pl.when(jnp.logical_not(mine))
        def _():
            remote.wait_send()
    for copy in done:
        copy.wait_send()


def mix(att, wo, res):
    return pl.pallas_call(
        mix_kernel,
        out_shape=sds((T, D), BF),
        in_specs=[VM, HB, VM],
        out_specs=HB,
        scratch_shapes=[
            pltpu.VMEM((1024, 128), BF),
            pltpu.VMEM((1024, D), BF),
            pltpu.VMEM((128, D), BF),
            DMA((1,)), DMA((16,)), DMA((16,)), DMA((2,)),
            DMA((8,)), DMA((8,)), DMA((8,)), DMA((8,)), DMA((8,)),
        ],
        compiler_params=pltpu.CompilerParams(has_side_effects=True),
        cost_estimate=pl.CostEstimate(flops=20_000_000_000, bytes_accessed=8_000_000, transcendentals=0),
        name="mix",
    )(att, wo, res)


def scatter_kernel(
    part, mid, out, sibbuf, stage, hop_a, hop_b, from_l, from_r, res,
    mid_sem, s_sib, r_sib, s_hop, r_hop, s_out, r_l, r_r,
):
    z, y, x, c = place()
    tp = x * 2 + c
    sib = dev(z, y, x, 1 - c)
    right, left = dev(z, y, up(x, 1), c), dev(z, y, up(x, 3), c)
    m_copy = pltpu.make_async_copy(mid.at[:, pl.ds(pl.multiple_of(tp * 256, 256), 256)], res, mid_sem.at[0])
    m_copy.start()
    done = []

    def go(copy):
        copy.start()
        done.append(copy)

    for rel in (2, 1, 3, 0):
        xt = up(x, rel)
        cols = pl.ds(pl.multiple_of((2 * xt + 1 - c) * 256, 256), 256)
        go(send(part.at[:, cols], sibbuf.at[rel], s_sib.at[rel], r_sib.at[rel], sib))

    def chunks(lo, n, f):
        def one(k, carry):
            f(pl.ds(pl.multiple_of(lo + k * 128, 128), 128), pl.ds(pl.multiple_of(k * 128, 128), 128))
            return carry

        lax.fori_loop(0, n, one, 0)

    def pair(rel):
        send(sibbuf.at[rel], sibbuf.at[rel], s_sib.at[rel], r_sib.at[rel], sib).wait_recv()
        xt = up(x, rel)
        cols = pl.ds(pl.multiple_of((2 * xt + c) * 256, 256), 256)
        return lambda rows: part[rows, cols].astype(F32) + sibbuf[rel, rows, :].astype(F32)

    A, B = pl.ds(0, HALF), pl.ds(HALF, HALF)

    def put(rel, value):
        def f(rows, _):
            stage[rel, rows, :] = value(rows).astype(BF)

        return f

    two = pair(2)
    chunks(0, 8, put(2, two))
    go(send(stage.at[2, A], hop_a, s_hop.at[0], r_hop.at[0], right))
    go(send(stage.at[2, B], hop_b, s_hop.at[1], r_hop.at[1], left))
    one = pair(1)
    chunks(HALF, 4, put(1, one))
    go(send(stage.at[1, B], from_l.at[B], s_out.at[0], r_l.at[1], right))
    three = pair(3)
    chunks(0, 4, put(3, three))
    go(send(stage.at[3, A], from_r.at[A], s_out.at[1], r_r.at[0], left))

    send(hop_a, hop_a, s_hop.at[0], r_hop.at[0], sib).wait_recv()

    def fold_a(rows, rel):
        stage[1, rows, :] = (one(rows) + hop_a[rel, :].astype(F32)).astype(BF)

    chunks(0, 4, fold_a)
    go(send(stage.at[1, A], from_l.at[A], s_out.at[2], r_l.at[0], right))
    send(hop_b, hop_b, s_hop.at[1], r_hop.at[1], sib).wait_recv()

    def fold_b(rows, rel):
        stage[3, rows, :] = (three(rows) + hop_b[rel, :].astype(F32)).astype(BF)

    chunks(HALF, 4, fold_b)
    go(send(stage.at[3, B], from_r.at[B], s_out.at[3], r_r.at[1], left))
    mine = pair(0)
    m_copy.wait()
    send(from_l.at[B], from_l.at[B], s_out.at[0], r_l.at[1], sib).wait_recv()
    send(from_r.at[A], from_r.at[A], s_out.at[0], r_r.at[0], sib).wait_recv()
    send(from_l.at[A], from_l.at[A], s_out.at[0], r_l.at[0], sib).wait_recv()
    send(from_r.at[B], from_r.at[B], s_out.at[0], r_r.at[1], sib).wait_recv()

    def final(rows, _):
        feed = mine(rows) + from_l[rows, :].astype(F32) + from_r[rows, :].astype(F32)
        out[rows, :] = (res[rows, :].astype(F32) + feed).astype(BF)

    chunks(0, 8, final)
    for copy in done:
        copy.wait_send()


def scatter(part, mid):
    return pl.pallas_call(
        scatter_kernel,
        out_shape=sds((T, 256), BF),
        in_specs=[VM, HB],
        out_specs=VM,
        scratch_shapes=[
            pltpu.VMEM((4, T, 256), BF),
            pltpu.VMEM((4, T, 256), BF),
            pltpu.VMEM((HALF, 256), BF),
            pltpu.VMEM((HALF, 256), BF),
            pltpu.VMEM((T, 256), BF),
            pltpu.VMEM((T, 256), BF),
            pltpu.VMEM((T, 256), BF),
            DMA((1,)), DMA((4,)), DMA((4,)), DMA((2,)), DMA((2,)), DMA((4,)), DMA((2,)), DMA((2,)),
        ],
        compiler_params=pltpu.CompilerParams(has_side_effects=True),
        cost_estimate=pl.CostEstimate(flops=20_000_000_000, bytes_accessed=8_000_000, transcendentals=0),
        name="scatter",
    )(part, mid)


def body(queries, keys, values, cum_gates, doc_ids, residual, w_out, norm_gain, w_up, w_down):
    both = jnp.concatenate([w_up, jnp.transpose(w_down)], axis=1)
    whole = lax.all_gather(both, "sp", axis=0, tiled=True)
    up_w, down_t = whole[:, :1024], whole[:, 1024:]
    qt, kv = pack(queries, keys, values, jnp.transpose(cum_gates), doc_ids.reshape(1, T))
    gain8 = jnp.broadcast_to(norm_gain.astype(F32)[None], (8, 256))
    qin, kvall, woall, resin, gainall = exchange(qt, kv, w_out, residual, gain8)
    att = attend(qin, kvall)
    mid = mix(att, woall, resin)
    wide = mid.astype(F32)
    scaled = wide * lax.rsqrt(jnp.mean(wide * wide, axis=-1, keepdims=True) + eps)
    normed = (scaled * gainall[0:1]).astype(BF)
    up_proj = jnp.dot(normed, up_w, preferred_element_type=F32)
    hidden = jnp.square(jax.nn.relu(up_proj)).astype(BF)
    part = lax.dot_general(hidden, down_t, (((1,), (1,)), ((), ())), preferred_element_type=F32).astype(BF)
    return scatter(part, mid)


def solution(mesh):
    in_specs = (
        P("sp", "tp"),
        P("sp", "tp"),
        P("sp", "tp"),
        P("sp", "tp"),
        P("sp"),
        P("sp", "tp"),
        P("tp", None),
        P("tp"),
        P("sp", "tp"),
        P("tp", "sp"),
    )
    return jax.shard_map(body, mesh=mesh, in_specs=in_specs, out_specs=P("sp", "tp"), check_vma=False)
```

```python
import functools

import jax
import jax.numpy as jnp
from jax import lax
from jax.experimental import pallas as pl
from jax.experimental.pallas import tpu as pltpu
from jax.sharding import PartitionSpec as P

D = 2048
HD = 64
T = 1024
HALF = 512
ITEM = 576
eps = 1e-06
far_below = -1e30
BIG = 8192.0
MESH = pl.DeviceIdType.MESH
BF = jnp.bfloat16
F32 = jnp.float32
VM = pl.BlockSpec(memory_space=pltpu.VMEM)
HB = pl.BlockSpec(memory_space=pl.ANY)
DMA = pltpu.SemaphoreType.DMA


def sds(shape, dtype):
    return jax.ShapeDtypeStruct(shape, dtype)


def place():
    sp, tp = lax.axis_index("sp"), lax.axis_index("tp")
    return lax.div(sp, 4), lax.rem(sp, 4), lax.div(tp, 2), lax.rem(tp, 2)


def dev(z, y, x, c):
    return (z * 4 + y, x * 2 + c)


def send(src, dst, ssem, rsem, device):
    return pltpu.make_async_remote_copy(
        src_ref=src, dst_ref=dst, send_sem=ssem, recv_sem=rsem, device_id=device, device_id_type=MESH
    )


def up(v, k):
    return lax.rem(v + k, 4)


def signal(barrier, device):
    pl.semaphore_signal(barrier, inc=1, device_id=device, device_id_type=MESH)


def pack_kernel(q_ref, k_ref, v_ref, g_ref, d_ref, qt_ref, kv_ref):
    qt = (q_ref[...].astype(F32) * (HD ** -0.5)).T.astype(BF)
    qt_ref[0] = qt[:HD]
    qt_ref[1] = qt[HD:]
    k_lo, k_hi = k_ref[:HALF].astype(F32), k_ref[HALF:].astype(F32)
    first = lax.broadcasted_iota(jnp.int32, (HALF, 128), 1) < HD
    kv_ref[0, 0, :HALF] = jnp.where(first, k_lo, pltpu.roll(k_hi, HD, 1)).astype(BF)
    kv_ref[0, 1, :HALF] = jnp.where(first, pltpu.roll(k_lo, HD, 1), k_hi).astype(BF)
    vt = v_ref[...].astype(F32).T.astype(BF)
    row = lax.broadcasted_iota(jnp.int32, (8, T), 0)
    doc0 = 1.0 - d_ref[...].astype(F32)
    for j in range(2):
        kv_ref[0, j, HALF:] = jnp.zeros((64, 128), BF)
        g = g_ref[j:j + 1, :]
        hi = g.astype(BF).astype(F32)
        mid = (g - hi).astype(BF).astype(F32)
        lo = (g - hi) - mid
        aux = jnp.where(row == 0, hi, jnp.where(row == 1, mid, jnp.where(row == 2, lo, jnp.where(row == 3, doc0, 0.0))))
        for n in range(8):
            kv_ref[1, j, n * 64:(n + 1) * 64] = vt[j * HD:(j + 1) * HD, n * 128:(n + 1) * 128]
        for n in range(4):
            two = jnp.concatenate([aux[:, (2 * n) * 128:(2 * n + 1) * 128], aux[:, (2 * n + 1) * 128:(2 * n + 2) * 128]], axis=0)
            kv_ref[1, j, HALF + n * 16:HALF + (n + 1) * 16] = two.astype(BF)


def pack(q, k, v, g, d):
    return pl.pallas_call(
        pack_kernel,
        out_shape=(sds((2, HD, T), BF), sds((2, 2, ITEM, 128), BF)),
        in_specs=[VM] * 5,
        out_specs=(VM, VM),
        name="pack",
    )(q, k, v, g, d)


def exchange_kernel(
    qt, kv, wo, res, gain, qin, kvall, woall, resin, gainall,
    qs, qr, ks, rr, s_sib, r_sib, s_r, s_l,
    wl, w_sib, wr_sib, w_s_r, w_s_l, w_r, es, er, gs, gr,
):
    z, y, x, c = place()
    sp, tp = z * 4 + y, x * 2 + c
    sib = dev(z, y, x, 1 - c)
    yp, ym, y2 = up(y, 1), up(y, 3), up(y, 2)
    xp, xm, x2 = up(x, 1), up(x, 3), up(x, 2)

    barrier = pltpu.get_barrier_semaphore()
    cs = lax.div(z, 2)
    for zs in range(4):
        @pl.when(jnp.logical_not((z == zs) & (c == cs)))
        def _():
            signal(barrier, dev(zs, y, x, cs))

    for k in range(1, 8):
        signal(barrier, (sp, lax.rem(tp + k, 8)))
    signal(barrier, dev(z, yp, x, c))
    signal(barrier, dev(z, ym, x, c))
    pl.semaphore_wait(barrier, jnp.where(c == cs, 12, 13))

    def guarded(is_self, local, remote):
        @pl.when(is_self)
        def _():
            local.start()

        @pl.when(jnp.logical_not(is_self))
        def _():
            remote.start()

    pending = []
    for j in range(2):
        zt = 2 * c + j
        for t in range(2):
            mine = (zt == z) & (c == t)
            src, dst = kv.at[t, j], kvall.at[t, sp]
            remote = send(src, dst, ks.at[2 * t + j], rr.at[sp], dev(zt, y, x, t))
            guarded(mine, pltpu.make_async_copy(src, dst, rr.at[sp]), remote)
            pending.append((mine, remote))
    for j in range(2):
        zt = 2 * c + j
        for hf in range(2):
            ct = lax.rem(hf + z, 2)
            mine = (zt == z) & (ct == c)
            src, dst = qt.at[j, :, pl.ds(hf * HALF, HALF)], qin.at[z]
            remote = send(src, dst, qs.at[2 * j + hf], qr.at[z], dev(zt, y, x, ct))
            guarded(mine, pltpu.make_async_copy(src, dst, qr.at[z]), remote)
            pending.append((mine, remote))

    done = []

    def wrows(xs, half):
        return pl.ds((2 * xs + c) * 128 + half * 64, 64)

    def go(copy):
        copy.start()
        done.append(copy)

    own_w = []
    for half in range(2):
        src, dst = wo.at[pl.ds(half * 64, 64)], woall.at[wrows(x, half)]
        n = 2 * x + half
        loc = pltpu.make_async_copy(src, dst, wl.at[half])
        loc.start()
        own_w.append(loc)
        go(send(src, dst, w_s_r.at[n], w_r.at[n], dev(z, y, xp, c)))
        go(send(src, dst, w_s_l.at[n], w_r.at[n], dev(z, y, xm, c)))
        go(send(src, dst, w_sib.at[n], wr_sib.at[n], sib))

    own_e = pltpu.make_async_copy(res.at[pl.ds(pl.multiple_of(tp * 128, 128), 128)],
                                  resin.at[:, pl.ds(pl.multiple_of(tp * 256, 256), 256)], er.at[tp])
    own_e.start()
    own_g = pltpu.make_async_copy(gain, gainall.at[:, pl.ds(pl.multiple_of(tp * 256, 256), 256)], gr.at[tp])
    own_g.start()
    for k in range(1, 8):
        to = lax.rem(tp + k, 8)
        cols = pl.ds(pl.multiple_of(tp * 256, 256), 256)
        go(send(res.at[pl.ds(pl.multiple_of(to * 128, 128), 128)], resin.at[:, cols], es.at[k], er.at[tp], (sp, to)))
        go(send(gain, gainall.at[:, cols], gs.at[k], gr.at[tp], (sp, to)))

    def arrived(b):
        send(kvall.at[c, b], kvall.at[c, b], s_sib.at[b], rr.at[b], sib).wait_recv()
        go(send(kvall.at[c, b], kvall.at[c, b], s_sib.at[b], r_sib.at[b], sib))

    def right(b):
        go(send(kvall.at[c, b], kvall.at[c, b], s_r.at[b], rr.at[b], dev(z, yp, x, c)))

    def left(b):
        go(send(kvall.at[c, b], kvall.at[c, b], s_l.at[b], rr.at[b], dev(z, ym, x, c)))

    zs = [z, up(z, 1), up(z, 3), up(z, 2)]

    def near(r):
        b = zs[r] * 4 + y
        arrived(b)
        right(b)
        left(b)

    def next_to(r):
        b = zs[r] * 4 + ym
        arrived(b)
        if r in (0, 2):
            right(b)
        b = zs[r] * 4 + yp
        arrived(b)
        if r in (1, 3):
            left(b)

    def w_arrived(xs, half):
        rows, n = wrows(xs, half), 2 * xs + half
        send(woall.at[rows], woall.at[rows], w_sib.at[n], w_r.at[n], sib).wait_recv()
        go(send(woall.at[rows], woall.at[rows], w_sib.at[n], wr_sib.at[n], sib))

    def w_next(half):
        w_arrived(xm, half)
        w_arrived(xp, half)
        if half == 0:
            rows, n = wrows(xm, 0), 2 * xm
            go(send(woall.at[rows], woall.at[rows], w_s_r.at[n], w_r.at[n], dev(z, y, xp, c)))
        else:
            rows, n = wrows(xp, 1), 2 * xp + 1
            go(send(woall.at[rows], woall.at[rows], w_s_l.at[n], w_r.at[n], dev(z, y, xm, c)))

    near(0)
    near(1)
    near(2)
    next_to(0)
    w_next(0)
    near(3)
    next_to(1)
    next_to(2)
    w_next(1)
    next_to(3)
    for r in range(4):
        arrived(zs[r] * 4 + y2)
    w_arrived(x2, 0)
    w_arrived(x2, 1)

    for b in range(16):
        send(kvall.at[1 - c, b], kvall.at[1 - c, b], s_sib.at[b], r_sib.at[b], sib).wait_recv()
    for n in range(8):
        rows = pl.ds((2 * (n // 2) + (1 - c)) * 128 + (n % 2) * 64, 64)
        send(woall.at[rows], woall.at[rows], w_sib.at[n], wr_sib.at[n], sib).wait_recv()
    for i in range(4):
        send(qin.at[i], qin.at[i], qs.at[0], qr.at[i], sib).wait_recv()
    for n in range(8):
        cols = pl.ds(n * 256, 256)
        send(resin.at[:, cols], resin.at[:, cols], es.at[0], er.at[n], sib).wait_recv()
        send(gainall.at[:, cols], gainall.at[:, cols], gs.at[0], gr.at[n], sib).wait_recv()
    for loc in own_w:
        loc.wait()
    for mine, remote in pending:
        @pl.when(jnp.logical_not(mine))
        def _():
            remote.wait_send()
    for copy in done:
        copy.wait_send()


def exchange(qt, kv, wo, res, gain):
    return pl.pallas_call(
        exchange_kernel,
        out_shape=(
            sds((4, HD, HALF), BF),
            sds((2, 16, ITEM, 128), BF),
            sds((1024, D), BF),
            sds((128, D), BF),
            sds((8, D), F32),
        ),
        in_specs=[VM] * 5,
        out_specs=(HB,) * 5,
        scratch_shapes=[
            DMA((4,)), DMA((4,)), DMA((4,)), DMA((16,)), DMA((16,)), DMA((16,)), DMA((16,)), DMA((16,)),
            DMA((2,)), DMA((8,)), DMA((8,)), DMA((8,)), DMA((8,)), DMA((8,)),
            DMA((8,)), DMA((8,)), DMA((8,)), DMA((8,)),
        ],
        compiler_params=pltpu.CompilerParams(has_side_effects=True, collective_id=0),
        cost_estimate=pl.CostEstimate(flops=20_000_000_000, bytes_accessed=16_000_000, transcendentals=0),
        name="exchange",
    )(qt, kv, wo, res, gain)


def attend_kernel(q_ref, kv_ref, o_ref, pieces, gmat, w_ref, acc, top):
    z, y, x, c = place()
    ones = jnp.ones((16, HALF), BF)
    count = jnp.zeros((1, 128), F32)
    for b in range(16):
        for n in range(8):
            a = kv_ref[1, b, HALF + n * 8:HALF + (n + 1) * 8, :].astype(F32)
            count = count + a[3:4]
            hf, at = n // 4, (n % 4) * 128
            pieces[b * 8 + hf * 4:b * 8 + hf * 4 + 4, at:at + 128] = a[:4]
    docs0 = jnp.sum(count).astype(jnp.int32)
    gmat[...] = pieces[...].T.astype(BF)
    unit_of_row = lax.broadcasted_iota(jnp.int32, (128, HALF), 0) // 4
    piece_of_row = lax.broadcasted_iota(jnp.int32, (128, HALF), 0) % 4

    for i in range(4):
        hq = 2 * (4 * i + y) + lax.rem(c + i, 2)
        q = q_ref[i]
        none = jnp.zeros_like(q)
        q_pos = hq * HALF + lax.broadcasted_iota(jnp.int32, (1, HALF), 1)
        doc1 = jnp.where(q_pos >= docs0, -BIG, 0.0)
        w_ref[...] = jnp.where(piece_of_row == 3, doc1, -1.0)
        acc[...] = jnp.zeros_like(acc)
        top[...] = jnp.full_like(top, far_below)

        def unit(u, masked):
            b, hf = lax.div(u, 2), lax.rem(u, 2)
            lhs = jnp.concatenate([kv_ref[0, b, :HALF, :], gmat[...]], axis=1)
            sel = jnp.where(unit_of_row == u, w_ref[...], 0.0).astype(BF)
            first = hf == 0
            rhs = jnp.concatenate([jnp.where(first, q, none), jnp.where(first, none, q), sel], axis=0)
            s = jnp.dot(lhs, rhs, preferred_element_type=F32)
            if masked:
                key = lax.broadcasted_iota(jnp.int32, (HALF, HALF), 0)
                s = jnp.where(key <= lax.broadcasted_iota(jnp.int32, (HALF, HALF), 1), s, far_below)
            m_old = top[...]
            m_new = jnp.maximum(m_old, jnp.max(s, axis=0, keepdims=True))
            p = jnp.exp(s - m_new).astype(BF)
            shrink = jnp.exp(m_old - m_new)
            top[...] = m_new
            vt = jnp.concatenate(
                [kv_ref[1, b, pl.ds(pl.multiple_of(hf * 256 + n * 64, 64), 64), :] for n in range(4)], axis=1
            )
            vt = jnp.concatenate([vt, ones], axis=0)
            acc[...] = acc[...] * shrink + jnp.dot(vt, p, preferred_element_type=F32)

        start = jnp.where(hq * HALF >= docs0, lax.div(docs0, HALF), 0)

        def step(u, carry):
            unit(u, False)
            return carry

        lax.fori_loop(start, hq, step, 0)
        unit(hq, True)
        total = acc[...]
        o_ref[i] = (total[:HD] / total[HD:HD + 1]).astype(BF)


def attend(q, kv):
    return pl.pallas_call(
        attend_kernel,
        out_shape=sds((4, HD, HALF), BF),
        in_specs=[VM, VM],
        out_specs=VM,
        scratch_shapes=[
            pltpu.VMEM((128, HALF), F32),
            pltpu.VMEM((HALF, 128), BF),
            pltpu.VMEM((128, HALF), F32),
            pltpu.VMEM((80, HALF), F32),
            pltpu.VMEM((1, HALF), F32),
        ],
        compiler_params=pltpu.CompilerParams(vmem_limit_bytes=40 * 1024 * 1024),
        cost_estimate=pl.CostEstimate(flops=20_000_000_000, bytes_accessed=8_000_000, transcendentals=0),
        name="attend",
    )(q, kv)


def mix_kernel(
    att, wo_any, res, mid, a_in, wo, own, w_sem, a_s, a_r, o_l, m_sib, mr_sib, m_s_r, m_s_l, m_r
):
    z, y, x, c = place()
    sp, tp = z * 4 + y, x * 2 + c
    sib = dev(z, y, x, 1 - c)
    xp, xm, x2 = up(x, 1), up(x, 3), up(x, 2)
    head = 4 * x + z
    barrier = pltpu.get_barrier_semaphore()
    cs = lax.rem(lax.div(tp, 4) + z, 2)
    for zs in range(4):
        for xs in range(4):
            @pl.when(jnp.logical_not((z == zs) & (x == xs) & (c == cs)))
            def _():
                signal(barrier, dev(zs, y, xs, cs))

    for near in (sib, dev(z, y, xp, c), dev(z, y, xm, c)):
        signal(barrier, near)
    pl.semaphore_wait(barrier, jnp.where(lax.div(x, 2) == lax.rem(c + z, 2), 18, 19))
    w_copy = pltpu.make_async_copy(wo_any, wo, w_sem.at[0])
    w_copy.start()
    pending = []
    for i in range(4):
        hf = lax.rem(c + i, 2)
        for k in range(4):
            to = 4 * hf + k
            mine = (z == i) & (to == tp)
            src = att.at[i, :, pl.ds(k * 128, 128)]
            dst = a_in.at[pl.ds(pl.multiple_of(head * HD, HD), HD)]
            local = pltpu.make_async_copy(src, dst, a_r.at[head])
            remote = send(src, dst, a_s.at[4 * i + k], a_r.at[head], (i * 4 + y, to))

            @pl.when(mine)
            def _():
                local.start()

            @pl.when(jnp.logical_not(mine))
            def _():
                remote.start()

            pending.append((mine, remote))
    for h in range(16):
        rows = pl.ds(h * HD, HD)
        send(a_in.at[rows], a_in.at[rows], a_s.at[0], a_r.at[h], sib).wait_recv()
    w_copy.wait()
    a = a_in[...].astype(F32).T.astype(BF)
    for n in range(4):
        cols = slice(n * 512, (n + 1) * 512)
        mixed = jnp.dot(a, wo[:, cols], preferred_element_type=F32)
        own[:, cols] = (res[:, cols].astype(F32) + mixed).astype(BF)

    done = []

    def go(copy):
        copy.start()
        done.append(copy)

    def rows_of(xs, cc, half):
        return pl.ds((2 * xs + cc) * 128 + half * 64, 64)

    locals_ = []
    for half in range(2):
        src, dst = own.at[pl.ds(half * 64, 64)], mid.at[rows_of(x, c, half)]
        n = 2 * x + half
        go(send(src, dst, m_s_r.at[n], m_r.at[n], dev(z, y, xp, c)))
        go(send(src, dst, m_s_l.at[n], m_r.at[n], dev(z, y, xm, c)))
        go(send(src, dst, m_sib.at[n], mr_sib.at[n], sib))
        loc = pltpu.make_async_copy(src, dst, o_l.at[half])
        loc.start()
        locals_.append(loc)

    def arrived(xs, half):
        rows, n = rows_of(xs, c, half), 2 * xs + half
        send(mid.at[rows], mid.at[rows], m_sib.at[n], m_r.at[n], sib).wait_recv()
        return rows, n

    def to_sib(rows, n):
        go(send(mid.at[rows], mid.at[rows], m_sib.at[n], mr_sib.at[n], sib))

    rows, n = arrived(xm, 0)
    go(send(mid.at[rows], mid.at[rows], m_s_r.at[n], m_r.at[n], dev(z, y, xp, c)))
    to_sib(rows, n)
    to_sib(*arrived(xp, 0))
    rows, n = arrived(xp, 1)
    go(send(mid.at[rows], mid.at[rows], m_s_l.at[n], m_r.at[n], dev(z, y, xm, c)))
    to_sib(rows, n)
    to_sib(*arrived(xm, 1))
    to_sib(*arrived(x2, 0))
    to_sib(*arrived(x2, 1))
    for n in range(8):
        rows = rows_of(n // 2, 1 - c, n % 2)
        send(mid.at[rows], mid.at[rows], m_sib.at[n], mr_sib.at[n], sib).wait_recv()
    for loc in locals_:
        loc.wait()
    for mine, remote in pending:
        @pl.when(jnp.logical_not(mine))
        def _():
            remote.wait_send()
    for copy in done:
        copy.wait_send()


def mix(att, wo, res):
    return pl.pallas_call(
        mix_kernel,
        out_shape=sds((T, D), BF),
        in_specs=[VM, HB, VM],
        out_specs=HB,
        scratch_shapes=[
            pltpu.VMEM((1024, 128), BF),
            pltpu.VMEM((1024, D), BF),
            pltpu.VMEM((128, D), BF),
            DMA((1,)), DMA((16,)), DMA((16,)), DMA((2,)),
            DMA((8,)), DMA((8,)), DMA((8,)), DMA((8,)), DMA((8,)),
        ],
        compiler_params=pltpu.CompilerParams(has_side_effects=True, collective_id=1),
        cost_estimate=pl.CostEstimate(flops=20_000_000_000, bytes_accessed=8_000_000, transcendentals=0),
        name="mix",
    )(att, wo, res)


def scatter_kernel(
    part, mid, out, sibbuf, stage, hop_a, hop_b, from_l, from_r, res,
    mid_sem, s_sib, r_sib, s_hop, r_hop, s_out, r_l, r_r,
):
    z, y, x, c = place()
    tp = x * 2 + c
    sib = dev(z, y, x, 1 - c)
    right, left = dev(z, y, up(x, 1), c), dev(z, y, up(x, 3), c)
    barrier = pltpu.get_barrier_semaphore()
    for near in (sib, right, left):
        signal(barrier, near)
    pl.semaphore_wait(barrier, 3)
    m_copy = pltpu.make_async_copy(mid.at[:, pl.ds(pl.multiple_of(tp * 256, 256), 256)], res, mid_sem.at[0])
    m_copy.start()
    done = []

    def go(copy):
        copy.start()
        done.append(copy)

    for rel in (2, 1, 3, 0):
        xt = up(x, rel)
        cols = pl.ds(pl.multiple_of((2 * xt + 1 - c) * 256, 256), 256)
        go(send(part.at[:, cols], sibbuf.at[rel], s_sib.at[rel], r_sib.at[rel], sib))

    def chunks(lo, n, f):
        def one(k, carry):
            f(pl.ds(pl.multiple_of(lo + k * 128, 128), 128), pl.ds(pl.multiple_of(k * 128, 128), 128))
            return carry

        lax.fori_loop(0, n, one, 0)

    def pair(rel):
        send(sibbuf.at[rel], sibbuf.at[rel], s_sib.at[rel], r_sib.at[rel], sib).wait_recv()
        xt = up(x, rel)
        cols = pl.ds(pl.multiple_of((2 * xt + c) * 256, 256), 256)
        return lambda rows: part[rows, cols].astype(F32) + sibbuf[rel, rows, :].astype(F32)

    A, B = pl.ds(0, HALF), pl.ds(HALF, HALF)

    def put(rel, value):
        def f(rows, _):
            stage[rel, rows, :] = value(rows).astype(BF)

        return f

    two = pair(2)
    chunks(0, 8, put(2, two))
    go(send(stage.at[2, A], hop_a, s_hop.at[0], r_hop.at[0], right))
    go(send(stage.at[2, B], hop_b, s_hop.at[1], r_hop.at[1], left))
    one = pair(1)
    chunks(HALF, 4, put(1, one))
    go(send(stage.at[1, B], from_l.at[B], s_out.at[0], r_l.at[1], right))
    three = pair(3)
    chunks(0, 4, put(3, three))
    go(send(stage.at[3, A], from_r.at[A], s_out.at[1], r_r.at[0], left))

    send(hop_a, hop_a, s_hop.at[0], r_hop.at[0], sib).wait_recv()

    def fold_a(rows, rel):
        stage[1, rows, :] = (one(rows) + hop_a[rel, :].astype(F32)).astype(BF)

    chunks(0, 4, fold_a)
    go(send(stage.at[1, A], from_l.at[A], s_out.at[2], r_l.at[0], right))
    send(hop_b, hop_b, s_hop.at[1], r_hop.at[1], sib).wait_recv()

    def fold_b(rows, rel):
        stage[3, rows, :] = (three(rows) + hop_b[rel, :].astype(F32)).astype(BF)

    chunks(HALF, 4, fold_b)
    go(send(stage.at[3, B], from_r.at[B], s_out.at[3], r_r.at[1], left))
    mine = pair(0)
    m_copy.wait()
    send(from_l.at[B], from_l.at[B], s_out.at[0], r_l.at[1], sib).wait_recv()
    send(from_r.at[A], from_r.at[A], s_out.at[0], r_r.at[0], sib).wait_recv()
    send(from_l.at[A], from_l.at[A], s_out.at[0], r_l.at[0], sib).wait_recv()
    send(from_r.at[B], from_r.at[B], s_out.at[0], r_r.at[1], sib).wait_recv()

    def final(rows, _):
        feed = mine(rows) + from_l[rows, :].astype(F32) + from_r[rows, :].astype(F32)
        out[rows, :] = (res[rows, :].astype(F32) + feed).astype(BF)

    chunks(0, 8, final)
    for copy in done:
        copy.wait_send()


def scatter(part, mid):
    return pl.pallas_call(
        scatter_kernel,
        out_shape=sds((T, 256), BF),
        in_specs=[VM, HB],
        out_specs=VM,
        scratch_shapes=[
            pltpu.VMEM((4, T, 256), BF),
            pltpu.VMEM((4, T, 256), BF),
            pltpu.VMEM((HALF, 256), BF),
            pltpu.VMEM((HALF, 256), BF),
            pltpu.VMEM((T, 256), BF),
            pltpu.VMEM((T, 256), BF),
            pltpu.VMEM((T, 256), BF),
            DMA((1,)), DMA((4,)), DMA((4,)), DMA((2,)), DMA((2,)), DMA((4,)), DMA((2,)), DMA((2,)),
        ],
        compiler_params=pltpu.CompilerParams(has_side_effects=True, collective_id=2),
        cost_estimate=pl.CostEstimate(flops=20_000_000_000, bytes_accessed=8_000_000, transcendentals=0),
        name="scatter",
    )(part, mid)


def body(queries, keys, values, cum_gates, doc_ids, residual, w_out, norm_gain, w_up, w_down):
    both = jnp.concatenate([w_up, jnp.transpose(w_down)], axis=1)
    whole = lax.all_gather(both, "sp", axis=0, tiled=True)
    up_w, down_t = whole[:, :1024], whole[:, 1024:]
    qt, kv = pack(queries, keys, values, jnp.transpose(cum_gates), doc_ids.reshape(1, T))
    gain8 = jnp.broadcast_to(norm_gain.astype(F32)[None], (8, 256))
    qin, kvall, woall, resin, gainall = exchange(qt, kv, w_out, residual, gain8)
    att = attend(qin, kvall)
    mid = mix(att, woall, resin)
    wide = mid.astype(F32)
    scaled = wide * lax.rsqrt(jnp.mean(wide * wide, axis=-1, keepdims=True) + eps)
    normed = (scaled * gainall[0:1]).astype(BF)
    up_proj = jnp.dot(normed, up_w, preferred_element_type=F32)
    hidden = jnp.square(jax.nn.relu(up_proj)).astype(BF)
    part = lax.dot_general(hidden, down_t, (((1,), (1,)), ((), ())), preferred_element_type=F32).astype(BF)
    return scatter(part, mid)


def solution(mesh):
    in_specs = (
        P("sp", "tp"),
        P("sp", "tp"),
        P("sp", "tp"),
        P("sp", "tp"),
        P("sp"),
        P("sp", "tp"),
        P("tp", None),
        P("tp"),
        P("sp", "tp"),
        P("tp", "sp"),
    )
    return jax.shard_map(body, mesh=mesh, in_specs=in_specs, out_specs=P("sp", "tp"), check_vma=False)
```

```python
import functools

import jax
import jax.numpy as jnp
from jax import lax
from jax.experimental import pallas as pl
from jax.experimental.pallas import tpu as pltpu
from jax.sharding import PartitionSpec as P

D = 2048
HD = 64
T = 1024
HALF = 512
ITEM = 576
eps = 1e-06
far_below = -1e30
BIG = 8192.0
MESH = pl.DeviceIdType.MESH
BF = jnp.bfloat16
F32 = jnp.float32
VM = pl.BlockSpec(memory_space=pltpu.VMEM)
HB = pl.BlockSpec(memory_space=pl.ANY)
DMA = pltpu.SemaphoreType.DMA


def sds(shape, dtype):
    return jax.ShapeDtypeStruct(shape, dtype)


def place():
    sp, tp = lax.axis_index("sp"), lax.axis_index("tp")
    return lax.div(sp, 4), lax.rem(sp, 4), lax.div(tp, 2), lax.rem(tp, 2)


def dev(z, y, x, c):
    return (z * 4 + y, x * 2 + c)


def send(src, dst, ssem, rsem, device):
    return pltpu.make_async_remote_copy(
        src_ref=src, dst_ref=dst, send_sem=ssem, recv_sem=rsem, device_id=device, device_id_type=MESH
    )


def up(v, k):
    return lax.rem(v + k, 4)


def signal(barrier, device):
    pl.semaphore_signal(barrier, inc=1, device_id=device, device_id_type=MESH)


class Ring:
    def __init__(self, go, me, slot, right, left, s_r, s_l, r, sib=None, s_sib=None, r_sib=None):
        self.go, self.me, self.slot, self.right, self.left = go, me, slot, right, left
        self.s_r, self.s_l, self.r = s_r, s_l, r
        self.sib, self.s_sib, self.r_sib = sib, s_sib, r_sib

    def start(self, src, order=(0, 1)):
        for half in order:
            n, dst = 2 * self.me + half, self.slot(self.me, half)
            self.go(send(src(half), dst, self.s_r.at[n], self.r.at[n], self.right))
            self.go(send(src(half), dst, self.s_l.at[n], self.r.at[n], self.left))
            if self.s_sib is not None:
                self.go(send(src(half), dst, self.s_sib.at[n], self.r_sib.at[n], self.sib))

    def take(self, i, half, forward=0):
        n, at = 2 * i + half, self.slot(i, half)
        send(at, at, self.s_r.at[n], self.r.at[n], self.right).wait_recv()
        if forward > 0:
            self.go(send(at, at, self.s_r.at[n], self.r.at[n], self.right))
        if forward < 0:
            self.go(send(at, at, self.s_l.at[n], self.r.at[n], self.left))
        if self.s_sib is not None:
            self.go(send(at, at, self.s_sib.at[n], self.r_sib.at[n], self.sib))

    def middle(self, half):
        lo, hi = up(self.me, 3), up(self.me, 1)
        if half == 0:
            self.take(lo, 0, 1)
            self.take(hi, 0)
        else:
            self.take(hi, 1, -1)
            self.take(lo, 1)

    def last(self):
        self.take(up(self.me, 2), 0)
        self.take(up(self.me, 2), 1)


def pack_kernel(q_ref, k_ref, v_ref, g_ref, d_ref, n_ref, qt_ref, kv_ref, gain_ref):
    gain_ref[...] = jnp.broadcast_to(n_ref[...].astype(F32), (8, 256))
    qt = (q_ref[...].astype(F32) * (HD ** -0.5)).T.astype(BF)
    qt_ref[0] = qt[:HD]
    qt_ref[1] = qt[HD:]
    k_lo, k_hi = k_ref[:HALF].astype(F32), k_ref[HALF:].astype(F32)
    first = lax.broadcasted_iota(jnp.int32, (HALF, 128), 1) < HD
    kv_ref[0, 0, :HALF] = jnp.where(first, k_lo, pltpu.roll(k_hi, HD, 1)).astype(BF)
    kv_ref[0, 1, :HALF] = jnp.where(first, pltpu.roll(k_lo, HD, 1), k_hi).astype(BF)
    vt = v_ref[...].astype(F32).T.astype(BF)
    row = lax.broadcasted_iota(jnp.int32, (8, T), 0)
    doc0 = 1.0 - d_ref[...].astype(F32)
    for j in range(2):
        kv_ref[0, j, HALF:] = jnp.zeros((64, 128), BF)
        g = g_ref[j:j + 1, :]
        hi = g.astype(BF).astype(F32)
        mid = (g - hi).astype(BF).astype(F32)
        lo = (g - hi) - mid
        aux = jnp.where(row == 0, hi, jnp.where(row == 1, mid, jnp.where(row == 2, lo, jnp.where(row == 3, doc0, 0.0))))
        for n in range(8):
            kv_ref[1, j, n * 64:(n + 1) * 64] = vt[j * HD:(j + 1) * HD, n * 128:(n + 1) * 128]
        for n in range(4):
            two = jnp.concatenate([aux[:, (2 * n) * 128:(2 * n + 1) * 128], aux[:, (2 * n + 1) * 128:(2 * n + 2) * 128]], axis=0)
            kv_ref[1, j, HALF + n * 16:HALF + (n + 1) * 16] = two.astype(BF)


def pack(q, k, v, g, d, gain):
    return pl.pallas_call(
        pack_kernel,
        out_shape=(sds((2, HD, T), BF), sds((2, 2, ITEM, 128), BF), sds((8, 256), F32)),
        in_specs=[VM] * 6,
        out_specs=(VM, VM, VM),
        name="pack",
    )(q, k, v, g, d, gain)


def exchange_kernel(
    qt, kv, wo, res, gain, wu, wd, qin, kvall, woall, resin, gainall, wu4, wd4,
    qs, qr, ks, rr, s_sib, r_sib, s_r, s_l,
    wl, w_sib, wr_sib, w_s_r, w_s_l, w_r, es, er, gs, gr,
    u_s_r, u_s_l, u_r, d_s_r, d_s_l, d_r, ul,
):
    z, y, x, c = place()
    sp, tp = z * 4 + y, x * 2 + c
    sib = dev(z, y, x, 1 - c)
    yp, ym, y2 = up(y, 1), up(y, 3), up(y, 2)
    xp, xm, x2 = up(x, 1), up(x, 3), up(x, 2)

    barrier = pltpu.get_barrier_semaphore()
    cs = lax.div(z, 2)
    for zs in range(4):
        @pl.when(jnp.logical_not((z == zs) & (c == cs)))
        def _():
            signal(barrier, dev(zs, y, x, cs))

    for k in range(1, 8):
        signal(barrier, (sp, lax.rem(tp + k, 8)))
    signal(barrier, dev(z, yp, x, c))
    signal(barrier, dev(z, ym, x, c))
    zp, zm = up(z, 1), up(z, 3)
    signal(barrier, dev(zp, y, x, c))
    signal(barrier, dev(zm, y, x, c))
    pl.semaphore_wait(barrier, jnp.where(c == cs, 14, 15))

    def guarded(is_self, local, remote):
        @pl.when(is_self)
        def _():
            local.start()

        @pl.when(jnp.logical_not(is_self))
        def _():
            remote.start()

    pending = []
    for j in range(2):
        zt = 2 * c + j
        for t in range(2):
            mine = (zt == z) & (c == t)
            src, dst = kv.at[t, j], kvall.at[t, sp]
            remote = send(src, dst, ks.at[2 * t + j], rr.at[sp], dev(zt, y, x, t))
            guarded(mine, pltpu.make_async_copy(src, dst, rr.at[sp]), remote)
            pending.append((mine, remote))
    for j in range(2):
        zt = 2 * c + j
        for hf in range(2):
            ct = lax.rem(hf + z, 2)
            mine = (zt == z) & (ct == c)
            src, dst = qt.at[j, :, pl.ds(hf * HALF, HALF)], qin.at[z]
            remote = send(src, dst, qs.at[2 * j + hf], qr.at[z], dev(zt, y, x, ct))
            guarded(mine, pltpu.make_async_copy(src, dst, qr.at[z]), remote)
            pending.append((mine, remote))

    done = []

    def wrows(xs, half):
        return pl.ds((2 * xs + c) * 128 + half * 64, 64)

    def go(copy):
        copy.start()
        done.append(copy)

    ring_w = Ring(go, x, lambda i, half: woall.at[wrows(i, half)], dev(z, y, xp, c), dev(z, y, xm, c),
                  w_s_r, w_s_l, w_r, sib, w_sib, wr_sib)
    ring_u = Ring(go, y, lambda i, half: wu4.at[i, pl.ds(half * 64, 64)], dev(z, yp, x, c), dev(z, ym, x, c),
                  u_s_r, u_s_l, u_r)
    ring_d = Ring(go, z, lambda i, half: wd4.at[i, pl.ds(half * HALF, HALF)], dev(zp, y, x, c), dev(zm, y, x, c),
                  d_s_r, d_s_l, d_r)
    own_w = [
        pltpu.make_async_copy(wo, woall.at[pl.ds(pl.multiple_of(tp * 128, 128), 128)], wl.at[0]),
        pltpu.make_async_copy(wu, wu4.at[y], ul.at[0]),
        pltpu.make_async_copy(wd, wd4.at[z], ul.at[1]),
    ]
    for loc in own_w:
        loc.start()
    ring_w.start(lambda half: wo.at[pl.ds(half * 64, 64)])

    own_e = pltpu.make_async_copy(res.at[pl.ds(pl.multiple_of(tp * 128, 128), 128)],
                                  resin.at[:, pl.ds(pl.multiple_of(tp * 256, 256), 256)], er.at[tp])
    own_e.start()
    own_g = pltpu.make_async_copy(gain, gainall.at[:, pl.ds(pl.multiple_of(tp * 256, 256), 256)], gr.at[tp])
    own_g.start()
    for k in range(1, 8):
        to = lax.rem(tp + k, 8)
        cols = pl.ds(pl.multiple_of(tp * 256, 256), 256)
        go(send(res.at[pl.ds(pl.multiple_of(to * 128, 128), 128)], resin.at[:, cols], es.at[k], er.at[tp], (sp, to)))
        go(send(gain, gainall.at[:, cols], gs.at[k], gr.at[tp], (sp, to)))

    def arrived(b):
        send(kvall.at[c, b], kvall.at[c, b], s_sib.at[b], rr.at[b], sib).wait_recv()
        go(send(kvall.at[c, b], kvall.at[c, b], s_sib.at[b], r_sib.at[b], sib))

    def right(b):
        go(send(kvall.at[c, b], kvall.at[c, b], s_r.at[b], rr.at[b], dev(z, yp, x, c)))

    def left(b):
        go(send(kvall.at[c, b], kvall.at[c, b], s_l.at[b], rr.at[b], dev(z, ym, x, c)))

    zs = [z, up(z, 1), up(z, 3), up(z, 2)]

    def near(r):
        b = zs[r] * 4 + y
        arrived(b)
        right(b)
        left(b)

    def next_to(r):
        b = zs[r] * 4 + ym
        arrived(b)
        if r in (0, 2):
            right(b)
        b = zs[r] * 4 + yp
        arrived(b)
        if r in (1, 3):
            left(b)

    near(0)
    ring_d.start(lambda half: wd.at[pl.ds(half * HALF, HALF)])
    ring_u.start(lambda half: wu.at[pl.ds(half * 64, 64)])
    near(1)
    near(2)
    next_to(0)
    ring_w.middle(0)
    near(3)
    ring_u.middle(0)
    ring_d.middle(0)
    next_to(1)
    next_to(2)
    ring_w.middle(1)
    ring_u.middle(1)
    ring_d.middle(1)
    next_to(3)
    for r in range(4):
        arrived(zs[r] * 4 + y2)
    ring_w.last()
    ring_u.last()
    ring_d.last()

    for b in range(16):
        send(kvall.at[1 - c, b], kvall.at[1 - c, b], s_sib.at[b], r_sib.at[b], sib).wait_recv()
    for n in range(8):
        rows = pl.ds((2 * (n // 2) + (1 - c)) * 128 + (n % 2) * 64, 64)
        send(woall.at[rows], woall.at[rows], w_sib.at[n], wr_sib.at[n], sib).wait_recv()
    for i in range(4):
        send(qin.at[i], qin.at[i], qs.at[0], qr.at[i], sib).wait_recv()
    for n in range(8):
        cols = pl.ds(n * 256, 256)
        send(resin.at[:, cols], resin.at[:, cols], es.at[0], er.at[n], sib).wait_recv()
        send(gainall.at[:, cols], gainall.at[:, cols], gs.at[0], gr.at[n], sib).wait_recv()
    for loc in own_w:
        loc.wait()
    for mine, remote in pending:
        @pl.when(jnp.logical_not(mine))
        def _():
            remote.wait_send()
    for copy in done:
        copy.wait_send()


def exchange(qt, kv, wo, res, gain, wu, wd):
    return pl.pallas_call(
        exchange_kernel,
        out_shape=(
            sds((4, HD, HALF), BF),
            sds((2, 16, ITEM, 128), BF),
            sds((1024, D), BF),
            sds((128, D), BF),
            sds((8, D), F32),
            sds((4, 128, 1024), BF),
            sds((4, T, 128), BF),
        ),
        in_specs=[VM] * 7,
        out_specs=(HB,) * 7,
        scratch_shapes=[
            DMA((4,)), DMA((4,)), DMA((4,)), DMA((16,)), DMA((16,)), DMA((16,)), DMA((16,)), DMA((16,)),
            DMA((2,)), DMA((8,)), DMA((8,)), DMA((8,)), DMA((8,)), DMA((8,)),
            DMA((8,)), DMA((8,)), DMA((8,)), DMA((8,)),
            DMA((8,)), DMA((8,)), DMA((8,)), DMA((8,)), DMA((8,)), DMA((8,)), DMA((2,)),
        ],
        compiler_params=pltpu.CompilerParams(has_side_effects=True, collective_id=0),
        cost_estimate=pl.CostEstimate(flops=20_000_000_000, bytes_accessed=16_000_000, transcendentals=0),
        name="exchange",
    )(qt, kv, wo, res, gain, wu, wd)


QW = 256
NS = HALF // QW


def attend_kernel(q_ref, kv_ref, o_ref, pieces, gmat, w_ref, *scr):
    z, y, x, c = place()
    s_refs, accs, tops, shrinks = scr[:NS], scr[NS:2 * NS], scr[2 * NS:3 * NS], scr[3 * NS:]
    ones = jnp.ones((16, HALF), BF)
    count = jnp.zeros((1, 128), F32)
    for b in range(16):
        for n in range(8):
            a = kv_ref[1, b, HALF + n * 8:HALF + (n + 1) * 8, :].astype(F32)
            count = count + a[3:4]
            hf, at = n // 4, (n % 4) * 128
            pieces[b * 8 + hf * 4:b * 8 + hf * 4 + 4, at:at + 128] = a[:4]
    docs0 = jnp.sum(count).astype(jnp.int32)
    gmat[...] = pieces[...].T.astype(BF)
    row = lax.broadcasted_iota(jnp.int32, (128, QW), 0)
    unit_of_row, piece_of_row = row // 4, row % 4

    def tile(i, carry):
        hq = 2 * (4 * i + y) + lax.rem(c + i, 2)
        start = jnp.where(hq * HALF >= docs0, lax.div(docs0, HALF), 0)
        q_pos = hq * HALF + lax.broadcasted_iota(jnp.int32, (1, HALF), 1)
        doc1 = jnp.where(q_pos >= docs0, -BIG, 0.0)
        for k in range(NS):
            cols = slice(k * QW, (k + 1) * QW)
            w_ref[:, cols] = jnp.where(piece_of_row == 3, doc1[:, cols], -1.0)

        def scores(k, u, first):
            cols = slice(k * QW, (k + 1) * QW)
            q = q_ref[i, :, cols]
            none = jnp.zeros_like(q)
            b, low = lax.div(u, 2), lax.rem(u, 2) == 0
            lhs = jnp.concatenate([kv_ref[0, b, :HALF, :], gmat[...]], axis=1)
            sel = jnp.where(unit_of_row == u, w_ref[:, cols], 0.0).astype(BF)
            rhs = jnp.concatenate([jnp.where(low, q, none), jnp.where(low, none, q), sel], axis=0)
            s = jnp.dot(lhs, rhs, preferred_element_type=F32)
            if first:
                key = lax.broadcasted_iota(jnp.int32, (HALF, QW), 0)
                s = jnp.where(key <= k * QW + lax.broadcasted_iota(jnp.int32, (HALF, QW), 1), s, far_below)
            s_refs[k][...] = s
            new = jnp.max(s, axis=0, keepdims=True)
            if not first:
                old = tops[k][...]
                new = jnp.maximum(old, new)
                shrinks[k][...] = jnp.exp(old - new)
            tops[k][...] = new

        def weigh(k, u, first):
            b, hf = lax.div(u, 2), lax.rem(u, 2)
            p = jnp.exp(s_refs[k][...] - tops[k][...]).astype(BF)
            vt = jnp.concatenate(
                [kv_ref[1, b, pl.ds(pl.multiple_of(hf * 256 + n * 64, 64), 64), :] for n in range(4)], axis=1
            )
            vt = jnp.concatenate([vt, ones], axis=0)
            product = jnp.dot(vt, p, preferred_element_type=F32)
            accs[k][...] = product if first else accs[k][...] * shrinks[k][...] + product

        ahead = jnp.maximum(hq - 1, 0)
        scores(0, hq, True)
        scores(1, hq, True)
        weigh(0, hq, True)
        scores(0, jnp.minimum(start, ahead), False)
        weigh(1, hq, True)

        def step(u, carry):
            scores(1, u, False)
            weigh(0, u, False)
            scores(0, jnp.minimum(u + 1, ahead), False)
            weigh(1, u, False)
            return carry

        lax.fori_loop(start, hq, step, 0)
        for k in range(NS):
            total = accs[k][...]
            o_ref[i, :, k * QW:(k + 1) * QW] = (total[:HD] / total[HD:HD + 1]).astype(BF)
        return carry

    lax.fori_loop(0, 4, tile, 0)


def attend(q, kv):
    return pl.pallas_call(
        attend_kernel,
        out_shape=sds((4, HD, HALF), BF),
        in_specs=[VM, VM],
        out_specs=VM,
        scratch_shapes=[
            pltpu.VMEM((128, HALF), F32),
            pltpu.VMEM((HALF, 128), BF),
            pltpu.VMEM((128, HALF), F32),
        ]
        + [pltpu.VMEM((HALF, QW), F32)] * NS
        + [pltpu.VMEM((80, QW), F32)] * NS
        + [pltpu.VMEM((1, QW), F32)] * (2 * NS),
        compiler_params=pltpu.CompilerParams(vmem_limit_bytes=40 * 1024 * 1024),
        cost_estimate=pl.CostEstimate(flops=20_000_000_000, bytes_accessed=8_000_000, transcendentals=0),
        name="attend",
    )(q, kv)


def mix_kernel(
    att, wo_any, res, um, upl, dm, dpl, mid, uo, do,
    a_in, wo, own, w_sem, a_s, a_r, o_l, m_sib, mr_sib, m_s_r, m_s_l, m_r, o_s, o_r
):
    z, y, x, c = place()
    sp, tp = z * 4 + y, x * 2 + c
    sib = dev(z, y, x, 1 - c)
    xp, xm, x2 = up(x, 1), up(x, 3), up(x, 2)
    head = 4 * x + z
    barrier = pltpu.get_barrier_semaphore()
    cs = lax.rem(lax.div(tp, 4) + z, 2)
    for zs in range(4):
        for xs in range(4):
            @pl.when(jnp.logical_not((z == zs) & (x == xs) & (c == cs)))
            def _():
                signal(barrier, dev(zs, y, xs, cs))

    zp, zm = dev(up(z, 1), y, x, c), dev(up(z, 3), y, x, c)
    yp, ym = dev(z, up(y, 1), x, c), dev(z, up(y, 3), x, c)
    for near in (sib, dev(z, y, xp, c), dev(z, y, xm, c), zp, zm, yp, ym):
        signal(barrier, near)
    pl.semaphore_wait(barrier, jnp.where(lax.div(x, 2) == lax.rem(c + z, 2), 22, 23))
    w_copy = pltpu.make_async_copy(wo_any, wo, w_sem.at[0])
    w_copy.start()
    pending = []
    for i in range(4):
        hf = lax.rem(c + i, 2)
        for k in range(4):
            to = 4 * hf + k
            mine = (z == i) & (to == tp)
            src = att.at[i, :, pl.ds(k * 128, 128)]
            dst = a_in.at[pl.ds(pl.multiple_of(head * HD, HD), HD)]
            local = pltpu.make_async_copy(src, dst, a_r.at[head])
            remote = send(src, dst, a_s.at[4 * i + k], a_r.at[head], (i * 4 + y, to))

            @pl.when(mine)
            def _():
                local.start()

            @pl.when(jnp.logical_not(mine))
            def _():
                remote.start()

            pending.append((mine, remote))
    done = []

    def go(copy):
        copy.start()
        done.append(copy)

    first, second = pl.ds(0, 2), pl.ds(2, 2)
    opposite = [
        send(um.at[first], uo.at[first], o_s.at[0], o_r.at[0], zp),
        send(upl.at[second], uo.at[second], o_s.at[1], o_r.at[1], zm),
        send(dm.at[first], do.at[first], o_s.at[2], o_r.at[2], yp),
        send(dpl.at[second], do.at[second], o_s.at[3], o_r.at[3], ym),
    ]
    for h in range(16):
        rows = pl.ds(h * HD, HD)
        send(a_in.at[rows], a_in.at[rows], a_s.at[0], a_r.at[h], sib).wait_recv()
    for copy in opposite:
        go(copy)
    w_copy.wait()
    a = a_in[...].astype(F32).T.astype(BF)
    for n in range(4):
        cols = slice(n * 512, (n + 1) * 512)
        mixed = jnp.dot(a, wo[:, cols], preferred_element_type=F32)
        own[:, cols] = (res[:, cols].astype(F32) + mixed).astype(BF)

    def rows_of(xs, cc, half):
        return pl.ds((2 * xs + cc) * 128 + half * 64, 64)

    ring = Ring(go, x, lambda i, half: mid.at[rows_of(i, c, half)], dev(z, y, xp, c), dev(z, y, xm, c),
                m_s_r, m_s_l, m_r, sib, m_sib, mr_sib)
    ring.start(lambda half: own.at[pl.ds(half * 64, 64)])
    locals_ = [pltpu.make_async_copy(own, mid.at[pl.ds(pl.multiple_of(tp * 128, 128), 128)], o_l.at[0])]
    locals_[0].start()
    ring.middle(0)
    ring.middle(1)
    ring.last()
    for n in range(8):
        rows = rows_of(n // 2, 1 - c, n % 2)
        send(mid.at[rows], mid.at[rows], m_sib.at[n], mr_sib.at[n], sib).wait_recv()
    for copy in opposite:
        copy.wait_recv()
    for loc in locals_:
        loc.wait()
    for mine, remote in pending:
        @pl.when(jnp.logical_not(mine))
        def _():
            remote.wait_send()
    for copy in done:
        copy.wait_send()


def mix(att, wo, res, um, upl, dm, dpl):
    return pl.pallas_call(
        mix_kernel,
        out_shape=(sds((T, D), BF), sds((4, 128, 1024), BF), sds((4, T, 128), BF)),
        in_specs=[VM, HB, VM, HB, HB, HB, HB],
        out_specs=(HB, HB, HB),
        scratch_shapes=[
            pltpu.VMEM((1024, 128), BF),
            pltpu.VMEM((1024, D), BF),
            pltpu.VMEM((128, D), BF),
            DMA((1,)), DMA((16,)), DMA((16,)), DMA((1,)),
            DMA((8,)), DMA((8,)), DMA((8,)), DMA((8,)), DMA((8,)), DMA((4,)), DMA((4,)),
        ],
        compiler_params=pltpu.CompilerParams(has_side_effects=True, collective_id=1),
        cost_estimate=pl.CostEstimate(flops=20_000_000_000, bytes_accessed=8_000_000, transcendentals=0),
        name="mix",
    )(att, wo, res, um, upl, dm, dpl)


def feed_kernel(mid, gain, u0, um, upl, uo, d0, dm, dpl, do, part, normed, hidden):
    z, y, x, c = place()
    wide = mid[...].astype(F32)
    inv = lax.rsqrt(jnp.mean(wide * wide, axis=-1, keepdims=True) + eps)
    normed[...] = (wide * inv * gain[0:1, :]).astype(BF)
    total = None
    for rel, u in ((0, u0), (3, um), (1, upl), (2, uo)):
        cols = pl.ds(pl.multiple_of(up(z, rel) * 512, 512), 512)
        term = jnp.dot(normed[:, cols], u[...], preferred_element_type=F32)
        total = term if total is None else total + term
    hidden[...] = jnp.square(jnp.maximum(total, 0.0)).astype(BF)
    for rel, d in ((0, d0), (3, dm), (1, dpl), (2, do)):
        yy = up(y, rel)
        for k in (0, 2):
            rhs = jnp.concatenate([d[k], d[k + 1]], axis=1)
            term = jnp.dot(hidden[...], rhs, preferred_element_type=F32).astype(BF)
            for n in range(2):
                cols = pl.ds(pl.multiple_of(((k + n) * 4 + yy) * 128, 128), 128)
                part[:, cols] = term[:, n * 128:(n + 1) * 128]


def feed(mid, gain, ups, downs):
    rows = 256
    u_spec = pl.BlockSpec((512, 1024), lambda i: (0, 0))
    d_spec = pl.BlockSpec((4, T, 128), lambda i: (0, 0, 0))
    return pl.pallas_call(
        feed_kernel,
        grid=(T // rows,),
        out_shape=sds((T, D), BF),
        in_specs=[pl.BlockSpec((rows, D), lambda i: (i, 0)), pl.BlockSpec((8, D), lambda i: (0, 0))] + [u_spec] * 4 + [d_spec] * 4,
        out_specs=pl.BlockSpec((rows, D), lambda i: (i, 0)),
        scratch_shapes=[pltpu.VMEM((rows, D), BF), pltpu.VMEM((rows, 1024), BF)],
        cost_estimate=pl.CostEstimate(flops=9_000_000_000, bytes_accessed=16_000_000, transcendentals=0),
        name="feed",
    )(mid, gain, *ups, *downs)


def scatter_kernel(
    part, mid, out, sibbuf, stage, hop_a, hop_b, from_l, from_r, res,
    mid_sem, s_sib, r_sib, s_hop, r_hop, s_out, r_l, r_r,
):
    z, y, x, c = place()
    tp = x * 2 + c
    sib = dev(z, y, x, 1 - c)
    right, left = dev(z, y, up(x, 1), c), dev(z, y, up(x, 3), c)
    barrier = pltpu.get_barrier_semaphore()
    for near in (sib, right, left):
        signal(barrier, near)
    pl.semaphore_wait(barrier, 3)
    m_copy = pltpu.make_async_copy(mid.at[:, pl.ds(pl.multiple_of(tp * 256, 256), 256)], res, mid_sem.at[0])
    m_copy.start()
    done = []

    def go(copy):
        copy.start()
        done.append(copy)

    for rel in (2, 1, 3, 0):
        xt = up(x, rel)
        cols = pl.ds(pl.multiple_of((2 * xt + 1 - c) * 256, 256), 256)
        go(send(part.at[:, cols], sibbuf.at[rel], s_sib.at[rel], r_sib.at[rel], sib))

    def chunks(lo, n, f):
        def one(k, carry):
            f(pl.ds(pl.multiple_of(lo + k * 128, 128), 128), pl.ds(pl.multiple_of(k * 128, 128), 128))
            return carry

        lax.fori_loop(0, n, one, 0)

    def pair(rel):
        send(sibbuf.at[rel], sibbuf.at[rel], s_sib.at[rel], r_sib.at[rel], sib).wait_recv()
        xt = up(x, rel)
        cols = pl.ds(pl.multiple_of((2 * xt + c) * 256, 256), 256)
        return lambda rows: part[rows, cols].astype(F32) + sibbuf[rel, rows, :].astype(F32)

    A, B = pl.ds(0, HALF), pl.ds(HALF, HALF)

    def put(rel, value):
        def f(rows, _):
            stage[rel, rows, :] = value(rows).astype(BF)

        return f

    two = pair(2)
    chunks(0, 8, put(2, two))
    go(send(stage.at[2, A], hop_a, s_hop.at[0], r_hop.at[0], right))
    go(send(stage.at[2, B], hop_b, s_hop.at[1], r_hop.at[1], left))
    one = pair(1)
    chunks(HALF, 4, put(1, one))
    go(send(stage.at[1, B], from_l.at[B], s_out.at[0], r_l.at[1], right))
    three = pair(3)
    chunks(0, 4, put(3, three))
    go(send(stage.at[3, A], from_r.at[A], s_out.at[1], r_r.at[0], left))

    send(hop_a, hop_a, s_hop.at[0], r_hop.at[0], sib).wait_recv()

    def fold_a(rows, rel):
        stage[1, rows, :] = (one(rows) + hop_a[rel, :].astype(F32)).astype(BF)

    chunks(0, 4, fold_a)
    go(send(stage.at[1, A], from_l.at[A], s_out.at[2], r_l.at[0], right))
    send(hop_b, hop_b, s_hop.at[1], r_hop.at[1], sib).wait_recv()

    def fold_b(rows, rel):
        stage[3, rows, :] = (three(rows) + hop_b[rel, :].astype(F32)).astype(BF)

    chunks(HALF, 4, fold_b)
    go(send(stage.at[3, B], from_r.at[B], s_out.at[3], r_r.at[1], left))
    mine = pair(0)
    m_copy.wait()
    send(from_l.at[B], from_l.at[B], s_out.at[0], r_l.at[1], sib).wait_recv()
    send(from_r.at[A], from_r.at[A], s_out.at[0], r_r.at[0], sib).wait_recv()
    send(from_l.at[A], from_l.at[A], s_out.at[0], r_l.at[0], sib).wait_recv()
    send(from_r.at[B], from_r.at[B], s_out.at[0], r_r.at[1], sib).wait_recv()

    def final(rows, _):
        feed = mine(rows) + from_l[rows, :].astype(F32) + from_r[rows, :].astype(F32)
        out[rows, :] = (res[rows, :].astype(F32) + feed).astype(BF)

    chunks(0, 8, final)
    for copy in done:
        copy.wait_send()


def scatter(part, mid):
    return pl.pallas_call(
        scatter_kernel,
        out_shape=sds((T, 256), BF),
        in_specs=[VM, HB],
        out_specs=VM,
        scratch_shapes=[
            pltpu.VMEM((4, T, 256), BF),
            pltpu.VMEM((4, T, 256), BF),
            pltpu.VMEM((HALF, 256), BF),
            pltpu.VMEM((HALF, 256), BF),
            pltpu.VMEM((T, 256), BF),
            pltpu.VMEM((T, 256), BF),
            pltpu.VMEM((T, 256), BF),
            DMA((1,)), DMA((4,)), DMA((4,)), DMA((2,)), DMA((2,)), DMA((4,)), DMA((2,)), DMA((2,)),
        ],
        compiler_params=pltpu.CompilerParams(has_side_effects=True, collective_id=2),
        cost_estimate=pl.CostEstimate(flops=20_000_000_000, bytes_accessed=8_000_000, transcendentals=0),
        name="scatter",
    )(part, mid)


def shifted(value, axis, step):
    def index(z, y):
        return (z % 4) * 4 + y % 4

    pairs = [
        (index(z, y), index(z + step, y) if axis == "z" else index(z, y + step)) for z in range(4) for y in range(4)
    ]
    return lax.ppermute(value, "sp", pairs)


def body(queries, keys, values, cum_gates, doc_ids, residual, w_out, norm_gain, w_up, w_down):
    qt, kv, gain8 = pack(queries, keys, values, jnp.transpose(cum_gates), doc_ids.reshape(1, T), norm_gain.reshape(1, 256))
    qin, kvall, woall, resin, gain, u0, d0 = exchange(qt, kv, w_out, residual, gain8, w_up, w_down)
    um, upl = shifted(u0, "z", 1), shifted(u0, "z", -1)
    dm, dpl = shifted(d0, "y", 1), shifted(d0, "y", -1)
    att = attend(qin, kvall)
    mid, uo, do = mix(att, woall, resin, um, upl, dm, dpl)
    ups = [u.reshape(512, 1024) for u in (u0, um, upl, uo)]
    part = feed(mid, gain, ups, (d0, dm, dpl, do))
    return scatter(part, mid)


def solution(mesh):
    in_specs = (
        P("sp", "tp"),
        P("sp", "tp"),
        P("sp", "tp"),
        P("sp", "tp"),
        P("sp"),
        P("sp", "tp"),
        P("tp", None),
        P("tp"),
        P("sp", "tp"),
        P("tp", "sp"),
    )
    return jax.shard_map(body, mesh=mesh, in_specs=in_specs, out_specs=P("sp", "tp"), check_vma=False)
```

```python
import functools

import jax
import jax.numpy as jnp
from jax import lax
from jax.experimental import pallas as pl
from jax.experimental.pallas import tpu as pltpu
from jax.sharding import PartitionSpec as P

D = 2048
HD = 64
T = 1024
HALF = 512
ITEM = 576
eps = 1e-06
far_below = -1e30
BIG = 8192.0
MESH = pl.DeviceIdType.MESH
BF = jnp.bfloat16
F32 = jnp.float32
VM = pl.BlockSpec(memory_space=pltpu.VMEM)
HB = pl.BlockSpec(memory_space=pl.ANY)
DMA = pltpu.SemaphoreType.DMA


def sds(shape, dtype):
    return jax.ShapeDtypeStruct(shape, dtype)


def place():
    sp, tp = lax.axis_index("sp"), lax.axis_index("tp")
    return lax.div(sp, 4), lax.rem(sp, 4), lax.div(tp, 2), lax.rem(tp, 2)


def dev(z, y, x, c):
    return (z * 4 + y, x * 2 + c)


def send(src, dst, ssem, rsem, device):
    return pltpu.make_async_remote_copy(
        src_ref=src, dst_ref=dst, send_sem=ssem, recv_sem=rsem, device_id=device, device_id_type=MESH
    )


def up(v, k):
    return lax.rem(v + k, 4)


def signal(barrier, device):
    pl.semaphore_signal(barrier, inc=1, device_id=device, device_id_type=MESH)


class Ring:
    def __init__(self, go, me, slot, right, left, s_r, s_l, r, sib=None, s_sib=None, r_sib=None):
        self.go, self.me, self.slot, self.right, self.left = go, me, slot, right, left
        self.s_r, self.s_l, self.r = s_r, s_l, r
        self.sib, self.s_sib, self.r_sib = sib, s_sib, r_sib

    def start(self, src, order=(0, 1)):
        for half in order:
            n, dst = 2 * self.me + half, self.slot(self.me, half)
            self.go(send(src(half), dst, self.s_r.at[n], self.r.at[n], self.right))
            self.go(send(src(half), dst, self.s_l.at[n], self.r.at[n], self.left))
            if self.s_sib is not None:
                self.go(send(src(half), dst, self.s_sib.at[n], self.r_sib.at[n], self.sib))

    def take(self, i, half, forward=0):
        n, at = 2 * i + half, self.slot(i, half)
        send(at, at, self.s_r.at[n], self.r.at[n], self.right).wait_recv()
        if forward > 0:
            self.go(send(at, at, self.s_r.at[n], self.r.at[n], self.right))
        if forward < 0:
            self.go(send(at, at, self.s_l.at[n], self.r.at[n], self.left))
        if self.s_sib is not None:
            self.go(send(at, at, self.s_sib.at[n], self.r_sib.at[n], self.sib))

    def middle(self, half):
        lo, hi = up(self.me, 3), up(self.me, 1)
        if half == 0:
            self.take(lo, 0, 1)
            self.take(hi, 0)
        else:
            self.take(hi, 1, -1)
            self.take(lo, 1)

    def last(self):
        self.take(up(self.me, 2), 0)
        self.take(up(self.me, 2), 1)


def pack_kernel(q_ref, k_ref, v_ref, g_ref, d_ref, n_ref, qt_ref, kv_ref, gain_ref):
    gain_ref[...] = jnp.broadcast_to(n_ref[...].astype(F32), (8, 256))
    qt = (q_ref[...].astype(F32) * (HD ** -0.5)).T.astype(BF)
    qt_ref[0] = qt[:HD]
    qt_ref[1] = qt[HD:]
    k_lo, k_hi = k_ref[:HALF].astype(F32), k_ref[HALF:].astype(F32)
    first = lax.broadcasted_iota(jnp.int32, (HALF, 128), 1) < HD
    kv_ref[0, 0, :HALF] = jnp.where(first, k_lo, pltpu.roll(k_hi, HD, 1)).astype(BF)
    kv_ref[0, 1, :HALF] = jnp.where(first, pltpu.roll(k_lo, HD, 1), k_hi).astype(BF)
    vt = v_ref[...].astype(F32).T.astype(BF)
    row = lax.broadcasted_iota(jnp.int32, (8, T), 0)
    doc0 = 1.0 - d_ref[...].astype(F32)
    for j in range(2):
        kv_ref[0, j, HALF:] = jnp.zeros((64, 128), BF)
        g = g_ref[j:j + 1, :]
        hi = g.astype(BF).astype(F32)
        mid = (g - hi).astype(BF).astype(F32)
        lo = (g - hi) - mid
        aux = jnp.where(row == 0, hi, jnp.where(row == 1, mid, jnp.where(row == 2, lo, jnp.where(row == 3, doc0, 0.0))))
        for n in range(8):
            kv_ref[1, j, n * 64:(n + 1) * 64] = vt[j * HD:(j + 1) * HD, n * 128:(n + 1) * 128]
        for n in range(4):
            two = jnp.concatenate([aux[:, (2 * n) * 128:(2 * n + 1) * 128], aux[:, (2 * n + 1) * 128:(2 * n + 2) * 128]], axis=0)
            kv_ref[1, j, HALF + n * 16:HALF + (n + 1) * 16] = two.astype(BF)


def pack(q, k, v, g, d, gain):
    return pl.pallas_call(
        pack_kernel,
        out_shape=(sds((2, HD, T), BF), sds((2, 2, ITEM, 128), BF), sds((8, 256), F32)),
        in_specs=[VM] * 6,
        out_specs=(VM, VM, VM),
        name="pack",
    )(q, k, v, g, d, gain)


def exchange_kernel(
    qt, kv, wo, res, gain, wu, wd, qin, kvall, woall, resin, gainall, wu4, wd4,
    qs, qr, ks, rr, s_sib, r_sib, s_r, s_l,
    wl, w_sib, wr_sib, w_s_r, w_s_l, w_r, es, er, gs, gr,
    u_s_r, u_s_l, u_r, d_s_r, d_s_l, d_r, ul,
):
    z, y, x, c = place()
    sp, tp = z * 4 + y, x * 2 + c
    sib = dev(z, y, x, 1 - c)
    yp, ym, y2 = up(y, 1), up(y, 3), up(y, 2)
    xp, xm, x2 = up(x, 1), up(x, 3), up(x, 2)

    barrier = pltpu.get_barrier_semaphore()
    cs = lax.div(z, 2)
    for zs in range(4):
        @pl.when(jnp.logical_not((z == zs) & (c == cs)))
        def _():
            signal(barrier, dev(zs, y, x, cs))

    for k in range(1, 8):
        signal(barrier, (sp, lax.rem(tp + k, 8)))
    signal(barrier, dev(z, yp, x, c))
    signal(barrier, dev(z, ym, x, c))
    zp, zm = up(z, 1), up(z, 3)
    signal(barrier, dev(zp, y, x, c))
    signal(barrier, dev(zm, y, x, c))
    pl.semaphore_wait(barrier, jnp.where(c == cs, 14, 15))

    def guarded(is_self, local, remote):
        @pl.when(is_self)
        def _():
            local.start()

        @pl.when(jnp.logical_not(is_self))
        def _():
            remote.start()

    pending = []
    for j in range(2):
        zt = 2 * c + j
        for t in range(2):
            mine = (zt == z) & (c == t)
            src, dst = kv.at[t, j], kvall.at[t, sp]
            remote = send(src, dst, ks.at[2 * t + j], rr.at[sp], dev(zt, y, x, t))
            guarded(mine, pltpu.make_async_copy(src, dst, rr.at[sp]), remote)
            pending.append((mine, remote))
    for j in range(2):
        zt = 2 * c + j
        for hf in range(2):
            ct = lax.rem(hf + z, 2)
            mine = (zt == z) & (ct == c)
            src, dst = qt.at[j, :, pl.ds(hf * HALF, HALF)], qin.at[z]
            remote = send(src, dst, qs.at[2 * j + hf], qr.at[z], dev(zt, y, x, ct))
            guarded(mine, pltpu.make_async_copy(src, dst, qr.at[z]), remote)
            pending.append((mine, remote))

    done = []

    def wrows(xs, half):
        return pl.ds((2 * xs + c) * 128 + half * 64, 64)

    def go(copy):
        copy.start()
        done.append(copy)

    ring_w = Ring(go, x, lambda i, half: woall.at[wrows(i, half)], dev(z, y, xp, c), dev(z, y, xm, c),
                  w_s_r, w_s_l, w_r, sib, w_sib, wr_sib)
    ring_u = Ring(go, y, lambda i, half: wu4.at[i, pl.ds(half * 64, 64)], dev(z, yp, x, c), dev(z, ym, x, c),
                  u_s_r, u_s_l, u_r)
    ring_d = Ring(go, z, lambda i, half: wd4.at[i, pl.ds(half * HALF, HALF)], dev(zp, y, x, c), dev(zm, y, x, c),
                  d_s_r, d_s_l, d_r)
    own_w = [
        pltpu.make_async_copy(wo, woall.at[pl.ds(pl.multiple_of(tp * 128, 128), 128)], wl.at[0]),
        pltpu.make_async_copy(wu, wu4.at[y], ul.at[0]),
        pltpu.make_async_copy(wd, wd4.at[z], ul.at[1]),
    ]
    for loc in own_w:
        loc.start()
    ring_w.start(lambda half: wo.at[pl.ds(half * 64, 64)])

    own_e = pltpu.make_async_copy(res.at[pl.ds(pl.multiple_of(tp * 128, 128), 128)],
                                  resin.at[:, pl.ds(pl.multiple_of(tp * 256, 256), 256)], er.at[tp])
    own_e.start()
    own_g = pltpu.make_async_copy(gain, gainall.at[:, pl.ds(pl.multiple_of(tp * 256, 256), 256)], gr.at[tp])
    own_g.start()
    for k in range(1, 8):
        to = lax.rem(tp + k, 8)
        cols = pl.ds(pl.multiple_of(tp * 256, 256), 256)
        go(send(res.at[pl.ds(pl.multiple_of(to * 128, 128), 128)], resin.at[:, cols], es.at[k], er.at[tp], (sp, to)))
        go(send(gain, gainall.at[:, cols], gs.at[k], gr.at[tp], (sp, to)))

    def arrived(b):
        send(kvall.at[c, b], kvall.at[c, b], s_sib.at[b], rr.at[b], sib).wait_recv()
        go(send(kvall.at[c, b], kvall.at[c, b], s_sib.at[b], r_sib.at[b], sib))

    def right(b):
        go(send(kvall.at[c, b], kvall.at[c, b], s_r.at[b], rr.at[b], dev(z, yp, x, c)))

    def left(b):
        go(send(kvall.at[c, b], kvall.at[c, b], s_l.at[b], rr.at[b], dev(z, ym, x, c)))

    zs = [z, up(z, 1), up(z, 3), up(z, 2)]

    def near(r):
        b = zs[r] * 4 + y
        arrived(b)
        right(b)
        left(b)

    def next_to(r):
        b = zs[r] * 4 + ym
        arrived(b)
        if r in (0, 2):
            right(b)
        b = zs[r] * 4 + yp
        arrived(b)
        if r in (1, 3):
            left(b)

    near(0)
    ring_d.start(lambda half: wd.at[pl.ds(half * HALF, HALF)])
    ring_u.start(lambda half: wu.at[pl.ds(half * 64, 64)])
    near(1)
    near(2)
    next_to(0)
    ring_w.middle(0)
    near(3)
    ring_u.middle(0)
    ring_d.middle(0)
    next_to(1)
    next_to(2)
    ring_w.middle(1)
    ring_u.middle(1)
    ring_d.middle(1)
    next_to(3)
    for r in range(4):
        arrived(zs[r] * 4 + y2)
    ring_w.last()
    ring_u.last()
    ring_d.last()

    for b in range(16):
        send(kvall.at[1 - c, b], kvall.at[1 - c, b], s_sib.at[b], r_sib.at[b], sib).wait_recv()
    for n in range(8):
        rows = pl.ds((2 * (n // 2) + (1 - c)) * 128 + (n % 2) * 64, 64)
        send(woall.at[rows], woall.at[rows], w_sib.at[n], wr_sib.at[n], sib).wait_recv()
    for i in range(4):
        send(qin.at[i], qin.at[i], qs.at[0], qr.at[i], sib).wait_recv()
    for n in range(8):
        cols = pl.ds(n * 256, 256)
        send(resin.at[:, cols], resin.at[:, cols], es.at[0], er.at[n], sib).wait_recv()
        send(gainall.at[:, cols], gainall.at[:, cols], gs.at[0], gr.at[n], sib).wait_recv()
    for loc in own_w:
        loc.wait()
    for mine, remote in pending:
        @pl.when(jnp.logical_not(mine))
        def _():
            remote.wait_send()
    for copy in done:
        copy.wait_send()


def exchange(qt, kv, wo, res, gain, wu, wd):
    return pl.pallas_call(
        exchange_kernel,
        out_shape=(
            sds((4, HD, HALF), BF),
            sds((2, 16, ITEM, 128), BF),
            sds((1024, D), BF),
            sds((128, D), BF),
            sds((8, D), F32),
            sds((4, 128, 1024), BF),
            sds((4, T, 128), BF),
        ),
        in_specs=[VM] * 7,
        out_specs=(HB,) * 7,
        scratch_shapes=[
            DMA((4,)), DMA((4,)), DMA((4,)), DMA((16,)), DMA((16,)), DMA((16,)), DMA((16,)), DMA((16,)),
            DMA((2,)), DMA((8,)), DMA((8,)), DMA((8,)), DMA((8,)), DMA((8,)),
            DMA((8,)), DMA((8,)), DMA((8,)), DMA((8,)),
            DMA((8,)), DMA((8,)), DMA((8,)), DMA((8,)), DMA((8,)), DMA((8,)), DMA((2,)),
        ],
        compiler_params=pltpu.CompilerParams(has_side_effects=True, collective_id=0),
        cost_estimate=pl.CostEstimate(flops=20_000_000_000, bytes_accessed=16_000_000, transcendentals=0),
        name="exchange",
    )(qt, kv, wo, res, gain, wu, wd)


QW = 256
NS = HALF // QW


def attend_kernel(q_ref, kv_ref, o_ref, pieces, gmat, w_ref, *scr):
    z, y, x, c = place()
    s_refs, accs, tops, shrinks = scr[:NS], scr[NS:2 * NS], scr[2 * NS:3 * NS], scr[3 * NS:]
    ones = jnp.ones((16, HALF), BF)
    count = jnp.zeros((1, 128), F32)
    for b in range(16):
        for n in range(8):
            a = kv_ref[1, b, HALF + n * 8:HALF + (n + 1) * 8, :].astype(F32)
            count = count + a[3:4]
            hf, at = n // 4, (n % 4) * 128
            pieces[b * 8 + hf * 4:b * 8 + hf * 4 + 4, at:at + 128] = a[:4]
    docs0 = jnp.sum(count).astype(jnp.int32)
    gmat[...] = pieces[...].T.astype(BF)
    row = lax.broadcasted_iota(jnp.int32, (128, QW), 0)
    unit_of_row, piece_of_row = row // 4, row % 4

    def tile(i, carry):
        hq = 2 * (4 * i + y) + lax.rem(c + i, 2)
        start = jnp.where(hq * HALF >= docs0, lax.div(docs0, HALF), 0)
        q_pos = hq * HALF + lax.broadcasted_iota(jnp.int32, (1, HALF), 1)
        doc1 = jnp.where(q_pos >= docs0, -BIG, 0.0)
        for k in range(NS):
            cols = slice(k * QW, (k + 1) * QW)
            w_ref[:, cols] = jnp.where(piece_of_row == 3, doc1[:, cols], -1.0)

        def scores(k, u, first):
            cols = slice(k * QW, (k + 1) * QW)
            q = q_ref[i, :, cols]
            none = jnp.zeros_like(q)
            b, low = lax.div(u, 2), lax.rem(u, 2) == 0
            lhs = jnp.concatenate([kv_ref[0, b, :HALF, :], gmat[...]], axis=1)
            sel = jnp.where(unit_of_row == u, w_ref[:, cols], 0.0).astype(BF)
            rhs = jnp.concatenate([jnp.where(low, q, none), jnp.where(low, none, q), sel], axis=0)
            s = jnp.dot(lhs, rhs, preferred_element_type=F32)
            if first:
                key = lax.broadcasted_iota(jnp.int32, (HALF, QW), 0)
                s = jnp.where(key <= k * QW + lax.broadcasted_iota(jnp.int32, (HALF, QW), 1), s, far_below)
            s_refs[k][...] = s
            new = jnp.max(s, axis=0, keepdims=True)
            if not first:
                old = tops[k][...]
                new = jnp.maximum(old, new)
                shrinks[k][...] = jnp.exp(old - new)
            tops[k][...] = new

        def weigh(k, u, first):
            b, hf = lax.div(u, 2), lax.rem(u, 2)
            p = jnp.exp(s_refs[k][...] - tops[k][...]).astype(BF)
            vt = jnp.concatenate(
                [kv_ref[1, b, pl.ds(pl.multiple_of(hf * 256 + n * 64, 64), 64), :] for n in range(4)], axis=1
            )
            vt = jnp.concatenate([vt, ones], axis=0)
            product = jnp.dot(vt, p, preferred_element_type=F32)
            accs[k][...] = product if first else accs[k][...] * shrinks[k][...] + product

        ahead = jnp.maximum(hq - 1, 0)
        scores(0, hq, True)
        scores(1, hq, True)
        weigh(0, hq, True)
        scores(0, jnp.minimum(start, ahead), False)
        weigh(1, hq, True)

        def step(u, carry):
            scores(1, u, False)
            weigh(0, u, False)
            scores(0, jnp.minimum(u + 1, ahead), False)
            weigh(1, u, False)
            return carry

        lax.fori_loop(start, hq, step, 0)
        for k in range(NS):
            total = accs[k][...]
            o_ref[i, :, k * QW:(k + 1) * QW] = (total[:HD] / total[HD:HD + 1]).astype(BF)
        return carry

    lax.fori_loop(0, 4, tile, 0)


def attend(q, kv):
    return pl.pallas_call(
        attend_kernel,
        out_shape=sds((4, HD, HALF), BF),
        in_specs=[VM, VM],
        out_specs=VM,
        scratch_shapes=[
            pltpu.VMEM((128, HALF), F32),
            pltpu.VMEM((HALF, 128), BF),
            pltpu.VMEM((128, HALF), F32),
        ]
        + [pltpu.VMEM((HALF, QW), F32)] * NS
        + [pltpu.VMEM((80, QW), F32)] * NS
        + [pltpu.VMEM((1, QW), F32)] * (2 * NS),
        compiler_params=pltpu.CompilerParams(vmem_limit_bytes=40 * 1024 * 1024),
        cost_estimate=pl.CostEstimate(flops=20_000_000_000, bytes_accessed=8_000_000, transcendentals=0),
        name="attend",
    )(q, kv)


G = 4
ROWS = T // G
PIECE = 128 // G
A, B = pl.ds(0, ROWS // 2), pl.ds(ROWS // 2, ROWS // 2)


def tail_kernel(
    att, wo_any, res, gain, u0, um, upl, d0, dm, dpl, out,
    a_in, wo, own, midb, wu, wd, normed, hidden, part, sibbuf, stage, hop_a, hop_b, from_l, from_r,
    w_sem, a_s, a_r, o_s, o_r, g_s, g_r, t_s, t_r,
):
    z, y, x, c = place()
    sp, tp = z * 4 + y, x * 2 + c
    sib = dev(z, y, x, 1 - c)
    xp, xm, x2 = up(x, 1), up(x, 3), up(x, 2)
    right, left = dev(z, y, xp, c), dev(z, y, xm, c)
    z_next, z_prev, y_next, y_prev = up(z, 1), up(z, 3), up(y, 1), up(y, 3)
    head = 4 * x + z

    barrier = pltpu.get_barrier_semaphore()
    cs = lax.rem(lax.div(tp, 4) + z, 2)
    for zs in range(4):
        for xs in range(4):
            @pl.when(jnp.logical_not((z == zs) & (x == xs) & (c == cs)))
            def _():
                signal(barrier, dev(zs, y, xs, cs))

    to_z = dev(z_next, y, x, c), dev(z_prev, y, x, c)
    to_y = dev(z, y_next, x, c), dev(z, y_prev, x, c)
    for device in (sib, right, left, *to_z, *to_y):
        signal(barrier, device)
    pl.semaphore_wait(barrier, jnp.where(lax.div(x, 2) == lax.rem(c + z, 2), 22, 23))

    done = []

    def go(copy):
        copy.start()
        done.append(copy)

    pending = []
    for i in range(4):
        hf = lax.rem(c + i, 2)
        for k in range(4):
            to = 4 * hf + k
            mine = (z == i) & (to == tp)
            src = att.at[i, :, pl.ds(k * 128, 128)]
            dst = a_in.at[pl.ds(pl.multiple_of(head * HD, HD), HD)]
            local = pltpu.make_async_copy(src, dst, a_r.at[head])
            remote = send(src, dst, a_s.at[4 * i + k], a_r.at[head], (i * 4 + y, to))

            @pl.when(mine)
            def _():
                local.start()

            @pl.when(jnp.logical_not(mine))
            def _():
                remote.start()

            pending.append((mine, remote))

    def wu_rows(zz, lo, n):
        return wu.at[pl.ds(pl.multiple_of(zz * 512 + lo, 256), n)]

    loads = [
        pltpu.make_async_copy(wo_any, wo, w_sem.at[0]),
        pltpu.make_async_copy(u0, wu_rows(z, 0, 512), w_sem.at[1]),
        pltpu.make_async_copy(um, wu_rows(z_prev, 0, 512), w_sem.at[2]),
        pltpu.make_async_copy(upl, wu_rows(z_next, 0, 512), w_sem.at[3]),
        pltpu.make_async_copy(d0, wd.at[y], w_sem.at[4]),
        pltpu.make_async_copy(dm, wd.at[y_prev], w_sem.at[5]),
        pltpu.make_async_copy(dpl, wd.at[y_next], w_sem.at[6]),
    ]
    for load in loads:
        load.start()
    go(send(um.at[pl.ds(0, 256)], wu_rows(z_prev, 0, 256), o_s.at[0], o_r.at[0], to_z[0]))
    go(send(upl.at[pl.ds(256, 256)], wu_rows(z_next, 256, 256), o_s.at[1], o_r.at[1], to_z[1]))
    go(send(dm.at[pl.ds(0, 2)], wd.at[y_prev, pl.ds(0, 2)], o_s.at[2], o_r.at[2], to_y[0]))
    go(send(dpl.at[pl.ds(2, 2)], wd.at[y_next, pl.ds(2, 2)], o_s.at[3], o_r.at[3], to_y[1]))

    for h in range(16):
        rows = pl.ds(h * HD, HD)
        send(a_in.at[rows], a_in.at[rows], a_s.at[0], a_r.at[h], sib).wait_recv()
    loads[0].wait()
    a = a_in[...].astype(F32).T.astype(BF)
    for n in range(4):
        cols = slice(n * 512, (n + 1) * 512)
        mixed = jnp.dot(a, wo[:, cols], preferred_element_type=F32)
        own[:, cols] = (res[:, cols].astype(F32) + mixed).astype(BF)

    def piece(g, xs, cc, lo=0, n=PIECE):
        return midb.at[g, pl.ds(pl.multiple_of((2 * xs + cc) * PIECE + lo, PIECE // 2), n)]

    def pass_on(g, at, k, device, kr=None):
        go(send(at, at, g_s.at[k, g], g_r.at[k if kr is None else kr, g], device))

    def came(g, at, k):
        send(at, at, g_s.at[k, g], g_r.at[k, g], sib).wait_recv()

    def gather_own(g):
        src, dst = own.at[pl.ds(g * PIECE, PIECE)], piece(g, x, c)
        go(send(src, dst, g_s.at[0, g], g_r.at[0, g], right))
        go(send(src, dst, g_s.at[1, g], g_r.at[1, g], left))
        go(send(src, dst, g_s.at[4, g], g_r.at[4, g], sib))
        midb[g, pl.ds(pl.multiple_of(tp * PIECE, PIECE), PIECE), :] = own[g * PIECE:(g + 1) * PIECE, :]

    def gather_near(g):
        came(g, piece(g, xm, c), 0)
        pass_on(g, piece(g, xm, c, 0, PIECE // 2), 2, right)
        pass_on(g, piece(g, xm, c), 5, sib)
        came(g, piece(g, xp, c), 1)
        pass_on(g, piece(g, xp, c, PIECE // 2, PIECE // 2), 3, left)
        pass_on(g, piece(g, xp, c), 6, sib)

    def gather_far(g):
        for k in (0, 1):
            at = piece(g, x2, c, k * (PIECE // 2), PIECE // 2)
            came(g, at, 2 + k)
            pass_on(g, at, 7 + k, sib)

    def gather_rest(g):
        came(g, piece(g, x, 1 - c), 4)
        came(g, piece(g, xm, 1 - c), 5)
        came(g, piece(g, xp, 1 - c), 6)
        came(g, piece(g, x2, 1 - c, 0, PIECE // 2), 7)
        came(g, piece(g, x2, 1 - c, PIECE // 2, PIECE // 2), 8)

    def feed(g):
        wide = midb[g].astype(F32)
        inv = lax.rsqrt(jnp.mean(wide * wide, axis=-1, keepdims=True) + eps)
        normed[...] = (wide * inv * gain[0:1, :]).astype(BF)

        def lift(n, carry):
            cols = pl.ds(pl.multiple_of(n * 256, 256), 256)
            h = jnp.dot(normed[...], wu[:, cols], preferred_element_type=F32)
            hidden[:, cols] = jnp.square(jnp.maximum(h, 0.0)).astype(BF)
            return carry

        lax.fori_loop(0, 4, lift, 0)

        def drop(core):
            def one(k, carry):
                yy = 2 * core + k
                cols = pl.multiple_of(k * 128, 128)
                for zp in (0, 2):
                    rhs = jnp.concatenate([wd[yy, zp], wd[yy, zp + 1]], axis=1)
                    term = jnp.dot(hidden[...], rhs, preferred_element_type=F32).astype(BF)
                    part[g, core, zp, :, pl.ds(cols, 128)] = term[:, :128]
                    part[g, core, zp + 1, :, pl.ds(cols, 128)] = term[:, 128:]
                return carry

            lax.fori_loop(0, 2, one, 0)

        drop(1 - c)
        go(send(part.at[g, 1 - c], sibbuf.at[g], t_s.at[0, g], t_r.at[0, g], sib))
        drop(c)

    def both(g, rel, rows):
        xt = up(x, rel)
        return part[g, c, xt, rows, :].astype(F32) + sibbuf[g, xt, rows, :].astype(F32)

    def scatter_first(g):
        send(sibbuf.at[g], sibbuf.at[g], t_s.at[0, g], t_r.at[0, g], sib).wait_recv()
        stage[g, 2] = both(g, 2, pl.ds(0, ROWS)).astype(BF)
        go(send(stage.at[g, 2, A], hop_a.at[g], t_s.at[1, g], t_r.at[1, g], right))
        go(send(stage.at[g, 2, B], hop_b.at[g], t_s.at[2, g], t_r.at[2, g], left))
        stage[g, 1, B, :] = both(g, 1, B).astype(BF)
        go(send(stage.at[g, 1, B], from_l.at[g, B], t_s.at[3, g], t_r.at[3, g], right))
        stage[g, 3, A, :] = both(g, 3, A).astype(BF)
        go(send(stage.at[g, 3, A], from_r.at[g, A], t_s.at[4, g], t_r.at[4, g], left))

    def scatter_second(g):
        send(hop_a.at[g], hop_a.at[g], t_s.at[1, g], t_r.at[1, g], sib).wait_recv()
        stage[g, 1, A, :] = (both(g, 1, A) + hop_a[g].astype(F32)).astype(BF)
        go(send(stage.at[g, 1, A], from_l.at[g, A], t_s.at[5, g], t_r.at[5, g], right))
        send(hop_b.at[g], hop_b.at[g], t_s.at[2, g], t_r.at[2, g], sib).wait_recv()
        stage[g, 3, B, :] = (both(g, 3, B) + hop_b[g].astype(F32)).astype(BF)
        go(send(stage.at[g, 3, B], from_r.at[g, B], t_s.at[6, g], t_r.at[6, g], left))

    def scatter_third(g):
        for k, buf, rows in ((3, from_l, B), (4, from_r, A), (5, from_l, A), (6, from_r, B)):
            send(buf.at[g, rows], buf.at[g, rows], t_s.at[k, g], t_r.at[k, g], sib).wait_recv()
        for n in range(8):
            rows = pl.ds(n * PIECE, PIECE)
            total = both(g, 0, rows) + from_l[g, rows, :].astype(F32) + from_r[g, rows, :].astype(F32)
            mid = midb[g, rows, pl.ds(pl.multiple_of(tp * 256, 256), 256)].astype(F32)
            out[n * 128 + g * PIECE:n * 128 + (g + 1) * PIECE, :] = (mid + total).astype(BF)

    for g in range(G):
        gather_own(g)
    gather_near(0)
    gather_near(1)
    gather_far(0)
    gather_rest(0)
    for load in loads[1:]:
        load.wait()
    for k, at in ((0, wu_rows(up(z, 2), 0, 256)), (1, wu_rows(up(z, 2), 256, 256)),
                  (2, wd.at[up(y, 2), pl.ds(0, 2)]), (3, wd.at[up(y, 2), pl.ds(2, 2)])):
        send(at, at, o_s.at[k], o_r.at[k], sib).wait_recv()
    feed(0)
    gather_near(2)
    gather_far(1)
    gather_rest(1)
    scatter_first(0)
    feed(1)
    gather_near(3)
    gather_far(2)
    gather_rest(2)
    scatter_first(1)
    scatter_second(0)
    feed(2)
    gather_far(3)
    gather_rest(3)
    scatter_first(2)
    scatter_second(1)
    feed(3)
    scatter_second(2)
    scatter_first(3)
    scatter_third(0)
    scatter_third(1)
    scatter_second(3)
    scatter_third(2)
    scatter_third(3)
    for mine, remote in pending:
        @pl.when(jnp.logical_not(mine))
        def _():
            remote.wait_send()
    for copy in done:
        copy.wait_send()


def tail(att, wo, res, gain, ups, downs):
    return pl.pallas_call(
        tail_kernel,
        out_shape=sds((T, 256), BF),
        in_specs=[VM, HB, VM, VM] + [HB] * 6,
        out_specs=VM,
        scratch_shapes=[
            pltpu.VMEM((1024, 128), BF),
            pltpu.VMEM((1024, D), BF),
            pltpu.VMEM((128, D), BF),
            pltpu.VMEM((G, ROWS, D), BF),
            pltpu.VMEM((D, 1024), BF),
            pltpu.VMEM((4, 4, 1024, 128), BF),
            pltpu.VMEM((ROWS, D), BF),
            pltpu.VMEM((ROWS, 1024), BF),
            pltpu.VMEM((G, 2, 4, ROWS, 256), BF),
            pltpu.VMEM((G, 4, ROWS, 256), BF),
            pltpu.VMEM((G, 4, ROWS, 256), BF),
            pltpu.VMEM((G, ROWS // 2, 256), BF),
            pltpu.VMEM((G, ROWS // 2, 256), BF),
            pltpu.VMEM((G, ROWS, 256), BF),
            pltpu.VMEM((G, ROWS, 256), BF),
            DMA((7,)), DMA((16,)), DMA((16,)), DMA((4,)), DMA((4,)),
            DMA((9, G)), DMA((9, G)), DMA((7, G)), DMA((7, G)),
        ],
        compiler_params=pltpu.CompilerParams(
            has_side_effects=True, collective_id=1, vmem_limit_bytes=56 * 1024 * 1024
        ),
        cost_estimate=pl.CostEstimate(flops=20_000_000_000, bytes_accessed=8_000_000, transcendentals=0),
        name="tail",
    )(att, wo, res, gain, *ups, *downs)


def shifted(value, axis, step):
    def index(z, y):
        return (z % 4) * 4 + y % 4

    pairs = [
        (index(z, y), index(z + step, y) if axis == "z" else index(z, y + step)) for z in range(4) for y in range(4)
    ]
    return lax.ppermute(value, "sp", pairs)


def body(queries, keys, values, cum_gates, doc_ids, residual, w_out, norm_gain, w_up, w_down):
    qt, kv, gain8 = pack(queries, keys, values, jnp.transpose(cum_gates), doc_ids.reshape(1, T), norm_gain.reshape(1, 256))
    qin, kvall, woall, resin, gain, u0, d0 = exchange(qt, kv, w_out, residual, gain8, w_up, w_down)
    um, upl = shifted(u0, "z", 1), shifted(u0, "z", -1)
    dm, dpl = shifted(d0, "y", 1), shifted(d0, "y", -1)
    att = attend(qin, kvall)
    ups = [u.reshape(512, 1024) for u in (u0, um, upl)]
    return tail(att, woall, resin, gain, ups, (d0, dm, dpl))


def solution(mesh):
    in_specs = (
        P("sp", "tp"),
        P("sp", "tp"),
        P("sp", "tp"),
        P("sp", "tp"),
        P("sp"),
        P("sp", "tp"),
        P("tp", None),
        P("tp"),
        P("sp", "tp"),
        P("tp", "sp"),
    )
    return jax.shard_map(body, mesh=mesh, in_specs=in_specs, out_specs=P("sp", "tp"), check_vma=False)
```

```python
import functools

import jax
import jax.numpy as jnp
from jax import lax
from jax.experimental import pallas as pl
from jax.experimental.pallas import tpu as pltpu
from jax.sharding import PartitionSpec as P

D = 2048
HD = 64
T = 1024
HALF = 512
ITEM = 576
eps = 1e-06
far_below = -1e30
BIG = 8192.0
MESH = pl.DeviceIdType.MESH
BF = jnp.bfloat16
F32 = jnp.float32
VM = pl.BlockSpec(memory_space=pltpu.VMEM)
HB = pl.BlockSpec(memory_space=pl.ANY)
DMA = pltpu.SemaphoreType.DMA


def sds(shape, dtype):
    return jax.ShapeDtypeStruct(shape, dtype)


def place():
    sp, tp = lax.axis_index("sp"), lax.axis_index("tp")
    return lax.div(sp, 4), lax.rem(sp, 4), lax.div(tp, 2), lax.rem(tp, 2)


def dev(z, y, x, c):
    return (z * 4 + y, x * 2 + c)


def send(src, dst, ssem, rsem, device):
    return pltpu.make_async_remote_copy(
        src_ref=src, dst_ref=dst, send_sem=ssem, recv_sem=rsem, device_id=device, device_id_type=MESH
    )


def up(v, k):
    return lax.rem(v + k, 4)


def signal(barrier, device):
    pl.semaphore_signal(barrier, inc=1, device_id=device, device_id_type=MESH)


class Ring:
    def __init__(self, go, me, slot, right, left, s_r, s_l, r, sib=None, s_sib=None, r_sib=None):
        self.go, self.me, self.slot, self.right, self.left = go, me, slot, right, left
        self.s_r, self.s_l, self.r = s_r, s_l, r
        self.sib, self.s_sib, self.r_sib = sib, s_sib, r_sib

    def start(self, src, order=(0, 1)):
        for half in order:
            n, dst = 2 * self.me + half, self.slot(self.me, half)
            self.go(send(src(half), dst, self.s_r.at[n], self.r.at[n], self.right))
            self.go(send(src(half), dst, self.s_l.at[n], self.r.at[n], self.left))
            if self.s_sib is not None:
                self.go(send(src(half), dst, self.s_sib.at[n], self.r_sib.at[n], self.sib))

    def take(self, i, half, forward=0):
        n, at = 2 * i + half, self.slot(i, half)
        send(at, at, self.s_r.at[n], self.r.at[n], self.right).wait_recv()
        if forward > 0:
            self.go(send(at, at, self.s_r.at[n], self.r.at[n], self.right))
        if forward < 0:
            self.go(send(at, at, self.s_l.at[n], self.r.at[n], self.left))
        if self.s_sib is not None:
            self.go(send(at, at, self.s_sib.at[n], self.r_sib.at[n], self.sib))

    def middle(self, half):
        lo, hi = up(self.me, 3), up(self.me, 1)
        if half == 0:
            self.take(lo, 0, 1)
            self.take(hi, 0)
        else:
            self.take(hi, 1, -1)
            self.take(lo, 1)

    def last(self):
        self.take(up(self.me, 2), 0)
        self.take(up(self.me, 2), 1)


def pack_kernel(q_ref, k_ref, v_ref, g_ref, d_ref, n_ref, qt_ref, kv_ref, gain_ref):
    gain_ref[...] = jnp.broadcast_to(n_ref[...].astype(F32)[None], (8, 256))
    qt = (q_ref[...].astype(F32) * (HD ** -0.5)).T.astype(BF)
    qt_ref[0] = qt[:HD]
    qt_ref[1] = qt[HD:]
    k_lo, k_hi = k_ref[:HALF].astype(F32), k_ref[HALF:].astype(F32)
    first = lax.broadcasted_iota(jnp.int32, (HALF, 128), 1) < HD
    kv_ref[0, 0, :HALF] = jnp.where(first, k_lo, pltpu.roll(k_hi, HD, 1)).astype(BF)
    kv_ref[0, 1, :HALF] = jnp.where(first, pltpu.roll(k_lo, HD, 1), k_hi).astype(BF)
    vt = v_ref[...].astype(F32).T.astype(BF)
    row = lax.broadcasted_iota(jnp.int32, (8, T), 0)
    doc0 = 1.0 - d_ref[...].astype(F32)
    for j in range(2):
        kv_ref[0, j, HALF:] = jnp.zeros((64, 128), BF)
        g = g_ref[j:j + 1, :]
        hi = g.astype(BF).astype(F32)
        mid = (g - hi).astype(BF).astype(F32)
        lo = (g - hi) - mid
        aux = jnp.where(row == 0, hi, jnp.where(row == 1, mid, jnp.where(row == 2, lo, jnp.where(row == 3, doc0, 0.0))))
        for n in range(8):
            kv_ref[1, j, n * 64:(n + 1) * 64] = vt[j * HD:(j + 1) * HD, n * 128:(n + 1) * 128]
        for n in range(4):
            two = jnp.concatenate([aux[:, (2 * n) * 128:(2 * n + 1) * 128], aux[:, (2 * n + 1) * 128:(2 * n + 2) * 128]], axis=0)
            kv_ref[1, j, HALF + n * 16:HALF + (n + 1) * 16] = two.astype(BF)


def exchange_kernel(
    q_h, k_h, v_h, g_h, d_h, n_h, wo_h, res_h, wu_h, wd_h, qin, kvall, woall, resin, gainall, wu4, wd4,
    q_v, k_v, v_v, g_v, d_v, n_v, wo, res, wu, wd, qt, kv, gain, in_sem,
    qs, qr, ks, rr, s_sib, r_sib, s_r, s_l,
    wl, w_sib, wr_sib, w_s_r, w_s_l, w_r, es, er, gs, gr,
    u_s_r, u_s_l, u_r, d_s_r, d_s_l, d_r, ul,
):
    z, y, x, c = place()
    sp, tp = z * 4 + y, x * 2 + c
    sib = dev(z, y, x, 1 - c)
    yp, ym, y2 = up(y, 1), up(y, 3), up(y, 2)
    xp, xm, x2 = up(x, 1), up(x, 3), up(x, 2)

    loads = [
        pltpu.make_async_copy(src, dst, in_sem.at[n])
        for n, (src, dst) in enumerate(
            zip((k_h, v_h, g_h, d_h, n_h, q_h, wo_h, res_h, wu_h, wd_h), (k_v, v_v, g_v, d_v, n_v, q_v, wo, res, wu, wd))
        )
    ]
    for load in loads:
        load.start()
    barrier = pltpu.get_barrier_semaphore()
    cs = lax.div(z, 2)
    for zs in range(4):
        @pl.when(jnp.logical_not((z == zs) & (c == cs)))
        def _():
            signal(barrier, dev(zs, y, x, cs))

    for k in range(1, 8):
        signal(barrier, (sp, lax.rem(tp + k, 8)))
    signal(barrier, dev(z, yp, x, c))
    signal(barrier, dev(z, ym, x, c))
    zp, zm = up(z, 1), up(z, 3)
    signal(barrier, dev(zp, y, x, c))
    signal(barrier, dev(zm, y, x, c))
    for load in loads:
        load.wait()
    pack_kernel(q_v, k_v, v_v, g_v, d_v, n_v, qt, kv, gain)
    pl.semaphore_wait(barrier, jnp.where(c == cs, 14, 15))

    def guarded(is_self, local, remote):
        @pl.when(is_self)
        def _():
            local.start()

        @pl.when(jnp.logical_not(is_self))
        def _():
            remote.start()

    pending = []
    for j in range(2):
        zt = 2 * c + j
        for t in range(2):
            mine = (zt == z) & (c == t)
            src, dst = kv.at[t, j], kvall.at[t, sp]
            remote = send(src, dst, ks.at[2 * t + j], rr.at[sp], dev(zt, y, x, t))
            guarded(mine, pltpu.make_async_copy(src, dst, rr.at[sp]), remote)
            pending.append((mine, remote))
    for j in range(2):
        zt = 2 * c + j
        for hf in range(2):
            ct = lax.rem(hf + z, 2)
            mine = (zt == z) & (ct == c)
            src, dst = qt.at[j, :, pl.ds(hf * HALF, HALF)], qin.at[z]
            remote = send(src, dst, qs.at[2 * j + hf], qr.at[z], dev(zt, y, x, ct))
            guarded(mine, pltpu.make_async_copy(src, dst, qr.at[z]), remote)
            pending.append((mine, remote))

    done = []

    def wrows(xs, half):
        return pl.ds((2 * xs + c) * 128 + half * 64, 64)

    def go(copy):
        copy.start()
        done.append(copy)

    ring_w = Ring(go, x, lambda i, half: woall.at[wrows(i, half)], dev(z, y, xp, c), dev(z, y, xm, c),
                  w_s_r, w_s_l, w_r, sib, w_sib, wr_sib)
    ring_u = Ring(go, y, lambda i, half: wu4.at[i, pl.ds(half * 64, 64)], dev(z, yp, x, c), dev(z, ym, x, c),
                  u_s_r, u_s_l, u_r)
    ring_d = Ring(go, z, lambda i, half: wd4.at[i, pl.ds(half * HALF, HALF)], dev(zp, y, x, c), dev(zm, y, x, c),
                  d_s_r, d_s_l, d_r)
    own_w = [
        pltpu.make_async_copy(wo, woall.at[pl.ds(pl.multiple_of(tp * 128, 128), 128)], wl.at[0]),
        pltpu.make_async_copy(wu, wu4.at[y], ul.at[0]),
        pltpu.make_async_copy(wd, wd4.at[z], ul.at[1]),
    ]
    for loc in own_w:
        loc.start()
    ring_w.start(lambda half: wo.at[pl.ds(half * 64, 64)])

    own_e = pltpu.make_async_copy(res.at[pl.ds(pl.multiple_of(tp * 128, 128), 128)],
                                  resin.at[:, pl.ds(pl.multiple_of(tp * 256, 256), 256)], er.at[tp])
    own_e.start()
    own_g = pltpu.make_async_copy(gain, gainall.at[:, pl.ds(pl.multiple_of(tp * 256, 256), 256)], gr.at[tp])
    own_g.start()
    for k in range(1, 8):
        to = lax.rem(tp + k, 8)
        cols = pl.ds(pl.multiple_of(tp * 256, 256), 256)
        go(send(res.at[pl.ds(pl.multiple_of(to * 128, 128), 128)], resin.at[:, cols], es.at[k], er.at[tp], (sp, to)))
        go(send(gain, gainall.at[:, cols], gs.at[k], gr.at[tp], (sp, to)))

    def arrived(b):
        send(kvall.at[c, b], kvall.at[c, b], s_sib.at[b], rr.at[b], sib).wait_recv()
        go(send(kvall.at[c, b], kvall.at[c, b], s_sib.at[b], r_sib.at[b], sib))

    def right(b):
        go(send(kvall.at[c, b], kvall.at[c, b], s_r.at[b], rr.at[b], dev(z, yp, x, c)))

    def left(b):
        go(send(kvall.at[c, b], kvall.at[c, b], s_l.at[b], rr.at[b], dev(z, ym, x, c)))

    zs = [z, up(z, 1), up(z, 3), up(z, 2)]

    def near(r):
        b = zs[r] * 4 + y
        arrived(b)
        right(b)
        left(b)

    def next_to(r):
        b = zs[r] * 4 + ym
        arrived(b)
        if r in (0, 2):
            right(b)
        b = zs[r] * 4 + yp
        arrived(b)
        if r in (1, 3):
            left(b)

    near(0)
    ring_d.start(lambda half: wd.at[pl.ds(half * HALF, HALF)])
    ring_u.start(lambda half: wu.at[pl.ds(half * 64, 64)])
    near(1)
    near(2)
    next_to(0)
    ring_w.middle(0)
    near(3)
    ring_u.middle(0)
    ring_d.middle(0)
    next_to(1)
    next_to(2)
    ring_w.middle(1)
    ring_u.middle(1)
    ring_d.middle(1)
    next_to(3)
    for r in range(4):
        arrived(zs[r] * 4 + y2)
    ring_w.last()
    ring_u.last()
    ring_d.last()

    for b in range(16):
        send(kvall.at[1 - c, b], kvall.at[1 - c, b], s_sib.at[b], r_sib.at[b], sib).wait_recv()
    for n in range(8):
        rows = pl.ds((2 * (n // 2) + (1 - c)) * 128 + (n % 2) * 64, 64)
        send(woall.at[rows], woall.at[rows], w_sib.at[n], wr_sib.at[n], sib).wait_recv()
    for i in range(4):
        send(qin.at[i], qin.at[i], qs.at[0], qr.at[i], sib).wait_recv()
    for n in range(8):
        cols = pl.ds(n * 256, 256)
        send(resin.at[:, cols], resin.at[:, cols], es.at[0], er.at[n], sib).wait_recv()
        send(gainall.at[:, cols], gainall.at[:, cols], gs.at[0], gr.at[n], sib).wait_recv()
    for loc in own_w:
        loc.wait()
    for mine, remote in pending:
        @pl.when(jnp.logical_not(mine))
        def _():
            remote.wait_send()
    for copy in done:
        copy.wait_send()


def exchange(*args):
    return pl.pallas_call(
        exchange_kernel,
        out_shape=(
            sds((4, HD, HALF), BF),
            sds((2, 16, ITEM, 128), BF),
            sds((1024, D), BF),
            sds((128, D), BF),
            sds((8, D), F32),
            sds((4, 128, 1024), BF),
            sds((4, T, 128), BF),
        ),
        in_specs=[HB] * 10,
        out_specs=(HB,) * 7,
        scratch_shapes=[
            pltpu.VMEM((T, 128), BF),
            pltpu.VMEM((T, 128), BF),
            pltpu.VMEM((T, 128), BF),
            pltpu.VMEM((2, T), F32),
            pltpu.VMEM((1, T), jnp.int32),
            pltpu.VMEM((256,), BF),
            pltpu.VMEM((128, D), BF),
            pltpu.VMEM((T, 256), BF),
            pltpu.VMEM((128, 1024), BF),
            pltpu.VMEM((1024, 128), BF),
            pltpu.VMEM((2, HD, T), BF),
            pltpu.VMEM((2, 2, ITEM, 128), BF),
            pltpu.VMEM((8, 256), F32),
            DMA((10,)),
            DMA((4,)), DMA((4,)), DMA((4,)), DMA((16,)), DMA((16,)), DMA((16,)), DMA((16,)), DMA((16,)),
            DMA((2,)), DMA((8,)), DMA((8,)), DMA((8,)), DMA((8,)), DMA((8,)),
            DMA((8,)), DMA((8,)), DMA((8,)), DMA((8,)),
            DMA((8,)), DMA((8,)), DMA((8,)), DMA((8,)), DMA((8,)), DMA((8,)), DMA((2,)),
        ],
        compiler_params=pltpu.CompilerParams(has_side_effects=True, collective_id=0),
        cost_estimate=pl.CostEstimate(flops=20_000_000_000, bytes_accessed=16_000_000, transcendentals=0),
        name="exchange",
    )(*args)


QW = 256
NS = HALF // QW


def attend_kernel(q_h, kv_h, o_ref, q_ref, kv_ref, aux_ref, in_sem, pieces, gmat, w_ref, *scr):
    z, y, x, c = place()
    main = pl.ds(0, HALF)
    loads = [
        pltpu.make_async_copy(kv_h.at[1, :, pl.ds(HALF, 64)], aux_ref, in_sem.at[0]),
        pltpu.make_async_copy(q_h, q_ref, in_sem.at[1]),
        pltpu.make_async_copy(kv_h.at[0, :, main], kv_ref.at[0], in_sem.at[2]),
        pltpu.make_async_copy(kv_h.at[1, :, main], kv_ref.at[1], in_sem.at[3]),
    ]
    for load in loads:
        load.start()
    loads[0].wait()
    s_refs, accs, tops, shrinks = scr[:NS], scr[NS:2 * NS], scr[2 * NS:3 * NS], scr[3 * NS:]
    ones = jnp.ones((16, HALF), BF)
    count = jnp.zeros((1, 128), F32)
    for b in range(16):
        for n in range(8):
            a = aux_ref[b, n * 8:(n + 1) * 8, :].astype(F32)
            count = count + a[3:4]
            hf, at = n // 4, (n % 4) * 128
            pieces[b * 8 + hf * 4:b * 8 + hf * 4 + 4, at:at + 128] = a[:4]
    docs0 = jnp.sum(count).astype(jnp.int32)
    gmat[...] = pieces[...].T.astype(BF)
    for load in loads[1:]:
        load.wait()
    row = lax.broadcasted_iota(jnp.int32, (128, QW), 0)
    unit_of_row, piece_of_row = row // 4, row % 4

    def tile(i, carry):
        hq = 2 * (4 * i + y) + lax.rem(c + i, 2)
        start = jnp.where(hq * HALF >= docs0, lax.div(docs0, HALF), 0)
        q_pos = hq * HALF + lax.broadcasted_iota(jnp.int32, (1, HALF), 1)
        doc1 = jnp.where(q_pos >= docs0, -BIG, 0.0)
        for k in range(NS):
            cols = slice(k * QW, (k + 1) * QW)
            w_ref[:, cols] = jnp.where(piece_of_row == 3, doc1[:, cols], -1.0)

        def scores(k, u, first):
            cols = slice(k * QW, (k + 1) * QW)
            q = q_ref[i, :, cols]
            none = jnp.zeros_like(q)
            b, low = lax.div(u, 2), lax.rem(u, 2) == 0
            lhs = jnp.concatenate([kv_ref[0, b], gmat[...]], axis=1)
            sel = jnp.where(unit_of_row == u, w_ref[:, cols], 0.0).astype(BF)
            rhs = jnp.concatenate([jnp.where(low, q, none), jnp.where(low, none, q), sel], axis=0)
            s = jnp.dot(lhs, rhs, preferred_element_type=F32)
            if first:
                key = lax.broadcasted_iota(jnp.int32, (HALF, QW), 0)
                s = jnp.where(key <= k * QW + lax.broadcasted_iota(jnp.int32, (HALF, QW), 1), s, far_below)
            s_refs[k][...] = s
            new = jnp.max(s, axis=0, keepdims=True)
            if not first:
                old = tops[k][...]
                new = jnp.maximum(old, new)
                shrinks[k][...] = jnp.exp(old - new)
            tops[k][...] = new

        def weigh(k, u, first):
            b, hf = lax.div(u, 2), lax.rem(u, 2)
            p = jnp.exp(s_refs[k][...] - tops[k][...]).astype(BF)
            vt = jnp.concatenate(
                [kv_ref[1, b, pl.ds(pl.multiple_of(hf * 256 + n * 64, 64), 64), :] for n in range(4)], axis=1
            )
            vt = jnp.concatenate([vt, ones], axis=0)
            product = jnp.dot(vt, p, preferred_element_type=F32)
            accs[k][...] = product if first else accs[k][...] * shrinks[k][...] + product

        ahead = jnp.maximum(hq - 1, 0)
        scores(0, hq, True)
        scores(1, hq, True)
        weigh(0, hq, True)
        scores(0, jnp.minimum(start, ahead), False)
        weigh(1, hq, True)

        def step(u, carry):
            scores(1, u, False)
            weigh(0, u, False)
            scores(0, jnp.minimum(u + 1, ahead), False)
            weigh(1, u, False)
            return carry

        lax.fori_loop(start, hq, step, 0)
        for k in range(NS):
            total = accs[k][...]
            o_ref[i, :, k * QW:(k + 1) * QW] = (total[:HD] / total[HD:HD + 1]).astype(BF)
        return carry

    lax.fori_loop(0, 4, tile, 0)


def attend(q, kv):
    return pl.pallas_call(
        attend_kernel,
        out_shape=sds((4, HD, HALF), BF),
        in_specs=[HB, HB],
        out_specs=VM,
        scratch_shapes=[
            pltpu.VMEM((4, HD, HALF), BF),
            pltpu.VMEM((2, 16, HALF, 128), BF),
            pltpu.VMEM((16, 64, 128), BF),
            DMA((4,)),
            pltpu.VMEM((128, HALF), F32),
            pltpu.VMEM((HALF, 128), BF),
            pltpu.VMEM((128, HALF), F32),
        ]
        + [pltpu.VMEM((HALF, QW), F32)] * NS
        + [pltpu.VMEM((80, QW), F32)] * NS
        + [pltpu.VMEM((1, QW), F32)] * (2 * NS),
        compiler_params=pltpu.CompilerParams(vmem_limit_bytes=66_500_000),
        cost_estimate=pl.CostEstimate(flops=20_000_000_000, bytes_accessed=8_000_000, transcendentals=0),
        name="attend",
    )(q, kv)


G = 4
ROWS = T // G
PIECE = 128 // G
A, B = pl.ds(0, ROWS // 2), pl.ds(ROWS // 2, ROWS // 2)


def tail_kernel(
    att, wo_any, res, gain, u0, um, upl, d0, dm, dpl, out,
    a_in, wo, own, midb, wu, wd, normed, hidden, part, sibbuf, stage, hop_a, hop_b, from_l, from_r,
    w_sem, a_s, a_r, o_s, o_r, g_s, g_r, t_s, t_r,
):
    z, y, x, c = place()
    sp, tp = z * 4 + y, x * 2 + c
    sib = dev(z, y, x, 1 - c)
    xp, xm, x2 = up(x, 1), up(x, 3), up(x, 2)
    right, left = dev(z, y, xp, c), dev(z, y, xm, c)
    z_next, z_prev, y_next, y_prev = up(z, 1), up(z, 3), up(y, 1), up(y, 3)
    head = 4 * x + z

    barrier = pltpu.get_barrier_semaphore()
    cs = lax.rem(lax.div(tp, 4) + z, 2)
    for zs in range(4):
        for xs in range(4):
            @pl.when(jnp.logical_not((z == zs) & (x == xs) & (c == cs)))
            def _():
                signal(barrier, dev(zs, y, xs, cs))

    to_z = dev(z_next, y, x, c), dev(z_prev, y, x, c)
    to_y = dev(z, y_next, x, c), dev(z, y_prev, x, c)
    for device in (sib, right, left, *to_z, *to_y):
        signal(barrier, device)
    pl.semaphore_wait(barrier, jnp.where(lax.div(x, 2) == lax.rem(c + z, 2), 22, 23))

    done = []

    def go(copy):
        copy.start()
        done.append(copy)

    pending = []
    for i in range(4):
        hf = lax.rem(c + i, 2)
        for k in range(4):
            to = 4 * hf + k
            mine = (z == i) & (to == tp)
            src = att.at[i, :, pl.ds(k * 128, 128)]
            dst = a_in.at[pl.ds(pl.multiple_of(head * HD, HD), HD)]
            local = pltpu.make_async_copy(src, dst, a_r.at[head])
            remote = send(src, dst, a_s.at[4 * i + k], a_r.at[head], (i * 4 + y, to))

            @pl.when(mine)
            def _():
                local.start()

            @pl.when(jnp.logical_not(mine))
            def _():
                remote.start()

            pending.append((mine, remote))

    def wu_rows(zz, lo, n):
        return wu.at[pl.ds(pl.multiple_of(zz * 512 + lo, 256), n)]

    loads = [
        pltpu.make_async_copy(wo_any, wo, w_sem.at[0]),
        pltpu.make_async_copy(u0, wu_rows(z, 0, 512), w_sem.at[1]),
        pltpu.make_async_copy(um, wu_rows(z_prev, 0, 512), w_sem.at[2]),
        pltpu.make_async_copy(upl, wu_rows(z_next, 0, 512), w_sem.at[3]),
        pltpu.make_async_copy(d0, wd.at[y], w_sem.at[4]),
        pltpu.make_async_copy(dm, wd.at[y_prev], w_sem.at[5]),
        pltpu.make_async_copy(dpl, wd.at[y_next], w_sem.at[6]),
    ]
    for load in loads:
        load.start()
    go(send(um.at[pl.ds(0, 256)], wu_rows(z_prev, 0, 256), o_s.at[0], o_r.at[0], to_z[0]))
    go(send(upl.at[pl.ds(256, 256)], wu_rows(z_next, 256, 256), o_s.at[1], o_r.at[1], to_z[1]))
    go(send(dm.at[pl.ds(0, 2)], wd.at[y_prev, pl.ds(0, 2)], o_s.at[2], o_r.at[2], to_y[0]))
    go(send(dpl.at[pl.ds(2, 2)], wd.at[y_next, pl.ds(2, 2)], o_s.at[3], o_r.at[3], to_y[1]))

    for h in range(16):
        rows = pl.ds(h * HD, HD)
        send(a_in.at[rows], a_in.at[rows], a_s.at[0], a_r.at[h], sib).wait_recv()
    loads[0].wait()
    a = a_in[...].astype(F32).T.astype(BF)
    for n in range(4):
        cols = slice(n * 512, (n + 1) * 512)
        mixed = jnp.dot(a, wo[:, cols], preferred_element_type=F32)
        own[:, cols] = (res[:, cols].astype(F32) + mixed).astype(BF)

    def piece(g, xs, cc, lo=0, n=PIECE):
        return midb.at[g, pl.ds(pl.multiple_of((2 * xs + cc) * PIECE + lo, PIECE // 2), n)]

    def pass_on(g, at, k, device, kr=None):
        go(send(at, at, g_s.at[k, g], g_r.at[k if kr is None else kr, g], device))

    def came(g, at, k):
        send(at, at, g_s.at[k, g], g_r.at[k, g], sib).wait_recv()

    def gather_own(g):
        src, dst = own.at[pl.ds(g * PIECE, PIECE)], piece(g, x, c)
        go(send(src, dst, g_s.at[0, g], g_r.at[0, g], right))
        go(send(src, dst, g_s.at[1, g], g_r.at[1, g], left))
        go(send(src, dst, g_s.at[4, g], g_r.at[4, g], sib))
        midb[g, pl.ds(pl.multiple_of(tp * PIECE, PIECE), PIECE), :] = own[g * PIECE:(g + 1) * PIECE, :]

    def gather_near(g):
        came(g, piece(g, xm, c), 0)
        pass_on(g, piece(g, xm, c, 0, PIECE // 2), 2, right)
        pass_on(g, piece(g, xm, c), 5, sib)
        came(g, piece(g, xp, c), 1)
        pass_on(g, piece(g, xp, c, PIECE // 2, PIECE // 2), 3, left)
        pass_on(g, piece(g, xp, c), 6, sib)

    def gather_far(g):
        for k in (0, 1):
            at = piece(g, x2, c, k * (PIECE // 2), PIECE // 2)
            came(g, at, 2 + k)
            pass_on(g, at, 7 + k, sib)

    def gather_rest(g):
        came(g, piece(g, x, 1 - c), 4)
        came(g, piece(g, xm, 1 - c), 5)
        came(g, piece(g, xp, 1 - c), 6)
        came(g, piece(g, x2, 1 - c, 0, PIECE // 2), 7)
        came(g, piece(g, x2, 1 - c, PIECE // 2, PIECE // 2), 8)

    def feed(g):
        wide = midb[g].astype(F32)
        inv = lax.rsqrt(jnp.mean(wide * wide, axis=-1, keepdims=True) + eps)
        normed[...] = (wide * inv * gain[0:1, :]).astype(BF)

        def lift(n, carry):
            cols = pl.ds(pl.multiple_of(n * 256, 256), 256)
            h = jnp.dot(normed[...], wu[:, cols], preferred_element_type=F32)
            hidden[:, cols] = jnp.square(jnp.maximum(h, 0.0)).astype(BF)
            return carry

        lax.fori_loop(0, 4, lift, 0)

        def drop(core):
            def one(k, carry):
                yy = 2 * core + k
                cols = pl.multiple_of(k * 128, 128)
                for zp in (0, 2):
                    rhs = jnp.concatenate([wd[yy, zp], wd[yy, zp + 1]], axis=1)
                    term = jnp.dot(hidden[...], rhs, preferred_element_type=F32).astype(BF)
                    part[g, core, zp, :, pl.ds(cols, 128)] = term[:, :128]
                    part[g, core, zp + 1, :, pl.ds(cols, 128)] = term[:, 128:]
                return carry

            lax.fori_loop(0, 2, one, 0)

        drop(1 - c)
        go(send(part.at[g, 1 - c], sibbuf.at[g], t_s.at[0, g], t_r.at[0, g], sib))
        drop(c)

    def both(g, rel, rows):
        xt = up(x, rel)
        return part[g, c, xt, rows, :].astype(F32) + sibbuf[g, xt, rows, :].astype(F32)

    def scatter_first(g):
        send(sibbuf.at[g], sibbuf.at[g], t_s.at[0, g], t_r.at[0, g], sib).wait_recv()
        stage[g, 2] = both(g, 2, pl.ds(0, ROWS)).astype(BF)
        go(send(stage.at[g, 2, A], hop_a.at[g], t_s.at[1, g], t_r.at[1, g], right))
        go(send(stage.at[g, 2, B], hop_b.at[g], t_s.at[2, g], t_r.at[2, g], left))
        stage[g, 1, B, :] = both(g, 1, B).astype(BF)
        go(send(stage.at[g, 1, B], from_l.at[g, B], t_s.at[3, g], t_r.at[3, g], right))
        stage[g, 3, A, :] = both(g, 3, A).astype(BF)
        go(send(stage.at[g, 3, A], from_r.at[g, A], t_s.at[4, g], t_r.at[4, g], left))

    def scatter_second(g):
        send(hop_a.at[g], hop_a.at[g], t_s.at[1, g], t_r.at[1, g], sib).wait_recv()
        stage[g, 1, A, :] = (both(g, 1, A) + hop_a[g].astype(F32)).astype(BF)
        go(send(stage.at[g, 1, A], from_l.at[g, A], t_s.at[5, g], t_r.at[5, g], right))
        send(hop_b.at[g], hop_b.at[g], t_s.at[2, g], t_r.at[2, g], sib).wait_recv()
        stage[g, 3, B, :] = (both(g, 3, B) + hop_b[g].astype(F32)).astype(BF)
        go(send(stage.at[g, 3, B], from_r.at[g, B], t_s.at[6, g], t_r.at[6, g], left))

    def scatter_third(g):
        for k, buf, rows in ((3, from_l, B), (4, from_r, A), (5, from_l, A), (6, from_r, B)):
            send(buf.at[g, rows], buf.at[g, rows], t_s.at[k, g], t_r.at[k, g], sib).wait_recv()
        for n in range(8):
            rows = pl.ds(n * PIECE, PIECE)
            total = both(g, 0, rows) + from_l[g, rows, :].astype(F32) + from_r[g, rows, :].astype(F32)
            mid = midb[g, rows, pl.ds(pl.multiple_of(tp * 256, 256), 256)].astype(F32)
            out[n * 128 + g * PIECE:n * 128 + (g + 1) * PIECE, :] = (mid + total).astype(BF)

    for g in range(G):
        gather_own(g)
    gather_near(0)
    gather_near(1)
    gather_far(0)
    gather_rest(0)
    gather_near(2)
    gather_far(1)
    for load in loads[1:]:
        load.wait()
    for k, at in ((0, wu_rows(up(z, 2), 0, 256)), (1, wu_rows(up(z, 2), 256, 256)),
                  (2, wd.at[up(y, 2), pl.ds(0, 2)]), (3, wd.at[up(y, 2), pl.ds(2, 2)])):
        send(at, at, o_s.at[k], o_r.at[k], sib).wait_recv()
    feed(0)
    gather_near(3)
    gather_rest(1)
    scatter_first(0)
    feed(1)
    gather_far(2)
    gather_rest(2)
    scatter_first(1)
    scatter_second(0)
    feed(2)
    gather_far(3)
    gather_rest(3)
    scatter_first(2)
    scatter_second(1)
    feed(3)
    scatter_second(2)
    scatter_first(3)
    scatter_third(0)
    scatter_third(1)
    scatter_second(3)
    scatter_third(2)
    scatter_third(3)
    for mine, remote in pending:
        @pl.when(jnp.logical_not(mine))
        def _():
            remote.wait_send()
    for copy in done:
        copy.wait_send()


def tail(att, wo, res, gain, ups, downs):
    return pl.pallas_call(
        tail_kernel,
        out_shape=sds((T, 256), BF),
        in_specs=[VM, HB, VM, VM] + [HB] * 6,
        out_specs=VM,
        scratch_shapes=[
            pltpu.VMEM((1024, 128), BF),
            pltpu.VMEM((1024, D), BF),
            pltpu.VMEM((128, D), BF),
            pltpu.VMEM((G, ROWS, D), BF),
            pltpu.VMEM((D, 1024), BF),
            pltpu.VMEM((4, 4, 1024, 128), BF),
            pltpu.VMEM((ROWS, D), BF),
            pltpu.VMEM((ROWS, 1024), BF),
            pltpu.VMEM((G, 2, 4, ROWS, 256), BF),
            pltpu.VMEM((G, 4, ROWS, 256), BF),
            pltpu.VMEM((G, 4, ROWS, 256), BF),
            pltpu.VMEM((G, ROWS // 2, 256), BF),
            pltpu.VMEM((G, ROWS // 2, 256), BF),
            pltpu.VMEM((G, ROWS, 256), BF),
            pltpu.VMEM((G, ROWS, 256), BF),
            DMA((7,)), DMA((16,)), DMA((16,)), DMA((4,)), DMA((4,)),
            DMA((9, G)), DMA((9, G)), DMA((7, G)), DMA((7, G)),
        ],
        compiler_params=pltpu.CompilerParams(
            has_side_effects=True, collective_id=1, vmem_limit_bytes=56 * 1024 * 1024
        ),
        cost_estimate=pl.CostEstimate(flops=20_000_000_000, bytes_accessed=8_000_000, transcendentals=0),
        name="tail",
    )(att, wo, res, gain, *ups, *downs)


def shifted(value, axis, step):
    def index(z, y):
        return (z % 4) * 4 + y % 4

    pairs = [
        (index(z, y), index(z + step, y) if axis == "z" else index(z, y + step)) for z in range(4) for y in range(4)
    ]
    return lax.ppermute(value, "sp", pairs)


def body(queries, keys, values, cum_gates, doc_ids, residual, w_out, norm_gain, w_up, w_down):
    qin, kvall, woall, resin, gain, u0, d0 = exchange(
        queries, keys, values, jnp.transpose(cum_gates), doc_ids.reshape(1, T), norm_gain, w_out, residual, w_up, w_down
    )
    um, upl = shifted(u0, "z", 1), shifted(u0, "z", -1)
    dm, dpl = shifted(d0, "y", 1), shifted(d0, "y", -1)
    att = attend(qin, kvall)
    ups = [u.reshape(512, 1024) for u in (u0, um, upl)]
    return tail(att, woall, resin, gain, ups, (d0, dm, dpl))


def solution(mesh):
    in_specs = (
        P("sp", "tp"),
        P("sp", "tp"),
        P("sp", "tp"),
        P("sp", "tp"),
        P("sp"),
        P("sp", "tp"),
        P("tp", None),
        P("tp"),
        P("sp", "tp"),
        P("tp", "sp"),
    )
    return jax.shard_map(body, mesh=mesh, in_specs=in_specs, out_specs=P("sp", "tp"), check_vma=False)
```

```python
import functools

import jax
import jax.numpy as jnp
from jax import lax
from jax.experimental import pallas as pl
from jax.experimental.pallas import tpu as pltpu
from jax.sharding import PartitionSpec as P

D = 2048
HD = 64
T = 1024
HALF = 512
ITEM = 576
eps = 1e-06
far_below = -1e30
BIG = 8192.0
MESH = pl.DeviceIdType.MESH
BF = jnp.bfloat16
F32 = jnp.float32
VM = pl.BlockSpec(memory_space=pltpu.VMEM)
HB = pl.BlockSpec(memory_space=pl.ANY)
DMA = pltpu.SemaphoreType.DMA


def sds(shape, dtype):
    return jax.ShapeDtypeStruct(shape, dtype)


def place():
    sp, tp = lax.axis_index("sp"), lax.axis_index("tp")
    return lax.div(sp, 4), lax.rem(sp, 4), lax.div(tp, 2), lax.rem(tp, 2)


def dev(z, y, x, c):
    return (z * 4 + y, x * 2 + c)


def send(src, dst, ssem, rsem, device):
    return pltpu.make_async_remote_copy(
        src_ref=src, dst_ref=dst, send_sem=ssem, recv_sem=rsem, device_id=device, device_id_type=MESH
    )


def up(v, k):
    return lax.rem(v + k, 4)


def signal(barrier, device):
    pl.semaphore_signal(barrier, inc=1, device_id=device, device_id_type=MESH)


class Ring:
    def __init__(self, go, me, slot, right, left, s_r, s_l, r, sib=None, s_sib=None, r_sib=None):
        self.go, self.me, self.slot, self.right, self.left = go, me, slot, right, left
        self.s_r, self.s_l, self.r = s_r, s_l, r
        self.sib, self.s_sib, self.r_sib = sib, s_sib, r_sib

    def start(self, src, order=(0, 1)):
        for half in order:
            n, dst = 2 * self.me + half, self.slot(self.me, half)
            self.go(send(src(half), dst, self.s_r.at[n], self.r.at[n], self.right))
            self.go(send(src(half), dst, self.s_l.at[n], self.r.at[n], self.left))
            if self.s_sib is not None:
                self.go(send(src(half), dst, self.s_sib.at[n], self.r_sib.at[n], self.sib))

    def take(self, i, half, forward=0):
        n, at = 2 * i + half, self.slot(i, half)
        send(at, at, self.s_r.at[n], self.r.at[n], self.right).wait_recv()
        if forward > 0:
            self.go(send(at, at, self.s_r.at[n], self.r.at[n], self.right))
        if forward < 0:
            self.go(send(at, at, self.s_l.at[n], self.r.at[n], self.left))
        if self.s_sib is not None:
            self.go(send(at, at, self.s_sib.at[n], self.r_sib.at[n], self.sib))

    def middle(self, half):
        lo, hi = up(self.me, 3), up(self.me, 1)
        if half == 0:
            self.take(lo, 0, 1)
            self.take(hi, 0)
        else:
            self.take(hi, 1, -1)
            self.take(lo, 1)

    def last(self):
        self.take(up(self.me, 2), 0)
        self.take(up(self.me, 2), 1)


def pack_kernel(q_ref, k_ref, v_ref, g_ref, d_ref, n_ref, qt_ref, kv_ref, gain_ref):
    gain_ref[...] = jnp.broadcast_to(n_ref[...].astype(F32)[None], (8, 256))
    qt = (q_ref[...].astype(F32) * (HD ** -0.5)).T.astype(BF)
    qt_ref[0] = qt[:HD]
    qt_ref[1] = qt[HD:]
    k_lo, k_hi = k_ref[:HALF].astype(F32), k_ref[HALF:].astype(F32)
    first = lax.broadcasted_iota(jnp.int32, (HALF, 128), 1) < HD
    kv_ref[0, 0, :HALF] = jnp.where(first, k_lo, pltpu.roll(k_hi, HD, 1)).astype(BF)
    kv_ref[0, 1, :HALF] = jnp.where(first, pltpu.roll(k_lo, HD, 1), k_hi).astype(BF)
    vt = v_ref[...].astype(F32).T.astype(BF)
    row = lax.broadcasted_iota(jnp.int32, (8, T), 0)
    doc0 = 1.0 - d_ref[...].astype(F32)
    for j in range(2):
        kv_ref[0, j, HALF:] = jnp.zeros((64, 128), BF)
        g = g_ref[j:j + 1, :]
        hi = g.astype(BF).astype(F32)
        mid = (g - hi).astype(BF).astype(F32)
        lo = (g - hi) - mid
        aux = jnp.where(row == 0, hi, jnp.where(row == 1, mid, jnp.where(row == 2, lo, jnp.where(row == 3, doc0, 0.0))))
        for n in range(8):
            kv_ref[1, j, n * 64:(n + 1) * 64] = vt[j * HD:(j + 1) * HD, n * 128:(n + 1) * 128]
        for n in range(4):
            two = jnp.concatenate([aux[:, (2 * n) * 128:(2 * n + 1) * 128], aux[:, (2 * n + 1) * 128:(2 * n + 2) * 128]], axis=0)
            kv_ref[1, j, HALF + n * 16:HALF + (n + 1) * 16] = two.astype(BF)


def exchange_kernel(
    q_h, k_h, v_h, g_h, d_h, n_h, wo_h, res_h, wu_h, wd_h, qin, kvall, woall, resin, gainall, wu4, wd4,
    q_v, k_v, v_v, g_v, d_v, n_v, wo, res, wu, wd, qt, kv, gain, in_sem,
    qs, qr, ks, rr, s_sib, r_sib, s_r, s_l,
    wl, w_sib, wr_sib, w_s_r, w_s_l, w_r, es, er, gs, gr,
    u_s_r, u_s_l, u_r, d_s_r, d_s_l, d_r, ul,
):
    z, y, x, c = place()
    sp, tp = z * 4 + y, x * 2 + c
    sib = dev(z, y, x, 1 - c)
    yp, ym, y2 = up(y, 1), up(y, 3), up(y, 2)
    xp, xm, x2 = up(x, 1), up(x, 3), up(x, 2)

    loads = [
        pltpu.make_async_copy(src, dst, in_sem.at[n])
        for n, (src, dst) in enumerate(
            zip((k_h, v_h, g_h, d_h, n_h, q_h, wo_h, res_h, wu_h, wd_h), (k_v, v_v, g_v, d_v, n_v, q_v, wo, res, wu, wd))
        )
    ]
    for load in loads:
        load.start()
    barrier = pltpu.get_barrier_semaphore()
    cs = lax.div(z, 2)
    for zs in range(4):
        @pl.when(jnp.logical_not((z == zs) & (c == cs)))
        def _():
            signal(barrier, dev(zs, y, x, cs))

    for k in range(1, 8):
        signal(barrier, (sp, lax.rem(tp + k, 8)))
    signal(barrier, dev(z, yp, x, c))
    signal(barrier, dev(z, ym, x, c))
    zp, zm = up(z, 1), up(z, 3)
    signal(barrier, dev(zp, y, x, c))
    signal(barrier, dev(zm, y, x, c))
    for load in loads:
        load.wait()
    pack_kernel(q_v, k_v, v_v, g_v, d_v, n_v, qt, kv, gain)
    pl.semaphore_wait(barrier, jnp.where(c == cs, 14, 15))

    def guarded(is_self, local, remote):
        @pl.when(is_self)
        def _():
            local.start()

        @pl.when(jnp.logical_not(is_self))
        def _():
            remote.start()

    pending = []
    for j in range(2):
        zt = 2 * c + j
        for t in range(2):
            mine = (zt == z) & (c == t)
            src, dst = kv.at[t, j], kvall.at[t, sp]
            remote = send(src, dst, ks.at[2 * t + j], rr.at[sp], dev(zt, y, x, t))
            guarded(mine, pltpu.make_async_copy(src, dst, rr.at[sp]), remote)
            pending.append((mine, remote))
    for j in range(2):
        zt = 2 * c + j
        for hf in range(2):
            ct = lax.rem(hf + z, 2)
            mine = (zt == z) & (ct == c)
            src, dst = qt.at[j, :, pl.ds(hf * HALF, HALF)], qin.at[z]
            remote = send(src, dst, qs.at[2 * j + hf], qr.at[z], dev(zt, y, x, ct))
            guarded(mine, pltpu.make_async_copy(src, dst, qr.at[z]), remote)
            pending.append((mine, remote))

    done = []

    def wrows(xs, half):
        return pl.ds((2 * xs + c) * 128 + half * 64, 64)

    def go(copy):
        copy.start()
        done.append(copy)

    ring_w = Ring(go, x, lambda i, half: woall.at[wrows(i, half)], dev(z, y, xp, c), dev(z, y, xm, c),
                  w_s_r, w_s_l, w_r, sib, w_sib, wr_sib)
    ring_u = Ring(go, y, lambda i, half: wu4.at[i, pl.ds(half * 64, 64)], dev(z, yp, x, c), dev(z, ym, x, c),
                  u_s_r, u_s_l, u_r)
    ring_d = Ring(go, z, lambda i, half: wd4.at[i, pl.ds(half * HALF, HALF)], dev(zp, y, x, c), dev(zm, y, x, c),
                  d_s_r, d_s_l, d_r)
    own_w = [
        pltpu.make_async_copy(wo, woall.at[pl.ds(pl.multiple_of(tp * 128, 128), 128)], wl.at[0]),
        pltpu.make_async_copy(wu, wu4.at[y], ul.at[0]),
        pltpu.make_async_copy(wd, wd4.at[z], ul.at[1]),
    ]
    for loc in own_w:
        loc.start()
    ring_w.start(lambda half: wo.at[pl.ds(half * 64, 64)])

    own_e = pltpu.make_async_copy(res.at[pl.ds(pl.multiple_of(tp * 128, 128), 128)],
                                  resin.at[:, pl.ds(pl.multiple_of(tp * 256, 256), 256)], er.at[tp])
    own_e.start()
    own_g = pltpu.make_async_copy(gain, gainall.at[:, pl.ds(pl.multiple_of(tp * 256, 256), 256)], gr.at[tp])
    own_g.start()
    for k in range(1, 8):
        to = lax.rem(tp + k, 8)
        cols = pl.ds(pl.multiple_of(tp * 256, 256), 256)
        go(send(res.at[pl.ds(pl.multiple_of(to * 128, 128), 128)], resin.at[:, cols], es.at[k], er.at[tp], (sp, to)))
        go(send(gain, gainall.at[:, cols], gs.at[k], gr.at[tp], (sp, to)))

    def arrived(b):
        send(kvall.at[c, b], kvall.at[c, b], s_sib.at[b], rr.at[b], sib).wait_recv()
        go(send(kvall.at[c, b], kvall.at[c, b], s_sib.at[b], r_sib.at[b], sib))

    def right(b):
        go(send(kvall.at[c, b], kvall.at[c, b], s_r.at[b], rr.at[b], dev(z, yp, x, c)))

    def left(b):
        go(send(kvall.at[c, b], kvall.at[c, b], s_l.at[b], rr.at[b], dev(z, ym, x, c)))

    zs = [z, up(z, 1), up(z, 3), up(z, 2)]

    def near(r):
        b = zs[r] * 4 + y
        arrived(b)
        right(b)
        left(b)

    def next_to(r):
        b = zs[r] * 4 + ym
        arrived(b)
        if r in (0, 2):
            right(b)
        b = zs[r] * 4 + yp
        arrived(b)
        if r in (1, 3):
            left(b)

    near(0)
    ring_d.start(lambda half: wd.at[pl.ds(half * HALF, HALF)])
    ring_u.start(lambda half: wu.at[pl.ds(half * 64, 64)])
    near(1)
    near(2)
    next_to(0)
    ring_w.middle(0)
    near(3)
    ring_u.middle(0)
    ring_d.middle(0)
    next_to(1)
    next_to(2)
    ring_w.middle(1)
    ring_u.middle(1)
    ring_d.middle(1)
    next_to(3)
    for r in range(4):
        arrived(zs[r] * 4 + y2)
    ring_w.last()
    ring_u.last()
    ring_d.last()

    for b in range(16):
        send(kvall.at[1 - c, b], kvall.at[1 - c, b], s_sib.at[b], r_sib.at[b], sib).wait_recv()
    for n in range(8):
        rows = pl.ds((2 * (n // 2) + (1 - c)) * 128 + (n % 2) * 64, 64)
        send(woall.at[rows], woall.at[rows], w_sib.at[n], wr_sib.at[n], sib).wait_recv()
    for i in range(4):
        send(qin.at[i], qin.at[i], qs.at[0], qr.at[i], sib).wait_recv()
    for n in range(8):
        cols = pl.ds(n * 256, 256)
        send(resin.at[:, cols], resin.at[:, cols], es.at[0], er.at[n], sib).wait_recv()
        send(gainall.at[:, cols], gainall.at[:, cols], gs.at[0], gr.at[n], sib).wait_recv()
    for loc in own_w:
        loc.wait()
    for mine, remote in pending:
        @pl.when(jnp.logical_not(mine))
        def _():
            remote.wait_send()
    for copy in done:
        copy.wait_send()


def exchange(*args):
    return pl.pallas_call(
        exchange_kernel,
        out_shape=(
            sds((4, HD, HALF), BF),
            sds((2, 16, ITEM, 128), BF),
            sds((1024, D), BF),
            sds((128, D), BF),
            sds((8, D), F32),
            sds((4, 128, 1024), BF),
            sds((4, T, 128), BF),
        ),
        in_specs=[HB] * 10,
        out_specs=(HB,) * 7,
        scratch_shapes=[
            pltpu.VMEM((T, 128), BF),
            pltpu.VMEM((T, 128), BF),
            pltpu.VMEM((T, 128), BF),
            pltpu.VMEM((2, T), F32),
            pltpu.VMEM((1, T), jnp.int32),
            pltpu.VMEM((256,), BF),
            pltpu.VMEM((128, D), BF),
            pltpu.VMEM((T, 256), BF),
            pltpu.VMEM((128, 1024), BF),
            pltpu.VMEM((1024, 128), BF),
            pltpu.VMEM((2, HD, T), BF),
            pltpu.VMEM((2, 2, ITEM, 128), BF),
            pltpu.VMEM((8, 256), F32),
            DMA((10,)),
            DMA((4,)), DMA((4,)), DMA((4,)), DMA((16,)), DMA((16,)), DMA((16,)), DMA((16,)), DMA((16,)),
            DMA((2,)), DMA((8,)), DMA((8,)), DMA((8,)), DMA((8,)), DMA((8,)),
            DMA((8,)), DMA((8,)), DMA((8,)), DMA((8,)),
            DMA((8,)), DMA((8,)), DMA((8,)), DMA((8,)), DMA((8,)), DMA((8,)), DMA((2,)),
        ],
        compiler_params=pltpu.CompilerParams(has_side_effects=True, collective_id=0),
        cost_estimate=pl.CostEstimate(flops=20_000_000_000, bytes_accessed=16_000_000, transcendentals=0),
        name="exchange",
    )(*args)


QW = 256
NS = HALF // QW


def attend_kernel(q_h, kv_h, o_ref, q_ref, kv_ref, aux_ref, in_sem, pieces, gmat, w_ref, *scr):
    z, y, x, c = place()
    main = pl.ds(0, HALF)
    loads = [
        pltpu.make_async_copy(kv_h.at[1, :, pl.ds(HALF, 64)], aux_ref, in_sem.at[0]),
        pltpu.make_async_copy(q_h, q_ref, in_sem.at[1]),
        pltpu.make_async_copy(kv_h.at[0, :, main], kv_ref.at[0], in_sem.at[2]),
        pltpu.make_async_copy(kv_h.at[1, :, main], kv_ref.at[1], in_sem.at[3]),
    ]
    for load in loads:
        load.start()
    loads[0].wait()
    s_refs, accs, tops, shrinks = scr[:NS], scr[NS:2 * NS], scr[2 * NS:3 * NS], scr[3 * NS:]
    ones = jnp.ones((16, HALF), BF)
    count = jnp.zeros((1, 128), F32)
    for b in range(16):
        for n in range(8):
            a = aux_ref[b, n * 8:(n + 1) * 8, :].astype(F32)
            count = count + a[3:4]
            hf, at = n // 4, (n % 4) * 128
            pieces[b * 8 + hf * 4:b * 8 + hf * 4 + 4, at:at + 128] = a[:4]
    docs0 = jnp.sum(count).astype(jnp.int32)
    gmat[...] = pieces[...].T.astype(BF)
    for load in loads[1:]:
        load.wait()
    row = lax.broadcasted_iota(jnp.int32, (128, QW), 0)
    unit_of_row, piece_of_row = row // 4, row % 4

    def tile(i, carry):
        hq = 2 * (4 * i + y) + lax.rem(c + i, 2)
        start = jnp.where(hq * HALF >= docs0, lax.div(docs0, HALF), 0)
        q_pos = hq * HALF + lax.broadcasted_iota(jnp.int32, (1, HALF), 1)
        doc1 = jnp.where(q_pos >= docs0, -BIG, 0.0)
        for k in range(NS):
            cols = slice(k * QW, (k + 1) * QW)
            w_ref[:, cols] = jnp.where(piece_of_row == 3, doc1[:, cols], -1.0)

        def scores(k, u, first):
            cols = slice(k * QW, (k + 1) * QW)
            q = q_ref[i, :, cols]
            none = jnp.zeros_like(q)
            b, low = lax.div(u, 2), lax.rem(u, 2) == 0
            lhs = jnp.concatenate([kv_ref[0, b], gmat[...]], axis=1)
            sel = jnp.where(unit_of_row == u, w_ref[:, cols], 0.0).astype(BF)
            rhs = jnp.concatenate([jnp.where(low, q, none), jnp.where(low, none, q), sel], axis=0)
            s = jnp.dot(lhs, rhs, preferred_element_type=F32)
            if first:
                key = lax.broadcasted_iota(jnp.int32, (HALF, QW), 0)
                s = jnp.where(key <= k * QW + lax.broadcasted_iota(jnp.int32, (HALF, QW), 1), s, far_below)
            s_refs[k][...] = s
            new = jnp.max(s, axis=0, keepdims=True)
            if not first:
                old = tops[k][...]
                new = jnp.maximum(old, new)
                shrinks[k][...] = jnp.exp(old - new)
            tops[k][...] = new

        def weigh(k, u, first):
            b, hf = lax.div(u, 2), lax.rem(u, 2)
            p = jnp.exp(s_refs[k][...] - tops[k][...]).astype(BF)
            vt = jnp.concatenate(
                [kv_ref[1, b, pl.ds(pl.multiple_of(hf * 256 + n * 64, 64), 64), :] for n in range(4)], axis=1
            )
            vt = jnp.concatenate([vt, ones], axis=0)
            product = jnp.dot(vt, p, preferred_element_type=F32)
            accs[k][...] = product if first else accs[k][...] * shrinks[k][...] + product

        ahead = jnp.maximum(hq - 1, 0)
        scores(0, hq, True)
        scores(1, hq, True)
        weigh(0, hq, True)
        scores(0, jnp.minimum(start, ahead), False)
        weigh(1, hq, True)

        def step(u, carry):
            scores(1, u, False)
            weigh(0, u, False)
            scores(0, jnp.minimum(u + 1, ahead), False)
            weigh(1, u, False)
            return carry

        lax.fori_loop(start, hq, step, 0)
        for k in range(NS):
            total = accs[k][...]
            o_ref[i, :, k * QW:(k + 1) * QW] = (total[:HD] / total[HD:HD + 1]).astype(BF)
        return carry

    lax.fori_loop(0, 4, tile, 0)


def attend(q, kv):
    return pl.pallas_call(
        attend_kernel,
        out_shape=sds((4, HD, HALF), BF),
        in_specs=[HB, HB],
        out_specs=VM,
        scratch_shapes=[
            pltpu.VMEM((4, HD, HALF), BF),
            pltpu.VMEM((2, 16, HALF, 128), BF),
            pltpu.VMEM((16, 64, 128), BF),
            DMA((4,)),
            pltpu.VMEM((128, HALF), F32),
            pltpu.VMEM((HALF, 128), BF),
            pltpu.VMEM((128, HALF), F32),
        ]
        + [pltpu.VMEM((HALF, QW), F32)] * NS
        + [pltpu.VMEM((80, QW), F32)] * NS
        + [pltpu.VMEM((1, QW), F32)] * (2 * NS),
        compiler_params=pltpu.CompilerParams(vmem_limit_bytes=66_500_000),
        cost_estimate=pl.CostEstimate(flops=20_000_000_000, bytes_accessed=8_000_000, transcendentals=0),
        name="attend",
    )(q, kv)


G = 4
ROWS = T // G
PIECE = 128 // G
A, B = pl.ds(0, ROWS // 2), pl.ds(ROWS // 2, ROWS // 2)


def tail_kernel(
    att, wo_any, res, gain, u0, um, upl, d0, dm, dpl, out,
    a_in, wo, own, midb, wu, wd, normed, hidden, part, sibbuf, stage, hop_a, hop_b, from_l, from_r,
    w_sem, a_s, a_r, o_s, o_r, g_s, g_r, t_s, t_r,
):
    z, y, x, c = place()
    sp, tp = z * 4 + y, x * 2 + c
    sib = dev(z, y, x, 1 - c)
    xp, xm, x2 = up(x, 1), up(x, 3), up(x, 2)
    right, left = dev(z, y, xp, c), dev(z, y, xm, c)
    z_next, z_prev, y_next, y_prev = up(z, 1), up(z, 3), up(y, 1), up(y, 3)
    head = 4 * x + z

    def wu_rows(zz, lo, n):
        return wu.at[pl.ds(pl.multiple_of(zz * 512 + lo, 256), n)]

    loads = [
        pltpu.make_async_copy(wo_any, wo, w_sem.at[0]),
        pltpu.make_async_copy(u0, wu_rows(z, 0, 512), w_sem.at[1]),
        pltpu.make_async_copy(um, wu_rows(z_prev, 0, 512), w_sem.at[2]),
        pltpu.make_async_copy(upl, wu_rows(z_next, 0, 512), w_sem.at[3]),
        pltpu.make_async_copy(d0, wd.at[y], w_sem.at[4]),
        pltpu.make_async_copy(dm, wd.at[y_prev], w_sem.at[5]),
        pltpu.make_async_copy(dpl, wd.at[y_next], w_sem.at[6]),
    ]
    for load in loads:
        load.start()
    barrier = pltpu.get_barrier_semaphore()
    cs = lax.rem(lax.div(tp, 4) + z, 2)
    for zs in range(4):
        for xs in range(4):
            @pl.when(jnp.logical_not((z == zs) & (x == xs) & (c == cs)))
            def _():
                signal(barrier, dev(zs, y, xs, cs))

    to_z = dev(z_next, y, x, c), dev(z_prev, y, x, c)
    to_y = dev(z, y_next, x, c), dev(z, y_prev, x, c)
    for device in (sib, right, left, *to_z, *to_y):
        signal(barrier, device)
    pl.semaphore_wait(barrier, jnp.where(lax.div(x, 2) == lax.rem(c + z, 2), 22, 23))

    done = []

    def go(copy):
        copy.start()
        done.append(copy)

    pending = []
    for i in range(4):
        hf = lax.rem(c + i, 2)
        for k in range(4):
            to = 4 * hf + k
            mine = (z == i) & (to == tp)
            src = att.at[i, :, pl.ds(k * 128, 128)]
            dst = a_in.at[pl.ds(pl.multiple_of(head * HD, HD), HD)]
            local = pltpu.make_async_copy(src, dst, a_r.at[head])
            remote = send(src, dst, a_s.at[4 * i + k], a_r.at[head], (i * 4 + y, to))

            @pl.when(mine)
            def _():
                local.start()

            @pl.when(jnp.logical_not(mine))
            def _():
                remote.start()

            pending.append((mine, remote))

    go(send(um.at[pl.ds(0, 256)], wu_rows(z_prev, 0, 256), o_s.at[0], o_r.at[0], to_z[0]))
    go(send(upl.at[pl.ds(256, 256)], wu_rows(z_next, 256, 256), o_s.at[1], o_r.at[1], to_z[1]))
    go(send(dm.at[pl.ds(0, 2)], wd.at[y_prev, pl.ds(0, 2)], o_s.at[2], o_r.at[2], to_y[0]))
    go(send(dpl.at[pl.ds(2, 2)], wd.at[y_next, pl.ds(2, 2)], o_s.at[3], o_r.at[3], to_y[1]))

    for h in range(16):
        rows = pl.ds(h * HD, HD)
        send(a_in.at[rows], a_in.at[rows], a_s.at[0], a_r.at[h], sib).wait_recv()
    loads[0].wait()
    a = a_in[...].astype(F32).T.astype(BF)
    for n in range(4):
        cols = slice(n * 512, (n + 1) * 512)
        mixed = jnp.dot(a, wo[:, cols], preferred_element_type=F32)
        own[:, cols] = (res[:, cols].astype(F32) + mixed).astype(BF)

    def piece(g, xs, cc, lo=0, n=PIECE):
        return midb.at[g, pl.ds(pl.multiple_of((2 * xs + cc) * PIECE + lo, PIECE // 2), n)]

    def pass_on(g, at, k, device, kr=None):
        go(send(at, at, g_s.at[k, g], g_r.at[k if kr is None else kr, g], device))

    def came(g, at, k):
        send(at, at, g_s.at[k, g], g_r.at[k, g], sib).wait_recv()

    def gather_own(g):
        src, dst = own.at[pl.ds(g * PIECE, PIECE)], piece(g, x, c)
        go(send(src, dst, g_s.at[0, g], g_r.at[0, g], right))
        go(send(src, dst, g_s.at[1, g], g_r.at[1, g], left))
        go(send(src, dst, g_s.at[4, g], g_r.at[4, g], sib))
        midb[g, pl.ds(pl.multiple_of(tp * PIECE, PIECE), PIECE), :] = own[g * PIECE:(g + 1) * PIECE, :]

    def gather_near(g):
        came(g, piece(g, xm, c), 0)
        pass_on(g, piece(g, xm, c, 0, PIECE // 2), 2, right)
        pass_on(g, piece(g, xm, c), 5, sib)
        came(g, piece(g, xp, c), 1)
        pass_on(g, piece(g, xp, c, PIECE // 2, PIECE // 2), 3, left)
        pass_on(g, piece(g, xp, c), 6, sib)

    def gather_far(g):
        for k in (0, 1):
            at = piece(g, x2, c, k * (PIECE // 2), PIECE // 2)
            came(g, at, 2 + k)
            pass_on(g, at, 7 + k, sib)

    def gather_rest(g):
        came(g, piece(g, x, 1 - c), 4)
        came(g, piece(g, xm, 1 - c), 5)
        came(g, piece(g, xp, 1 - c), 6)
        came(g, piece(g, x2, 1 - c, 0, PIECE // 2), 7)
        came(g, piece(g, x2, 1 - c, PIECE // 2, PIECE // 2), 8)

    def feed(g):
        wide = midb[g].astype(F32)
        inv = lax.rsqrt(jnp.mean(wide * wide, axis=-1, keepdims=True) + eps)
        normed[...] = (wide * inv * gain[0:1, :]).astype(BF)

        def lift(n, carry):
            cols = pl.ds(pl.multiple_of(n * 256, 256), 256)
            h = jnp.dot(normed[...], wu[:, cols], preferred_element_type=F32)
            hidden[:, cols] = jnp.square(jnp.maximum(h, 0.0)).astype(BF)
            return carry

        lax.fori_loop(0, 4, lift, 0)

        def drop(core):
            def one(k, carry):
                yy = 2 * core + k
                cols = pl.multiple_of(k * 128, 128)
                for zp in (0, 2):
                    rhs = jnp.concatenate([wd[yy, zp], wd[yy, zp + 1]], axis=1)
                    term = jnp.dot(hidden[...], rhs, preferred_element_type=F32).astype(BF)
                    part[g, core, zp, :, pl.ds(cols, 128)] = term[:, :128]
                    part[g, core, zp + 1, :, pl.ds(cols, 128)] = term[:, 128:]
                return carry

            lax.fori_loop(0, 2, one, 0)

        drop(1 - c)
        go(send(part.at[g, 1 - c], sibbuf.at[g], t_s.at[0, g], t_r.at[0, g], sib))
        drop(c)

    def both(g, rel, rows):
        xt = up(x, rel)
        return part[g, c, xt, rows, :].astype(F32) + sibbuf[g, xt, rows, :].astype(F32)

    def scatter_first(g):
        send(sibbuf.at[g], sibbuf.at[g], t_s.at[0, g], t_r.at[0, g], sib).wait_recv()
        stage[g, 2] = both(g, 2, pl.ds(0, ROWS)).astype(BF)
        go(send(stage.at[g, 2, A], hop_a.at[g], t_s.at[1, g], t_r.at[1, g], right))
        go(send(stage.at[g, 2, B], hop_b.at[g], t_s.at[2, g], t_r.at[2, g], left))
        stage[g, 1, B, :] = both(g, 1, B).astype(BF)
        go(send(stage.at[g, 1, B], from_l.at[g, B], t_s.at[3, g], t_r.at[3, g], right))
        stage[g, 3, A, :] = both(g, 3, A).astype(BF)
        go(send(stage.at[g, 3, A], from_r.at[g, A], t_s.at[4, g], t_r.at[4, g], left))

    def scatter_second(g):
        send(hop_a.at[g], hop_a.at[g], t_s.at[1, g], t_r.at[1, g], sib).wait_recv()
        stage[g, 1, A, :] = (both(g, 1, A) + hop_a[g].astype(F32)).astype(BF)
        go(send(stage.at[g, 1, A], from_l.at[g, A], t_s.at[5, g], t_r.at[5, g], right))
        send(hop_b.at[g], hop_b.at[g], t_s.at[2, g], t_r.at[2, g], sib).wait_recv()
        stage[g, 3, B, :] = (both(g, 3, B) + hop_b[g].astype(F32)).astype(BF)
        go(send(stage.at[g, 3, B], from_r.at[g, B], t_s.at[6, g], t_r.at[6, g], left))

    def scatter_third(g):
        for k, buf, rows in ((3, from_l, B), (4, from_r, A), (5, from_l, A), (6, from_r, B)):
            send(buf.at[g, rows], buf.at[g, rows], t_s.at[k, g], t_r.at[k, g], sib).wait_recv()
        for n in range(8):
            rows = pl.ds(n * PIECE, PIECE)
            total = both(g, 0, rows) + from_l[g, rows, :].astype(F32) + from_r[g, rows, :].astype(F32)
            mid = midb[g, rows, pl.ds(pl.multiple_of(tp * 256, 256), 256)].astype(F32)
            out[n * 128 + g * PIECE:n * 128 + (g + 1) * PIECE, :] = (mid + total).astype(BF)

    gather_own(0)
    gather_own(1)
    gather_near(0)
    gather_own(2)
    gather_near(1)
    gather_own(3)
    gather_far(0)
    gather_rest(0)
    for load in loads[1:]:
        load.wait()
    for k, at in ((0, wu_rows(up(z, 2), 0, 256)), (1, wu_rows(up(z, 2), 256, 256)),
                  (2, wd.at[up(y, 2), pl.ds(0, 2)]), (3, wd.at[up(y, 2), pl.ds(2, 2)])):
        send(at, at, o_s.at[k], o_r.at[k], sib).wait_recv()
    feed(0)
    gather_near(2)
    gather_far(1)
    gather_rest(1)
    gather_near(3)
    scatter_first(0)
    feed(1)
    gather_far(2)
    gather_rest(2)
    gather_far(3)
    scatter_first(1)
    scatter_second(0)
    feed(2)
    gather_rest(3)
    scatter_first(2)
    scatter_second(1)
    feed(3)
    scatter_second(2)
    scatter_first(3)
    scatter_third(0)
    scatter_third(1)
    scatter_second(3)
    scatter_third(2)
    scatter_third(3)
    for mine, remote in pending:
        @pl.when(jnp.logical_not(mine))
        def _():
            remote.wait_send()
    for copy in done:
        copy.wait_send()


def tail(att, wo, res, gain, ups, downs):
    return pl.pallas_call(
        tail_kernel,
        out_shape=sds((T, 256), BF),
        in_specs=[VM, HB, VM, VM] + [HB] * 6,
        out_specs=VM,
        scratch_shapes=[
            pltpu.VMEM((1024, 128), BF),
            pltpu.VMEM((1024, D), BF),
            pltpu.VMEM((128, D), BF),
            pltpu.VMEM((G, ROWS, D), BF),
            pltpu.VMEM((D, 1024), BF),
            pltpu.VMEM((4, 4, 1024, 128), BF),
            pltpu.VMEM((ROWS, D), BF),
            pltpu.VMEM((ROWS, 1024), BF),
            pltpu.VMEM((G, 2, 4, ROWS, 256), BF),
            pltpu.VMEM((G, 4, ROWS, 256), BF),
            pltpu.VMEM((G, 4, ROWS, 256), BF),
            pltpu.VMEM((G, ROWS // 2, 256), BF),
            pltpu.VMEM((G, ROWS // 2, 256), BF),
            pltpu.VMEM((G, ROWS, 256), BF),
            pltpu.VMEM((G, ROWS, 256), BF),
            DMA((7,)), DMA((16,)), DMA((16,)), DMA((4,)), DMA((4,)),
            DMA((9, G)), DMA((9, G)), DMA((7, G)), DMA((7, G)),
        ],
        compiler_params=pltpu.CompilerParams(
            has_side_effects=True, collective_id=1, vmem_limit_bytes=56 * 1024 * 1024
        ),
        cost_estimate=pl.CostEstimate(flops=20_000_000_000, bytes_accessed=8_000_000, transcendentals=0),
        name="tail",
    )(att, wo, res, gain, *ups, *downs)


def shifted(value, axis, step):
    def index(z, y):
        return (z % 4) * 4 + y % 4

    pairs = [
        (index(z, y), index(z + step, y) if axis == "z" else index(z, y + step)) for z in range(4) for y in range(4)
    ]
    return lax.ppermute(value, "sp", pairs)


def body(queries, keys, values, cum_gates, doc_ids, residual, w_out, norm_gain, w_up, w_down):
    qin, kvall, woall, resin, gain, u0, d0 = exchange(
        queries, keys, values, jnp.transpose(cum_gates), doc_ids.reshape(1, T), norm_gain, w_out, residual, w_up, w_down
    )
    um, upl = shifted(u0, "z", 1), shifted(u0, "z", -1)
    dm, dpl = shifted(d0, "y", 1), shifted(d0, "y", -1)
    att = attend(qin, kvall)
    ups = [u.reshape(512, 1024) for u in (u0, um, upl)]
    return tail(att, woall, resin, gain, ups, (d0, dm, dpl))


def solution(mesh):
    in_specs = (
        P("sp", "tp"),
        P("sp", "tp"),
        P("sp", "tp"),
        P("sp", "tp"),
        P("sp"),
        P("sp", "tp"),
        P("tp", None),
        P("tp"),
        P("sp", "tp"),
        P("tp", "sp"),
    )
    return jax.shard_map(body, mesh=mesh, in_specs=in_specs, out_specs=P("sp", "tp"), check_vma=False)
```

```python
import functools

import jax
import jax.numpy as jnp
from jax import lax
from jax.experimental import pallas as pl
from jax.experimental.pallas import tpu as pltpu
from jax.sharding import PartitionSpec as P

D = 2048
HD = 64
T = 1024
HALF = 512
ITEM = 528
eps = 1e-06
far_below = -1e30
BIG = 8192.0
MESH = pl.DeviceIdType.MESH
BF = jnp.bfloat16
F32 = jnp.float32
VM = pl.BlockSpec(memory_space=pltpu.VMEM)
HB = pl.BlockSpec(memory_space=pl.ANY)
DMA = pltpu.SemaphoreType.DMA


def sds(shape, dtype):
    return jax.ShapeDtypeStruct(shape, dtype)


def place():
    sp, tp = lax.axis_index("sp"), lax.axis_index("tp")
    return lax.div(sp, 4), lax.rem(sp, 4), lax.div(tp, 2), lax.rem(tp, 2)


def dev(z, y, x, c):
    return (z * 4 + y, x * 2 + c)


def send(src, dst, ssem, rsem, device):
    return pltpu.make_async_remote_copy(
        src_ref=src, dst_ref=dst, send_sem=ssem, recv_sem=rsem, device_id=device, device_id_type=MESH
    )


def up(v, k):
    return lax.rem(v + k, 4)


def column(i, y):
    return jnp.where(lax.rem(i, 2) == 0, y, 3 - y) if not isinstance(i, int) else (y if i % 2 == 0 else 3 - y)


def signal(barrier, device):
    pl.semaphore_signal(barrier, inc=1, device_id=device, device_id_type=MESH)


class Ring:
    def __init__(self, go, me, slot, right, left, s_r, s_l, r, sib=None, s_sib=None, r_sib=None):
        self.go, self.me, self.slot, self.right, self.left = go, me, slot, right, left
        self.s_r, self.s_l, self.r = s_r, s_l, r
        self.sib, self.s_sib, self.r_sib = sib, s_sib, r_sib

    def start(self, src, order=(0, 1)):
        for half in order:
            n, dst = 2 * self.me + half, self.slot(self.me, half)
            self.go(send(src(half), dst, self.s_r.at[n], self.r.at[n], self.right))
            self.go(send(src(half), dst, self.s_l.at[n], self.r.at[n], self.left))
            if self.s_sib is not None:
                self.go(send(src(half), dst, self.s_sib.at[n], self.r_sib.at[n], self.sib))

    def take(self, i, half, forward=0):
        n, at = 2 * i + half, self.slot(i, half)
        send(at, at, self.s_r.at[n], self.r.at[n], self.right).wait_recv()
        if forward > 0:
            self.go(send(at, at, self.s_r.at[n], self.r.at[n], self.right))
        if forward < 0:
            self.go(send(at, at, self.s_l.at[n], self.r.at[n], self.left))
        if self.s_sib is not None:
            self.go(send(at, at, self.s_sib.at[n], self.r_sib.at[n], self.sib))

    def middle(self, half):
        lo, hi = up(self.me, 3), up(self.me, 1)
        if half == 0:
            self.take(lo, 0, 1)
            self.take(hi, 0)
        else:
            self.take(hi, 1, -1)
            self.take(lo, 1)

    def last(self):
        self.take(up(self.me, 2), 0)
        self.take(up(self.me, 2), 1)


def pack_kernel(q_ref, k_ref, v_ref, g_ref, d_ref, n_ref, qt_ref, kv_ref, gain_ref):
    gain_ref[...] = jnp.broadcast_to(n_ref[...].astype(F32)[None], (8, 256))
    qt = (q_ref[...].astype(F32) * (HD ** -0.5)).T.astype(BF)
    qt_ref[0] = qt[:HD]
    qt_ref[1] = qt[HD:]
    k_lo, k_hi = k_ref[:HALF].astype(F32), k_ref[HALF:].astype(F32)
    first = lax.broadcasted_iota(jnp.int32, (HALF, 128), 1) < HD
    kv_ref[0, 0, :HALF] = jnp.where(first, k_lo, pltpu.roll(k_hi, HD, 1)).astype(BF)
    kv_ref[0, 1, :HALF] = jnp.where(first, pltpu.roll(k_lo, HD, 1), k_hi).astype(BF)
    vt = v_ref[...].astype(F32).T.astype(BF)
    row = lax.broadcasted_iota(jnp.int32, (8, T), 0)
    kind = lax.rem(row, 4)
    doc0 = 1.0 - d_ref[...].astype(F32)
    for j in range(2):
        g = g_ref[j:j + 1, :]
        hi = g.astype(BF).astype(F32)
        mid = (g - hi).astype(BF).astype(F32)
        lo = (g - hi) - mid
        aux = jnp.where(kind == 0, hi, jnp.where(kind == 1, mid, jnp.where(kind == 2, lo, doc0)))
        aux = jnp.where(row < 4, aux, pltpu.roll(aux, T - 128, 1))
        for n in range(8):
            kv_ref[1, j, n * 64:(n + 1) * 64] = vt[j * HD:(j + 1) * HD, n * 128:(n + 1) * 128]
        for t in range(2):
            at = t * 512
            two = jnp.concatenate([aux[:, at:at + 128], aux[:, at + 256:at + 384]], axis=0)
            kv_ref[t, j, HALF:] = two.astype(BF)


def exchange_kernel(
    q_h, k_h, v_h, g_h, d_h, n_h, wo_h, res_h, wu_h, wd_h, qin, kvall, woall, resin, gainall, wu4, wd4,
    q_v, k_v, v_v, g_v, d_v, n_v, wo, res, wu, wd, qt, kv, gain, in_sem,
    qs, qr, ks, rr, s_sib, r_sib, s_r, s_l,
    wl, w_sib, wr_sib, w_s_r, w_s_l, w_r, es, er, gs, gr,
    u_s_r, u_s_l, u_r, d_s_r, d_s_l, d_r, ul,
):
    z, y, x, c = place()
    sp, tp = z * 4 + y, x * 2 + c
    sib = dev(z, y, x, 1 - c)
    yp, ym, y2 = up(y, 1), up(y, 3), up(y, 2)
    xp, xm, x2 = up(x, 1), up(x, 3), up(x, 2)

    loads = [
        pltpu.make_async_copy(src, dst, in_sem.at[n])
        for n, (src, dst) in enumerate(
            zip((k_h, v_h, g_h, d_h, n_h, q_h, wo_h, res_h, wu_h, wd_h), (k_v, v_v, g_v, d_v, n_v, q_v, wo, res, wu, wd))
        )
    ]
    for load in loads:
        load.start()
    barrier = pltpu.get_barrier_semaphore()
    cs = lax.div(z, 2)
    for zs in range(4):
        @pl.when(jnp.logical_not((z == zs) & (c == cs)))
        def _():
            signal(barrier, dev(zs, y, x, cs))

    for k in range(1, 8):
        signal(barrier, (sp, lax.rem(tp + k, 8)))
    signal(barrier, dev(z, yp, x, c))
    signal(barrier, dev(z, ym, x, c))
    zp, zm = up(z, 1), up(z, 3)
    signal(barrier, dev(zp, y, x, c))
    signal(barrier, dev(zm, y, x, c))
    for load in loads:
        load.wait()
    pack_kernel(q_v, k_v, v_v, g_v, d_v, n_v, qt, kv, gain)
    for i in (1, 3):
        signal(barrier, dev(i, 3 - y, x, cs))
    pl.semaphore_wait(barrier, jnp.where(c == cs, 14, 15) + 4 * lax.rem(z, 2))

    def guarded(is_self, local, remote):
        @pl.when(is_self)
        def _():
            local.start()

        @pl.when(jnp.logical_not(is_self))
        def _():
            remote.start()

    pending = []
    for j in range(2):
        zt = 2 * c + j
        for t in range(2):
            mine = (zt == z) & (c == t)
            src, dst = kv.at[t, j], kvall.at[t, sp]
            remote = send(src, dst, ks.at[2 * t + j], rr.at[sp], dev(zt, y, x, t))
            guarded(mine, pltpu.make_async_copy(src, dst, rr.at[sp]), remote)
            pending.append((mine, remote))
    for j in range(2):
        zt = 2 * c + j
        for hf in range(2):
            ct = lax.rem(hf + z, 2)
            mine = (zt == z) & (ct == c) & (lax.rem(z, 2) == 0)
            src, dst = qt.at[j, :, pl.ds(hf * HALF, HALF)], qin.at[z]
            remote = send(src, dst, qs.at[2 * j + hf], qr.at[z], dev(zt, column(z, y), x, ct))
            guarded(mine, pltpu.make_async_copy(src, dst, qr.at[z]), remote)
            pending.append((mine, remote))

    done = []

    def wrows(xs, half):
        return pl.ds((2 * xs + c) * 128 + half * 64, 64)

    def go(copy):
        copy.start()
        done.append(copy)

    ring_w = Ring(go, x, lambda i, half: woall.at[wrows(i, half)], dev(z, y, xp, c), dev(z, y, xm, c),
                  w_s_r, w_s_l, w_r, sib, w_sib, wr_sib)
    ring_u = Ring(go, y, lambda i, half: wu4.at[i, pl.ds(half * 64, 64)], dev(z, yp, x, c), dev(z, ym, x, c),
                  u_s_r, u_s_l, u_r)
    ring_d = Ring(go, z, lambda i, half: wd4.at[i, pl.ds(half * HALF, HALF)], dev(zp, y, x, c), dev(zm, y, x, c),
                  d_s_r, d_s_l, d_r)
    own_w = [
        pltpu.make_async_copy(wo, woall.at[pl.ds(pl.multiple_of(tp * 128, 128), 128)], wl.at[0]),
        pltpu.make_async_copy(wu, wu4.at[y], ul.at[0]),
        pltpu.make_async_copy(wd, wd4.at[z], ul.at[1]),
    ]
    for loc in own_w:
        loc.start()
    ring_w.start(lambda half: wo.at[pl.ds(half * 64, 64)])

    own_e = pltpu.make_async_copy(res.at[pl.ds(pl.multiple_of(tp * 128, 128), 128)],
                                  resin.at[:, pl.ds(pl.multiple_of(tp * 256, 256), 256)], er.at[tp])
    own_e.start()
    own_g = pltpu.make_async_copy(gain, gainall.at[:, pl.ds(pl.multiple_of(tp * 256, 256), 256)], gr.at[tp])
    own_g.start()
    for k in range(1, 8):
        to = lax.rem(tp + k, 8)
        cols = pl.ds(pl.multiple_of(tp * 256, 256), 256)
        go(send(res.at[pl.ds(pl.multiple_of(to * 128, 128), 128)], resin.at[:, cols], es.at[k], er.at[tp], (sp, to)))
        go(send(gain, gainall.at[:, cols], gs.at[k], gr.at[tp], (sp, to)))

    def arrived(b):
        send(kvall.at[c, b], kvall.at[c, b], s_sib.at[b], rr.at[b], sib).wait_recv()
        go(send(kvall.at[c, b], kvall.at[c, b], s_sib.at[b], r_sib.at[b], sib))

    def right(b):
        go(send(kvall.at[c, b], kvall.at[c, b], s_r.at[b], rr.at[b], dev(z, yp, x, c)))

    def left(b):
        go(send(kvall.at[c, b], kvall.at[c, b], s_l.at[b], rr.at[b], dev(z, ym, x, c)))

    zs = [z, up(z, 1), up(z, 3), up(z, 2)]

    def near(r):
        b = zs[r] * 4 + y
        arrived(b)
        right(b)
        left(b)

    def next_to(r):
        b = zs[r] * 4 + ym
        arrived(b)
        if r in (0, 2):
            right(b)
        b = zs[r] * 4 + yp
        arrived(b)
        if r in (1, 3):
            left(b)

    near(0)
    ring_d.start(lambda half: wd.at[pl.ds(half * HALF, HALF)])
    ring_u.start(lambda half: wu.at[pl.ds(half * 64, 64)])
    near(1)
    near(2)
    next_to(0)
    ring_w.middle(0)
    near(3)
    ring_u.middle(0)
    ring_d.middle(0)
    next_to(1)
    next_to(2)
    ring_w.middle(1)
    ring_u.middle(1)
    ring_d.middle(1)
    next_to(3)
    for r in range(4):
        arrived(zs[r] * 4 + y2)
    ring_w.last()
    ring_u.last()
    ring_d.last()

    for b in range(16):
        send(kvall.at[1 - c, b], kvall.at[1 - c, b], s_sib.at[b], r_sib.at[b], sib).wait_recv()
    for n in range(8):
        rows = pl.ds((2 * (n // 2) + (1 - c)) * 128 + (n % 2) * 64, 64)
        send(woall.at[rows], woall.at[rows], w_sib.at[n], wr_sib.at[n], sib).wait_recv()
    for i in range(4):
        send(qin.at[i], qin.at[i], qs.at[0], qr.at[i], sib).wait_recv()
    for n in range(8):
        cols = pl.ds(n * 256, 256)
        send(resin.at[:, cols], resin.at[:, cols], es.at[0], er.at[n], sib).wait_recv()
        send(gainall.at[:, cols], gainall.at[:, cols], gs.at[0], gr.at[n], sib).wait_recv()
    for loc in own_w:
        loc.wait()
    for mine, remote in pending:
        @pl.when(jnp.logical_not(mine))
        def _():
            remote.wait_send()
    for copy in done:
        copy.wait_send()


def exchange(*args):
    return pl.pallas_call(
        exchange_kernel,
        out_shape=(
            sds((4, HD, HALF), BF),
            sds((2, 16, ITEM, 128), BF),
            sds((1024, D), BF),
            sds((128, D), BF),
            sds((8, D), F32),
            sds((4, 128, 1024), BF),
            sds((4, T, 128), BF),
        ),
        in_specs=[HB] * 10,
        out_specs=(HB,) * 7,
        scratch_shapes=[
            pltpu.VMEM((T, 128), BF),
            pltpu.VMEM((T, 128), BF),
            pltpu.VMEM((T, 128), BF),
            pltpu.VMEM((2, T), F32),
            pltpu.VMEM((1, T), jnp.int32),
            pltpu.VMEM((256,), BF),
            pltpu.VMEM((128, D), BF),
            pltpu.VMEM((T, 256), BF),
            pltpu.VMEM((128, 1024), BF),
            pltpu.VMEM((1024, 128), BF),
            pltpu.VMEM((2, HD, T), BF),
            pltpu.VMEM((2, 2, ITEM, 128), BF),
            pltpu.VMEM((8, 256), F32),
            DMA((10,)),
            DMA((4,)), DMA((4,)), DMA((4,)), DMA((16,)), DMA((16,)), DMA((16,)), DMA((16,)), DMA((16,)),
            DMA((2,)), DMA((8,)), DMA((8,)), DMA((8,)), DMA((8,)), DMA((8,)),
            DMA((8,)), DMA((8,)), DMA((8,)), DMA((8,)),
            DMA((8,)), DMA((8,)), DMA((8,)), DMA((8,)), DMA((8,)), DMA((8,)), DMA((2,)),
        ],
        compiler_params=pltpu.CompilerParams(has_side_effects=True, collective_id=0),
        cost_estimate=pl.CostEstimate(flops=20_000_000_000, bytes_accessed=16_000_000, transcendentals=0),
        name="exchange",
    )(*args)


QW = 256
NS = HALF // QW


def attend_kernel(q_h, kv_h, o_ref, q_ref, kv_ref, aux_ref, in_sem, pieces, gmat, w_ref, *scr):
    z, y, x, c = place()
    main = pl.ds(0, HALF)
    loads = [
        pltpu.make_async_copy(kv_h.at[0, :, pl.ds(HALF, 16)], aux_ref.at[0], in_sem.at[0]),
        pltpu.make_async_copy(kv_h.at[1, :, pl.ds(HALF, 16)], aux_ref.at[1], in_sem.at[4]),
        pltpu.make_async_copy(q_h, q_ref, in_sem.at[1]),
        pltpu.make_async_copy(kv_h.at[0, :, main], kv_ref.at[0], in_sem.at[2]),
        pltpu.make_async_copy(kv_h.at[1, :, main], kv_ref.at[1], in_sem.at[3]),
    ]
    for load in loads:
        load.start()
    loads[0].wait()
    loads[1].wait()
    s_refs, accs, tops, shrinks = scr[:NS], scr[NS:2 * NS], scr[2 * NS:3 * NS], scr[3 * NS:]
    ones = jnp.ones((16, HALF), BF)
    count = jnp.zeros((1, 128), F32)
    for b in range(16):
        for t in range(2):
            a = aux_ref[t, b].astype(F32)
            for k in range(4):
                hf, at = t, k * 128
                count = count + a[k * 4 + 3:k * 4 + 4]
                pieces[b * 8 + hf * 4:b * 8 + hf * 4 + 4, at:at + 128] = a[k * 4:k * 4 + 4]
    docs0 = jnp.sum(count).astype(jnp.int32)
    gmat[...] = pieces[...].T.astype(BF)
    for load in loads[2:]:
        load.wait()
    row = lax.broadcasted_iota(jnp.int32, (128, QW), 0)
    unit_of_row, piece_of_row = row // 4, row % 4

    def tile(i, carry):
        hq = 2 * (4 * i + column(i, y)) + lax.rem(c + i, 2)
        start = jnp.where(hq * HALF >= docs0, lax.div(docs0, HALF), 0)
        q_pos = hq * HALF + lax.broadcasted_iota(jnp.int32, (1, HALF), 1)
        doc1 = jnp.where(q_pos >= docs0, -BIG, 0.0)
        for k in range(NS):
            cols = slice(k * QW, (k + 1) * QW)
            w_ref[:, cols] = jnp.where(piece_of_row == 3, doc1[:, cols], -1.0)

        def scores(k, u, first):
            cols = slice(k * QW, (k + 1) * QW)
            q = q_ref[i, :, cols]
            none = jnp.zeros_like(q)
            b, low = lax.div(u, 2), lax.rem(u, 2) == 0
            lhs = jnp.concatenate([kv_ref[0, b], gmat[...]], axis=1)
            sel = jnp.where(unit_of_row == u, w_ref[:, cols], 0.0).astype(BF)
            rhs = jnp.concatenate([jnp.where(low, q, none), jnp.where(low, none, q), sel], axis=0)
            s = jnp.dot(lhs, rhs, preferred_element_type=F32)
            if first:
                key = lax.broadcasted_iota(jnp.int32, (HALF, QW), 0)
                s = jnp.where(key <= k * QW + lax.broadcasted_iota(jnp.int32, (HALF, QW), 1), s, far_below)
            s_refs[k][...] = s
            new = jnp.max(s, axis=0, keepdims=True)
            if not first:
                old = tops[k][...]
                new = jnp.maximum(old, new)
                shrinks[k][...] = jnp.exp(old - new)
            tops[k][...] = new

        def weigh(k, u, first):
            b, hf = lax.div(u, 2), lax.rem(u, 2)
            p = jnp.exp(s_refs[k][...] - tops[k][...]).astype(BF)
            vt = jnp.concatenate(
                [kv_ref[1, b, pl.ds(pl.multiple_of(hf * 256 + n * 64, 64), 64), :] for n in range(4)], axis=1
            )
            vt = jnp.concatenate([vt, ones], axis=0)
            product = jnp.dot(vt, p, preferred_element_type=F32)
            accs[k][...] = product if first else accs[k][...] * shrinks[k][...] + product

        ahead = jnp.maximum(hq - 1, 0)
        scores(0, hq, True)
        scores(1, hq, True)
        weigh(0, hq, True)
        scores(0, jnp.minimum(start, ahead), False)
        weigh(1, hq, True)

        def step(u, carry):
            scores(1, u, False)
            weigh(0, u, False)
            scores(0, jnp.minimum(u + 1, ahead), False)
            weigh(1, u, False)
            return carry

        lax.fori_loop(start, hq, step, 0)
        for k in range(NS):
            total = accs[k][...]
            o_ref[i, :, k * QW:(k + 1) * QW] = (total[:HD] / total[HD:HD + 1]).astype(BF)
        return carry

    lax.fori_loop(0, 4, tile, 0)


def attend(q, kv):
    return pl.pallas_call(
        attend_kernel,
        out_shape=sds((4, HD, HALF), BF),
        in_specs=[HB, HB],
        out_specs=VM,
        scratch_shapes=[
            pltpu.VMEM((4, HD, HALF), BF),
            pltpu.VMEM((2, 16, HALF, 128), BF),
            pltpu.VMEM((2, 16, 16, 128), BF),
            DMA((5,)),
            pltpu.VMEM((128, HALF), F32),
            pltpu.VMEM((HALF, 128), BF),
            pltpu.VMEM((128, HALF), F32),
        ]
        + [pltpu.VMEM((HALF, QW), F32)] * NS
        + [pltpu.VMEM((80, QW), F32)] * NS
        + [pltpu.VMEM((1, QW), F32)] * (2 * NS),
        compiler_params=pltpu.CompilerParams(vmem_limit_bytes=66_500_000),
        cost_estimate=pl.CostEstimate(flops=20_000_000_000, bytes_accessed=8_000_000, transcendentals=0),
        name="attend",
    )(q, kv)


G = 4
ROWS = T // G
PIECE = 128 // G
A, B = pl.ds(0, ROWS // 2), pl.ds(ROWS // 2, ROWS // 2)


def tail_kernel(
    att, wo_any, res, gain, u0, um, upl, d0, dm, dpl, out,
    a_in, wo, own, midb, wu, wd, normed, hidden, part, sibbuf, stage, hop_a, hop_b, from_l, from_r,
    w_sem, a_s, a_r, o_s, o_r, g_s, g_r, t_s, t_r,
):
    z, y, x, c = place()
    sp, tp = z * 4 + y, x * 2 + c
    sib = dev(z, y, x, 1 - c)
    xp, xm, x2 = up(x, 1), up(x, 3), up(x, 2)
    right, left = dev(z, y, xp, c), dev(z, y, xm, c)
    z_next, z_prev, y_next, y_prev = up(z, 1), up(z, 3), up(y, 1), up(y, 3)
    head = 4 * x + z

    def wu_rows(zz, lo, n):
        return wu.at[pl.ds(pl.multiple_of(zz * 512 + lo, 256), n)]

    loads = [
        pltpu.make_async_copy(wo_any, wo, w_sem.at[0]),
        pltpu.make_async_copy(u0, wu_rows(z, 0, 512), w_sem.at[1]),
        pltpu.make_async_copy(um, wu_rows(z_prev, 0, 512), w_sem.at[2]),
        pltpu.make_async_copy(upl, wu_rows(z_next, 0, 512), w_sem.at[3]),
        pltpu.make_async_copy(d0, wd.at[y], w_sem.at[4]),
        pltpu.make_async_copy(dm, wd.at[y_prev], w_sem.at[5]),
        pltpu.make_async_copy(dpl, wd.at[y_next], w_sem.at[6]),
    ]
    for load in loads:
        load.start()
    barrier = pltpu.get_barrier_semaphore()
    cs = lax.rem(lax.div(tp, 4) + z, 2)
    for zs in range(4):
        for xs in range(4):
            @pl.when(jnp.logical_not((z == zs) & (x == xs) & (c == cs) & (lax.rem(z, 2) == 0)))
            def _():
                signal(barrier, dev(zs, column(z, y), xs, cs))

    to_z = dev(z_next, y, x, c), dev(z_prev, y, x, c)
    to_y = dev(z, y_next, x, c), dev(z, y_prev, x, c)
    for device in (sib, right, left, *to_z, *to_y):
        signal(barrier, device)
    pl.semaphore_wait(barrier, jnp.where((lax.div(x, 2) == lax.rem(c + z, 2)) & (lax.rem(z, 2) == 0), 22, 23))

    done = []

    def go(copy):
        copy.start()
        done.append(copy)

    pending = []
    for i in range(4):
        hf = lax.rem(c + i, 2)
        for k in range(4):
            to = 4 * hf + k
            mine = (z == i) & (to == tp) if i % 2 == 0 else None
            src = att.at[i, :, pl.ds(k * 128, 128)]
            dst = a_in.at[pl.ds(pl.multiple_of(head * HD, HD), HD)]
            remote = send(src, dst, a_s.at[4 * i + k], a_r.at[head], (i * 4 + column(i, y), to))
            if mine is None:
                go(remote)
                continue
            local = pltpu.make_async_copy(src, dst, a_r.at[head])

            @pl.when(mine)
            def _():
                local.start()

            @pl.when(jnp.logical_not(mine))
            def _():
                remote.start()

            pending.append((mine, remote))

    go(send(um.at[pl.ds(0, 256)], wu_rows(z_prev, 0, 256), o_s.at[0], o_r.at[0], to_z[0]))
    go(send(upl.at[pl.ds(256, 256)], wu_rows(z_next, 256, 256), o_s.at[1], o_r.at[1], to_z[1]))
    go(send(dm.at[pl.ds(0, 2)], wd.at[y_prev, pl.ds(0, 2)], o_s.at[2], o_r.at[2], to_y[0]))
    go(send(dpl.at[pl.ds(2, 2)], wd.at[y_next, pl.ds(2, 2)], o_s.at[3], o_r.at[3], to_y[1]))

    for h in range(16):
        rows = pl.ds(h * HD, HD)
        send(a_in.at[rows], a_in.at[rows], a_s.at[0], a_r.at[h], sib).wait_recv()
    loads[0].wait()
    a = a_in[...].astype(F32).T.astype(BF)
    for n in range(4):
        cols = slice(n * 512, (n + 1) * 512)
        mixed = jnp.dot(a, wo[:, cols], preferred_element_type=F32)
        own[:, cols] = (res[:, cols].astype(F32) + mixed).astype(BF)

    def piece(g, xs, cc, lo=0, n=PIECE):
        return midb.at[g, pl.ds(pl.multiple_of((2 * xs + cc) * PIECE + lo, PIECE // 2), n)]

    def pass_on(g, at, k, device, kr=None):
        go(send(at, at, g_s.at[k, g], g_r.at[k if kr is None else kr, g], device))

    def came(g, at, k):
        send(at, at, g_s.at[k, g], g_r.at[k, g], sib).wait_recv()

    def gather_own(g):
        src, dst = own.at[pl.ds(g * PIECE, PIECE)], piece(g, x, c)
        go(send(src, dst, g_s.at[0, g], g_r.at[0, g], right))
        go(send(src, dst, g_s.at[1, g], g_r.at[1, g], left))
        go(send(src, dst, g_s.at[4, g], g_r.at[4, g], sib))
        midb[g, pl.ds(pl.multiple_of(tp * PIECE, PIECE), PIECE), :] = own[g * PIECE:(g + 1) * PIECE, :]

    def gather_near(g):
        came(g, piece(g, xm, c), 0)
        pass_on(g, piece(g, xm, c, 0, PIECE // 2), 2, right)
        pass_on(g, piece(g, xm, c), 5, sib)
        came(g, piece(g, xp, c), 1)
        pass_on(g, piece(g, xp, c, PIECE // 2, PIECE // 2), 3, left)
        pass_on(g, piece(g, xp, c), 6, sib)

    def gather_far(g):
        for k in (0, 1):
            at = piece(g, x2, c, k * (PIECE // 2), PIECE // 2)
            came(g, at, 2 + k)
            pass_on(g, at, 7 + k, sib)

    def gather_rest(g):
        came(g, piece(g, x, 1 - c), 4)
        came(g, piece(g, xm, 1 - c), 5)
        came(g, piece(g, xp, 1 - c), 6)
        came(g, piece(g, x2, 1 - c, 0, PIECE // 2), 7)
        came(g, piece(g, x2, 1 - c, PIECE // 2, PIECE // 2), 8)

    def feed(g):
        wide = midb[g].astype(F32)
        inv = lax.rsqrt(jnp.mean(wide * wide, axis=-1, keepdims=True) + eps)
        normed[...] = (wide * inv * gain[0:1, :]).astype(BF)

        def lift(n, carry):
            cols = pl.ds(pl.multiple_of(n * 256, 256), 256)
            h = jnp.dot(normed[...], wu[:, cols], preferred_element_type=F32)
            hidden[:, cols] = jnp.square(jnp.maximum(h, 0.0)).astype(BF)
            return carry

        lax.fori_loop(0, 4, lift, 0)

        def drop(core):
            def one(k, carry):
                yy = 2 * core + k
                cols = pl.multiple_of(k * 128, 128)
                for zp in (0, 2):
                    rhs = jnp.concatenate([wd[yy, zp], wd[yy, zp + 1]], axis=1)
                    term = jnp.dot(hidden[...], rhs, preferred_element_type=F32).astype(BF)
                    part[g, core, zp, :, pl.ds(cols, 128)] = term[:, :128]
                    part[g, core, zp + 1, :, pl.ds(cols, 128)] = term[:, 128:]
                return carry

            lax.fori_loop(0, 2, one, 0)

        drop(1 - c)
        go(send(part.at[g, 1 - c], sibbuf.at[g], t_s.at[0, g], t_r.at[0, g], sib))
        drop(c)

    def both(g, rel, rows):
        xt = up(x, rel)
        return part[g, c, xt, rows, :].astype(F32) + sibbuf[g, xt, rows, :].astype(F32)

    def scatter_first(g):
        send(sibbuf.at[g], sibbuf.at[g], t_s.at[0, g], t_r.at[0, g], sib).wait_recv()
        stage[g, 2] = both(g, 2, pl.ds(0, ROWS)).astype(BF)
        go(send(stage.at[g, 2, A], hop_a.at[g], t_s.at[1, g], t_r.at[1, g], right))
        go(send(stage.at[g, 2, B], hop_b.at[g], t_s.at[2, g], t_r.at[2, g], left))
        stage[g, 1, B, :] = both(g, 1, B).astype(BF)
        go(send(stage.at[g, 1, B], from_l.at[g, B], t_s.at[3, g], t_r.at[3, g], right))
        stage[g, 3, A, :] = both(g, 3, A).astype(BF)
        go(send(stage.at[g, 3, A], from_r.at[g, A], t_s.at[4, g], t_r.at[4, g], left))

    def scatter_second(g):
        send(hop_a.at[g], hop_a.at[g], t_s.at[1, g], t_r.at[1, g], sib).wait_recv()
        stage[g, 1, A, :] = (both(g, 1, A) + hop_a[g].astype(F32)).astype(BF)
        go(send(stage.at[g, 1, A], from_l.at[g, A], t_s.at[5, g], t_r.at[5, g], right))
        send(hop_b.at[g], hop_b.at[g], t_s.at[2, g], t_r.at[2, g], sib).wait_recv()
        stage[g, 3, B, :] = (both(g, 3, B) + hop_b[g].astype(F32)).astype(BF)
        go(send(stage.at[g, 3, B], from_r.at[g, B], t_s.at[6, g], t_r.at[6, g], left))

    def scatter_third(g):
        for k, buf, rows in ((3, from_l, B), (4, from_r, A), (5, from_l, A), (6, from_r, B)):
            send(buf.at[g, rows], buf.at[g, rows], t_s.at[k, g], t_r.at[k, g], sib).wait_recv()
        for n in range(8):
            rows = pl.ds(n * PIECE, PIECE)
            total = both(g, 0, rows) + from_l[g, rows, :].astype(F32) + from_r[g, rows, :].astype(F32)
            mid = midb[g, rows, pl.ds(pl.multiple_of(tp * 256, 256), 256)].astype(F32)
            out[n * 128 + g * PIECE:n * 128 + (g + 1) * PIECE, :] = (mid + total).astype(BF)

    gather_own(0)
    gather_own(1)
    gather_near(0)
    gather_own(2)
    gather_near(1)
    gather_own(3)
    gather_far(0)
    gather_rest(0)
    for load in loads[1:]:
        load.wait()
    for k, at in ((0, wu_rows(up(z, 2), 0, 256)), (1, wu_rows(up(z, 2), 256, 256)),
                  (2, wd.at[up(y, 2), pl.ds(0, 2)]), (3, wd.at[up(y, 2), pl.ds(2, 2)])):
        send(at, at, o_s.at[k], o_r.at[k], sib).wait_recv()
    feed(0)
    gather_near(2)
    gather_far(1)
    gather_rest(1)
    gather_near(3)
    scatter_first(0)
    feed(1)
    gather_far(2)
    gather_rest(2)
    gather_far(3)
    scatter_first(1)
    scatter_second(0)
    feed(2)
    gather_rest(3)
    scatter_first(2)
    scatter_second(1)
    feed(3)
    scatter_second(2)
    scatter_first(3)
    scatter_third(0)
    scatter_third(1)
    scatter_second(3)
    scatter_third(2)
    scatter_third(3)
    for mine, remote in pending:
        @pl.when(jnp.logical_not(mine))
        def _():
            remote.wait_send()
    for copy in done:
        copy.wait_send()


def tail(att, wo, res, gain, ups, downs):
    return pl.pallas_call(
        tail_kernel,
        out_shape=sds((T, 256), BF),
        in_specs=[VM, HB, VM, VM] + [HB] * 6,
        out_specs=VM,
        scratch_shapes=[
            pltpu.VMEM((1024, 128), BF),
            pltpu.VMEM((1024, D), BF),
            pltpu.VMEM((128, D), BF),
            pltpu.VMEM((G, ROWS, D), BF),
            pltpu.VMEM((D, 1024), BF),
            pltpu.VMEM((4, 4, 1024, 128), BF),
            pltpu.VMEM((ROWS, D), BF),
            pltpu.VMEM((ROWS, 1024), BF),
            pltpu.VMEM((G, 2, 4, ROWS, 256), BF),
            pltpu.VMEM((G, 4, ROWS, 256), BF),
            pltpu.VMEM((G, 4, ROWS, 256), BF),
            pltpu.VMEM((G, ROWS // 2, 256), BF),
            pltpu.VMEM((G, ROWS // 2, 256), BF),
            pltpu.VMEM((G, ROWS, 256), BF),
            pltpu.VMEM((G, ROWS, 256), BF),
            DMA((7,)), DMA((16,)), DMA((16,)), DMA((4,)), DMA((4,)),
            DMA((9, G)), DMA((9, G)), DMA((7, G)), DMA((7, G)),
        ],
        compiler_params=pltpu.CompilerParams(
            has_side_effects=True, collective_id=1, vmem_limit_bytes=56 * 1024 * 1024
        ),
        cost_estimate=pl.CostEstimate(flops=20_000_000_000, bytes_accessed=8_000_000, transcendentals=0),
        name="tail",
    )(att, wo, res, gain, *ups, *downs)


def shifted(value, axis, step):
    def index(z, y):
        return (z % 4) * 4 + y % 4

    pairs = [
        (index(z, y), index(z + step, y) if axis == "z" else index(z, y + step)) for z in range(4) for y in range(4)
    ]
    return lax.ppermute(value, "sp", pairs)


def body(queries, keys, values, cum_gates, doc_ids, residual, w_out, norm_gain, w_up, w_down):
    qin, kvall, woall, resin, gain, u0, d0 = exchange(
        queries, keys, values, jnp.transpose(cum_gates), doc_ids.reshape(1, T), norm_gain, w_out, residual, w_up, w_down
    )
    um, upl = shifted(u0, "z", 1), shifted(u0, "z", -1)
    dm, dpl = shifted(d0, "y", 1), shifted(d0, "y", -1)
    att = attend(qin, kvall)
    ups = [u.reshape(512, 1024) for u in (u0, um, upl)]
    return tail(att, woall, resin, gain, ups, (d0, dm, dpl))


def solution(mesh):
    in_specs = (
        P("sp", "tp"),
        P("sp", "tp"),
        P("sp", "tp"),
        P("sp", "tp"),
        P("sp"),
        P("sp", "tp"),
        P("tp", None),
        P("tp"),
        P("sp", "tp"),
        P("tp", "sp"),
    )
    return jax.shard_map(body, mesh=mesh, in_specs=in_specs, out_specs=P("sp", "tp"), check_vma=False)
```

```python
import functools

import jax
import jax.numpy as jnp
from jax import lax
from jax.experimental import pallas as pl
from jax.experimental.pallas import tpu as pltpu
from jax.sharding import PartitionSpec as P

D = 2048
HD = 64
T = 1024
HALF = 512
ITEM = 528
eps = 1e-06
far_below = -1e30
BIG = 8192.0
MESH = pl.DeviceIdType.MESH
BF = jnp.bfloat16
F32 = jnp.float32
VM = pl.BlockSpec(memory_space=pltpu.VMEM)
HB = pl.BlockSpec(memory_space=pl.ANY)
DMA = pltpu.SemaphoreType.DMA


def sds(shape, dtype):
    return jax.ShapeDtypeStruct(shape, dtype)


def place():
    sp, tp = lax.axis_index("sp"), lax.axis_index("tp")
    return lax.div(sp, 4), lax.rem(sp, 4), lax.div(tp, 2), lax.rem(tp, 2)


def dev(z, y, x, c):
    return (z * 4 + y, x * 2 + c)


def send(src, dst, ssem, rsem, device):
    return pltpu.make_async_remote_copy(
        src_ref=src, dst_ref=dst, send_sem=ssem, recv_sem=rsem, device_id=device, device_id_type=MESH
    )


def up(v, k):
    return lax.rem(v + k, 4)


def signal(barrier, device):
    pl.semaphore_signal(barrier, inc=1, device_id=device, device_id_type=MESH)


class Ring:
    def __init__(self, go, me, slot, right, left, s_r, s_l, r, sib=None, s_sib=None, r_sib=None):
        self.go, self.me, self.slot, self.right, self.left = go, me, slot, right, left
        self.s_r, self.s_l, self.r = s_r, s_l, r
        self.sib, self.s_sib, self.r_sib = sib, s_sib, r_sib

    def start(self, src, order=(0, 1)):
        for half in order:
            n, dst = 2 * self.me + half, self.slot(self.me, half)
            self.go(send(src(half), dst, self.s_r.at[n], self.r.at[n], self.right))
            self.go(send(src(half), dst, self.s_l.at[n], self.r.at[n], self.left))
            if self.s_sib is not None:
                self.go(send(src(half), dst, self.s_sib.at[n], self.r_sib.at[n], self.sib))

    def take(self, i, half, forward=0):
        n, at = 2 * i + half, self.slot(i, half)
        send(at, at, self.s_r.at[n], self.r.at[n], self.right).wait_recv()
        if forward > 0:
            self.go(send(at, at, self.s_r.at[n], self.r.at[n], self.right))
        if forward < 0:
            self.go(send(at, at, self.s_l.at[n], self.r.at[n], self.left))
        if self.s_sib is not None:
            self.go(send(at, at, self.s_sib.at[n], self.r_sib.at[n], self.sib))

    def middle(self, half):
        lo, hi = up(self.me, 3), up(self.me, 1)
        if half == 0:
            self.take(lo, 0, 1)
            self.take(hi, 0)
        else:
            self.take(hi, 1, -1)
            self.take(lo, 1)

    def last(self):
        self.take(up(self.me, 2), 0)
        self.take(up(self.me, 2), 1)


def pack_kernel(q_ref, k_ref, v_ref, g_ref, d_ref, n_ref, qt_ref, kv_ref, gain_ref):
    gain_ref[...] = jnp.broadcast_to(n_ref[...].astype(F32)[None], (8, 256))
    qt = (q_ref[...].astype(F32) * (HD ** -0.5)).T.astype(BF)
    qt_ref[0] = qt[:HD]
    qt_ref[1] = qt[HD:]
    k_lo, k_hi = k_ref[:HALF].astype(F32), k_ref[HALF:].astype(F32)
    first = lax.broadcasted_iota(jnp.int32, (HALF, 128), 1) < HD
    kv_ref[0, 0, :HALF] = jnp.where(first, k_lo, pltpu.roll(k_hi, HD, 1)).astype(BF)
    kv_ref[0, 1, :HALF] = jnp.where(first, pltpu.roll(k_lo, HD, 1), k_hi).astype(BF)
    vt = v_ref[...].astype(F32).T.astype(BF)
    row = lax.broadcasted_iota(jnp.int32, (8, T), 0)
    kind = lax.rem(row, 4)
    doc0 = 1.0 - d_ref[...].astype(F32)
    for j in range(2):
        g = g_ref[j:j + 1, :]
        hi = g.astype(BF).astype(F32)
        mid = (g - hi).astype(BF).astype(F32)
        lo = (g - hi) - mid
        aux = jnp.where(kind == 0, hi, jnp.where(kind == 1, mid, jnp.where(kind == 2, lo, doc0)))
        aux = jnp.where(row < 4, aux, pltpu.roll(aux, T - 128, 1))
        for n in range(8):
            kv_ref[1, j, n * 64:(n + 1) * 64] = vt[j * HD:(j + 1) * HD, n * 128:(n + 1) * 128]
        for t in range(2):
            at = t * 512
            two = jnp.concatenate([aux[:, at:at + 128], aux[:, at + 256:at + 384]], axis=0)
            kv_ref[t, j, HALF:] = two.astype(BF)


def exchange_kernel(
    q_h, k_h, v_h, g_h, d_h, n_h, wo_h, res_h, wu_h, wd_h, qin, kvall, woall, resin, gainall, wu4, wd4,
    q_v, k_v, v_v, g_v, d_v, n_v, wo, res, wu, wd, qt, kv, gain, in_sem,
    qs, qr, ks, rr, s_sib, r_sib, s_r, s_l,
    wl, w_sib, wr_sib, w_s_r, w_s_l, w_r, es, er, gs, gr,
    u_s_r, u_s_l, u_r, d_s_r, d_s_l, d_r, ul,
):
    z, y, x, c = place()
    sp, tp = z * 4 + y, x * 2 + c
    sib = dev(z, y, x, 1 - c)
    yp, ym, y2 = up(y, 1), up(y, 3), up(y, 2)
    xp, xm, x2 = up(x, 1), up(x, 3), up(x, 2)

    loads = [
        pltpu.make_async_copy(src, dst, in_sem.at[n])
        for n, (src, dst) in enumerate(
            zip((k_h, v_h, g_h, d_h, n_h, q_h, wo_h, res_h, wu_h, wd_h), (k_v, v_v, g_v, d_v, n_v, q_v, wo, res, wu, wd))
        )
    ]
    for load in loads:
        load.start()
    barrier = pltpu.get_barrier_semaphore()
    cs = lax.div(z, 2)
    for zs in range(4):
        @pl.when(jnp.logical_not((z == zs) & (c == cs)))
        def _():
            signal(barrier, dev(zs, y, x, cs))

    for k in range(1, 8):
        signal(barrier, (sp, lax.rem(tp + k, 8)))
    signal(barrier, dev(z, yp, x, c))
    signal(barrier, dev(z, ym, x, c))
    zp, zm = up(z, 1), up(z, 3)
    signal(barrier, dev(zp, y, x, c))
    signal(barrier, dev(zm, y, x, c))
    for load in loads:
        load.wait()
    pack_kernel(q_v, k_v, v_v, g_v, d_v, n_v, qt, kv, gain)
    pl.semaphore_wait(barrier, jnp.where(c == cs, 14, 15))

    def guarded(is_self, local, remote):
        @pl.when(is_self)
        def _():
            local.start()

        @pl.when(jnp.logical_not(is_self))
        def _():
            remote.start()

    pending = []
    for j in range(2):
        zt = 2 * c + j
        for t in range(2):
            mine = (zt == z) & (c == t)
            src, dst = kv.at[t, j], kvall.at[t, sp]
            remote = send(src, dst, ks.at[2 * t + j], rr.at[sp], dev(zt, y, x, t))
            guarded(mine, pltpu.make_async_copy(src, dst, rr.at[sp]), remote)
            pending.append((mine, remote))
    for j in range(2):
        zt = 2 * c + j
        for hf in range(2):
            ct = lax.rem(hf + z, 2)
            mine = (zt == z) & (ct == c)
            src, dst = qt.at[j, :, pl.ds(hf * HALF, HALF)], qin.at[z]
            remote = send(src, dst, qs.at[2 * j + hf], qr.at[z], dev(zt, y, x, ct))
            guarded(mine, pltpu.make_async_copy(src, dst, qr.at[z]), remote)
            pending.append((mine, remote))

    done = []

    def wrows(xs, half):
        return pl.ds((2 * xs + c) * 128 + half * 64, 64)

    def go(copy):
        copy.start()
        done.append(copy)

    ring_w = Ring(go, x, lambda i, half: woall.at[wrows(i, half)], dev(z, y, xp, c), dev(z, y, xm, c),
                  w_s_r, w_s_l, w_r, sib, w_sib, wr_sib)
    ring_u = Ring(go, y, lambda i, half: wu4.at[i, pl.ds(half * 64, 64)], dev(z, yp, x, c), dev(z, ym, x, c),
                  u_s_r, u_s_l, u_r)
    ring_d = Ring(go, z, lambda i, half: wd4.at[i, pl.ds(half * HALF, HALF)], dev(zp, y, x, c), dev(zm, y, x, c),
                  d_s_r, d_s_l, d_r)
    own_w = [
        pltpu.make_async_copy(wo, woall.at[pl.ds(pl.multiple_of(tp * 128, 128), 128)], wl.at[0]),
        pltpu.make_async_copy(wu, wu4.at[y], ul.at[0]),
        pltpu.make_async_copy(wd, wd4.at[z], ul.at[1]),
    ]
    for loc in own_w:
        loc.start()
    ring_w.start(lambda half: wo.at[pl.ds(half * 64, 64)])

    own_e = pltpu.make_async_copy(res.at[pl.ds(pl.multiple_of(tp * 128, 128), 128)],
                                  resin.at[:, pl.ds(pl.multiple_of(tp * 256, 256), 256)], er.at[tp])
    own_e.start()
    own_g = pltpu.make_async_copy(gain, gainall.at[:, pl.ds(pl.multiple_of(tp * 256, 256), 256)], gr.at[tp])
    own_g.start()
    for k in range(1, 8):
        to = lax.rem(tp + k, 8)
        cols = pl.ds(pl.multiple_of(tp * 256, 256), 256)
        go(send(res.at[pl.ds(pl.multiple_of(to * 128, 128), 128)], resin.at[:, cols], es.at[k], er.at[tp], (sp, to)))
        go(send(gain, gainall.at[:, cols], gs.at[k], gr.at[tp], (sp, to)))

    def arrived(b):
        send(kvall.at[c, b], kvall.at[c, b], s_sib.at[b], rr.at[b], sib).wait_recv()
        go(send(kvall.at[c, b], kvall.at[c, b], s_sib.at[b], r_sib.at[b], sib))

    def right(b):
        go(send(kvall.at[c, b], kvall.at[c, b], s_r.at[b], rr.at[b], dev(z, yp, x, c)))

    def left(b):
        go(send(kvall.at[c, b], kvall.at[c, b], s_l.at[b], rr.at[b], dev(z, ym, x, c)))

    zs = [z, up(z, 1), up(z, 3), up(z, 2)]

    def near(r):
        b = zs[r] * 4 + y
        arrived(b)
        right(b)
        left(b)

    def next_to(r):
        b = zs[r] * 4 + ym
        arrived(b)
        if r in (0, 2):
            right(b)
        b = zs[r] * 4 + yp
        arrived(b)
        if r in (1, 3):
            left(b)

    near(0)
    ring_d.start(lambda half: wd.at[pl.ds(half * HALF, HALF)])
    ring_u.start(lambda half: wu.at[pl.ds(half * 64, 64)])
    near(1)
    near(2)
    next_to(0)
    ring_w.middle(0)
    near(3)
    ring_u.middle(0)
    ring_d.middle(0)
    next_to(1)
    next_to(2)
    ring_w.middle(1)
    ring_u.middle(1)
    ring_d.middle(1)
    next_to(3)
    for r in range(4):
        arrived(zs[r] * 4 + y2)
    ring_w.last()
    ring_u.last()
    ring_d.last()

    for b in range(16):
        send(kvall.at[1 - c, b], kvall.at[1 - c, b], s_sib.at[b], r_sib.at[b], sib).wait_recv()
    for n in range(8):
        rows = pl.ds((2 * (n // 2) + (1 - c)) * 128 + (n % 2) * 64, 64)
        send(woall.at[rows], woall.at[rows], w_sib.at[n], wr_sib.at[n], sib).wait_recv()
    for i in range(4):
        send(qin.at[i], qin.at[i], qs.at[0], qr.at[i], sib).wait_recv()
    for n in range(8):
        cols = pl.ds(n * 256, 256)
        send(resin.at[:, cols], resin.at[:, cols], es.at[0], er.at[n], sib).wait_recv()
        send(gainall.at[:, cols], gainall.at[:, cols], gs.at[0], gr.at[n], sib).wait_recv()
    for loc in own_w:
        loc.wait()
    for mine, remote in pending:
        @pl.when(jnp.logical_not(mine))
        def _():
            remote.wait_send()
    for copy in done:
        copy.wait_send()


def exchange(*args):
    return pl.pallas_call(
        exchange_kernel,
        out_shape=(
            sds((4, HD, HALF), BF),
            sds((2, 16, ITEM, 128), BF),
            sds((1024, D), BF),
            sds((128, D), BF),
            sds((8, D), F32),
            sds((4, 128, 1024), BF),
            sds((4, T, 128), BF),
        ),
        in_specs=[HB] * 10,
        out_specs=(HB,) * 7,
        scratch_shapes=[
            pltpu.VMEM((T, 128), BF),
            pltpu.VMEM((T, 128), BF),
            pltpu.VMEM((T, 128), BF),
            pltpu.VMEM((2, T), F32),
            pltpu.VMEM((1, T), jnp.int32),
            pltpu.VMEM((256,), BF),
            pltpu.VMEM((128, D), BF),
            pltpu.VMEM((T, 256), BF),
            pltpu.VMEM((128, 1024), BF),
            pltpu.VMEM((1024, 128), BF),
            pltpu.VMEM((2, HD, T), BF),
            pltpu.VMEM((2, 2, ITEM, 128), BF),
            pltpu.VMEM((8, 256), F32),
            DMA((10,)),
            DMA((4,)), DMA((4,)), DMA((4,)), DMA((16,)), DMA((16,)), DMA((16,)), DMA((16,)), DMA((16,)),
            DMA((2,)), DMA((8,)), DMA((8,)), DMA((8,)), DMA((8,)), DMA((8,)),
            DMA((8,)), DMA((8,)), DMA((8,)), DMA((8,)),
            DMA((8,)), DMA((8,)), DMA((8,)), DMA((8,)), DMA((8,)), DMA((8,)), DMA((2,)),
        ],
        compiler_params=pltpu.CompilerParams(has_side_effects=True, collective_id=0),
        cost_estimate=pl.CostEstimate(flops=20_000_000_000, bytes_accessed=16_000_000, transcendentals=0),
        name="exchange",
    )(*args)


QW = 256
NS = HALF // QW
PARTS = (slice(0, 256), slice(256, 512))


def in_turn(*streams):
    streams = list(streams)
    while streams:
        for stream in list(streams):
            if next(stream, streams) is streams:
                streams.remove(stream)


def attend_kernel(q_h, kv_h, o_ref, q_ref, kv_ref, aux_ref, in_sem, pieces, gmat, w_ref, *scr):
    z, y, x, c = place()
    main = pl.ds(0, HALF)
    loads = [
        pltpu.make_async_copy(kv_h.at[0, :, pl.ds(HALF, 16)], aux_ref.at[0], in_sem.at[0]),
        pltpu.make_async_copy(kv_h.at[1, :, pl.ds(HALF, 16)], aux_ref.at[1], in_sem.at[4]),
        pltpu.make_async_copy(q_h, q_ref, in_sem.at[1]),
        pltpu.make_async_copy(kv_h.at[0, :, main], kv_ref.at[0], in_sem.at[2]),
        pltpu.make_async_copy(kv_h.at[1, :, main], kv_ref.at[1], in_sem.at[3]),
    ]
    for load in loads:
        load.start()
    loads[0].wait()
    loads[1].wait()
    s_refs, accs, tops, shrinks = scr[:NS], scr[NS:2 * NS], scr[2 * NS:3 * NS], scr[3 * NS:]
    ones = jnp.ones((16, HALF), BF)
    count = jnp.zeros((1, 128), F32)
    for b in range(16):
        for t in range(2):
            a = aux_ref[t, b].astype(F32)
            for k in range(4):
                hf, at = t, k * 128
                count = count + a[k * 4 + 3:k * 4 + 4]
                pieces[b * 8 + hf * 4:b * 8 + hf * 4 + 4, at:at + 128] = a[k * 4:k * 4 + 4]
    docs0 = jnp.sum(count).astype(jnp.int32)
    gmat[...] = pieces[...].T.astype(BF)
    for load in loads[2:]:
        load.wait()
    row = lax.broadcasted_iota(jnp.int32, (128, QW), 0)
    unit_of_row, piece_of_row = row // 4, row % 4

    def tile(i, carry):
        hq = 2 * (4 * i + y) + lax.rem(c + i, 2)
        start = jnp.where(hq * HALF >= docs0, lax.div(docs0, HALF), 0)
        q_pos = hq * HALF + lax.broadcasted_iota(jnp.int32, (1, HALF), 1)
        doc1 = jnp.where(q_pos >= docs0, -BIG, 0.0)
        for k in range(NS):
            cols = slice(k * QW, (k + 1) * QW)
            w_ref[:, cols] = jnp.where(piece_of_row == 3, doc1[:, cols], -1.0)

        def scores(k, u, first):
            cols = slice(k * QW, (k + 1) * QW)
            q = q_ref[i, :, cols]
            none = jnp.zeros_like(q)
            b, low = lax.div(u, 2), lax.rem(u, 2) == 0
            sel = jnp.where(unit_of_row == u, w_ref[:, cols], 0.0).astype(BF)
            rhs = jnp.concatenate([jnp.where(low, q, none), jnp.where(low, none, q), sel], axis=0)
            largest = []
            for rows in PARTS:
                lhs = jnp.concatenate([kv_ref[0, b, rows, :], gmat[rows, :]], axis=1)
                s = jnp.dot(lhs, rhs, preferred_element_type=F32)
                if first:
                    key = rows.start + lax.broadcasted_iota(jnp.int32, s.shape, 0)
                    s = jnp.where(key <= k * QW + lax.broadcasted_iota(jnp.int32, s.shape, 1), s, far_below)
                s_refs[k][rows, :] = s
                largest.append(jnp.max(s, axis=0, keepdims=True))
                yield
            new = functools.reduce(jnp.maximum, largest)
            if not first:
                old = tops[k][...]
                new = jnp.maximum(old, new)
                shrinks[k][...] = jnp.exp(old - new)
            tops[k][...] = new

        def weigh(k, u, first):
            b, hf = lax.div(u, 2), lax.rem(u, 2)
            vt = jnp.concatenate(
                [kv_ref[1, b, pl.ds(pl.multiple_of(hf * 256 + n * 64, 64), 64), :] for n in range(4)], axis=1
            )
            vt = jnp.concatenate([vt, ones], axis=0)
            most = tops[k][...]
            product = None
            for rows in PARTS:
                p = jnp.exp(s_refs[k][rows, :] - most).astype(BF)
                term = jnp.dot(vt[:, rows], p, preferred_element_type=F32)
                product = term if product is None else product + term
                yield
            accs[k][...] = product if first else accs[k][...] * shrinks[k][...] + product

        ahead = jnp.maximum(hq - 1, 0)
        in_turn(scores(0, hq, True))
        in_turn(scores(1, hq, True), weigh(0, hq, True))
        in_turn(scores(0, jnp.minimum(start, ahead), False), weigh(1, hq, True))

        def step(u, carry):
            in_turn(scores(1, u, False), weigh(0, u, False))
            in_turn(scores(0, jnp.minimum(u + 1, ahead), False), weigh(1, u, False))
            return carry

        lax.fori_loop(start, hq, step, 0)
        for k in range(NS):
            total = accs[k][...]
            o_ref[i, :, k * QW:(k + 1) * QW] = (total[:HD] / total[HD:HD + 1]).astype(BF)
        return carry

    lax.fori_loop(0, 4, tile, 0)


def attend(q, kv):
    return pl.pallas_call(
        attend_kernel,
        out_shape=sds((4, HD, HALF), BF),
        in_specs=[HB, HB],
        out_specs=VM,
        scratch_shapes=[
            pltpu.VMEM((4, HD, HALF), BF),
            pltpu.VMEM((2, 16, HALF, 128), BF),
            pltpu.VMEM((2, 16, 16, 128), BF),
            DMA((5,)),
            pltpu.VMEM((128, HALF), F32),
            pltpu.VMEM((HALF, 128), BF),
            pltpu.VMEM((128, HALF), F32),
        ]
        + [pltpu.VMEM((HALF, QW), F32)] * NS
        + [pltpu.VMEM((80, QW), F32)] * NS
        + [pltpu.VMEM((1, QW), F32)] * (2 * NS),
        compiler_params=pltpu.CompilerParams(vmem_limit_bytes=66_500_000),
        cost_estimate=pl.CostEstimate(flops=20_000_000_000, bytes_accessed=8_000_000, transcendentals=0),
        name="attend",
    )(q, kv)


G = 4
ROWS = T // G
PIECE = 128 // G
A, B = pl.ds(0, ROWS // 2), pl.ds(ROWS // 2, ROWS // 2)


def tail_kernel(
    att, wo_any, res, gain, u0, um, upl, d0, dm, dpl, out,
    a_in, wo, own, midb, wu, wd, normed, hidden, part, sibbuf, stage, hop_a, hop_b, from_l, from_r,
    w_sem, a_s, a_r, o_s, o_r, g_s, g_r, t_s, t_r,
):
    z, y, x, c = place()
    sp, tp = z * 4 + y, x * 2 + c
    sib = dev(z, y, x, 1 - c)
    xp, xm, x2 = up(x, 1), up(x, 3), up(x, 2)
    right, left = dev(z, y, xp, c), dev(z, y, xm, c)
    z_next, z_prev, y_next, y_prev = up(z, 1), up(z, 3), up(y, 1), up(y, 3)
    head = 4 * x + z

    def wu_rows(zz, lo, n):
        return wu.at[pl.ds(pl.multiple_of(zz * 512 + lo, 256), n)]

    loads = [
        pltpu.make_async_copy(wo_any, wo, w_sem.at[0]),
        pltpu.make_async_copy(u0, wu_rows(z, 0, 512), w_sem.at[1]),
        pltpu.make_async_copy(um, wu_rows(z_prev, 0, 512), w_sem.at[2]),
        pltpu.make_async_copy(upl, wu_rows(z_next, 0, 512), w_sem.at[3]),
        pltpu.make_async_copy(d0, wd.at[y], w_sem.at[4]),
        pltpu.make_async_copy(dm, wd.at[y_prev], w_sem.at[5]),
        pltpu.make_async_copy(dpl, wd.at[y_next], w_sem.at[6]),
    ]
    for load in loads:
        load.start()
    barrier = pltpu.get_barrier_semaphore()
    cs = lax.rem(lax.div(tp, 4) + z, 2)
    for zs in range(4):
        for xs in range(4):
            @pl.when(jnp.logical_not((z == zs) & (x == xs) & (c == cs)))
            def _():
                signal(barrier, dev(zs, y, xs, cs))

    to_z = dev(z_next, y, x, c), dev(z_prev, y, x, c)
    to_y = dev(z, y_next, x, c), dev(z, y_prev, x, c)
    for device in (sib, right, left, *to_z, *to_y):
        signal(barrier, device)
    pl.semaphore_wait(barrier, jnp.where(lax.div(x, 2) == lax.rem(c + z, 2), 22, 23))

    done = []

    def go(copy):
        copy.start()
        done.append(copy)

    pending = []
    for i in range(4):
        hf = lax.rem(c + i, 2)
        for k in range(4):
            to = 4 * hf + k
            mine = (z == i) & (to == tp)
            src = att.at[i, :, pl.ds(k * 128, 128)]
            dst = a_in.at[pl.ds(pl.multiple_of(head * HD, HD), HD)]
            remote = send(src, dst, a_s.at[4 * i + k], a_r.at[head], (i * 4 + y, to))
            local = pltpu.make_async_copy(src, dst, a_r.at[head])

            @pl.when(mine)
            def _():
                local.start()

            @pl.when(jnp.logical_not(mine))
            def _():
                remote.start()

            pending.append((mine, remote))

    go(send(um.at[pl.ds(0, 256)], wu_rows(z_prev, 0, 256), o_s.at[0], o_r.at[0], to_z[0]))
    go(send(upl.at[pl.ds(256, 256)], wu_rows(z_next, 256, 256), o_s.at[1], o_r.at[1], to_z[1]))
    go(send(dm.at[pl.ds(0, 2)], wd.at[y_prev, pl.ds(0, 2)], o_s.at[2], o_r.at[2], to_y[0]))
    go(send(dpl.at[pl.ds(2, 2)], wd.at[y_next, pl.ds(2, 2)], o_s.at[3], o_r.at[3], to_y[1]))

    for h in range(16):
        rows = pl.ds(h * HD, HD)
        send(a_in.at[rows], a_in.at[rows], a_s.at[0], a_r.at[h], sib).wait_recv()
    loads[0].wait()
    a = a_in[...].astype(F32).T.astype(BF)
    for n in range(4):
        cols = slice(n * 512, (n + 1) * 512)
        mixed = jnp.dot(a, wo[:, cols], preferred_element_type=F32)
        own[:, cols] = (res[:, cols].astype(F32) + mixed).astype(BF)

    def piece(g, xs, cc, lo=0, n=PIECE):
        return midb.at[g, pl.ds(pl.multiple_of((2 * xs + cc) * PIECE + lo, PIECE // 2), n)]

    def pass_on(g, at, k, device, kr=None):
        go(send(at, at, g_s.at[k, g], g_r.at[k if kr is None else kr, g], device))

    def came(g, at, k):
        send(at, at, g_s.at[k, g], g_r.at[k, g], sib).wait_recv()

    def gather_own(g):
        src, dst = own.at[pl.ds(g * PIECE, PIECE)], piece(g, x, c)
        go(send(src, dst, g_s.at[0, g], g_r.at[0, g], right))
        go(send(src, dst, g_s.at[1, g], g_r.at[1, g], left))
        go(send(src, dst, g_s.at[4, g], g_r.at[4, g], sib))
        midb[g, pl.ds(pl.multiple_of(tp * PIECE, PIECE), PIECE), :] = own[g * PIECE:(g + 1) * PIECE, :]

    def gather_near(g):
        came(g, piece(g, xm, c), 0)
        pass_on(g, piece(g, xm, c, 0, PIECE // 2), 2, right)
        pass_on(g, piece(g, xm, c), 5, sib)
        came(g, piece(g, xp, c), 1)
        pass_on(g, piece(g, xp, c, PIECE // 2, PIECE // 2), 3, left)
        pass_on(g, piece(g, xp, c), 6, sib)

    def gather_far(g):
        for k in (0, 1):
            at = piece(g, x2, c, k * (PIECE // 2), PIECE // 2)
            came(g, at, 2 + k)
            pass_on(g, at, 7 + k, sib)

    def gather_rest(g):
        came(g, piece(g, x, 1 - c), 4)
        came(g, piece(g, xm, 1 - c), 5)
        came(g, piece(g, xp, 1 - c), 6)
        came(g, piece(g, x2, 1 - c, 0, PIECE // 2), 7)
        came(g, piece(g, x2, 1 - c, PIECE // 2, PIECE // 2), 8)

    def feed(g):
        wide = midb[g].astype(F32)
        inv = lax.rsqrt(jnp.mean(wide * wide, axis=-1, keepdims=True) + eps)
        normed[...] = (wide * inv * gain[0:1, :]).astype(BF)

        def lift(n, carry):
            cols = pl.ds(pl.multiple_of(n * 256, 256), 256)
            h = jnp.dot(normed[...], wu[:, cols], preferred_element_type=F32)
            hidden[:, cols] = jnp.square(jnp.maximum(h, 0.0)).astype(BF)
            return carry

        lax.fori_loop(0, 4, lift, 0)

        def drop(core):
            def one(k, carry):
                yy = 2 * core + k
                cols = pl.multiple_of(k * 128, 128)
                for zp in (0, 2):
                    rhs = jnp.concatenate([wd[yy, zp], wd[yy, zp + 1]], axis=1)
                    term = jnp.dot(hidden[...], rhs, preferred_element_type=F32).astype(BF)
                    part[g, core, zp, :, pl.ds(cols, 128)] = term[:, :128]
                    part[g, core, zp + 1, :, pl.ds(cols, 128)] = term[:, 128:]
                return carry

            lax.fori_loop(0, 2, one, 0)

        drop(1 - c)
        go(send(part.at[g, 1 - c], sibbuf.at[g], t_s.at[0, g], t_r.at[0, g], sib))
        drop(c)

    def both(g, rel, rows):
        xt = up(x, rel)
        return part[g, c, xt, rows, :].astype(F32) + sibbuf[g, xt, rows, :].astype(F32)

    def scatter_first(g):
        send(sibbuf.at[g], sibbuf.at[g], t_s.at[0, g], t_r.at[0, g], sib).wait_recv()
        stage[g, 2] = both(g, 2, pl.ds(0, ROWS)).astype(BF)
        go(send(stage.at[g, 2, A], hop_a.at[g], t_s.at[1, g], t_r.at[1, g], right))
        go(send(stage.at[g, 2, B], hop_b.at[g], t_s.at[2, g], t_r.at[2, g], left))
        stage[g, 1, B, :] = both(g, 1, B).astype(BF)
        go(send(stage.at[g, 1, B], from_l.at[g, B], t_s.at[3, g], t_r.at[3, g], right))
        stage[g, 3, A, :] = both(g, 3, A).astype(BF)
        go(send(stage.at[g, 3, A], from_r.at[g, A], t_s.at[4, g], t_r.at[4, g], left))

    def scatter_second(g):
        send(hop_a.at[g], hop_a.at[g], t_s.at[1, g], t_r.at[1, g], sib).wait_recv()
        stage[g, 1, A, :] = (both(g, 1, A) + hop_a[g].astype(F32)).astype(BF)
        go(send(stage.at[g, 1, A], from_l.at[g, A], t_s.at[5, g], t_r.at[5, g], right))
        send(hop_b.at[g], hop_b.at[g], t_s.at[2, g], t_r.at[2, g], sib).wait_recv()
        stage[g, 3, B, :] = (both(g, 3, B) + hop_b[g].astype(F32)).astype(BF)
        go(send(stage.at[g, 3, B], from_r.at[g, B], t_s.at[6, g], t_r.at[6, g], left))

    def scatter_third(g):
        for k, buf, rows in ((3, from_l, B), (4, from_r, A), (5, from_l, A), (6, from_r, B)):
            send(buf.at[g, rows], buf.at[g, rows], t_s.at[k, g], t_r.at[k, g], sib).wait_recv()
        for n in range(8):
            rows = pl.ds(n * PIECE, PIECE)
            total = both(g, 0, rows) + from_l[g, rows, :].astype(F32) + from_r[g, rows, :].astype(F32)
            mid = midb[g, rows, pl.ds(pl.multiple_of(tp * 256, 256), 256)].astype(F32)
            out[n * 128 + g * PIECE:n * 128 + (g + 1) * PIECE, :] = (mid + total).astype(BF)

    gather_own(0)
    gather_own(1)
    gather_near(0)
    gather_own(2)
    gather_near(1)
    gather_own(3)
    gather_far(0)
    gather_rest(0)
    for load in loads[1:]:
        load.wait()
    for k, at in ((0, wu_rows(up(z, 2), 0, 256)), (1, wu_rows(up(z, 2), 256, 256)),
                  (2, wd.at[up(y, 2), pl.ds(0, 2)]), (3, wd.at[up(y, 2), pl.ds(2, 2)])):
        send(at, at, o_s.at[k], o_r.at[k], sib).wait_recv()
    feed(0)
    gather_near(2)
    gather_far(1)
    gather_rest(1)
    gather_near(3)
    scatter_first(0)
    feed(1)
    gather_far(2)
    gather_rest(2)
    gather_far(3)
    scatter_first(1)
    scatter_second(0)
    feed(2)
    gather_rest(3)
    scatter_first(2)
    scatter_second(1)
    feed(3)
    scatter_second(2)
    scatter_first(3)
    scatter_third(0)
    scatter_third(1)
    scatter_second(3)
    scatter_third(2)
    scatter_third(3)
    for mine, remote in pending:
        @pl.when(jnp.logical_not(mine))
        def _():
            remote.wait_send()
    for copy in done:
        copy.wait_send()


def tail(att, wo, res, gain, ups, downs):
    return pl.pallas_call(
        tail_kernel,
        out_shape=sds((T, 256), BF),
        in_specs=[VM, HB, VM, VM] + [HB] * 6,
        out_specs=VM,
        scratch_shapes=[
            pltpu.VMEM((1024, 128), BF),
            pltpu.VMEM((1024, D), BF),
            pltpu.VMEM((128, D), BF),
            pltpu.VMEM((G, ROWS, D), BF),
            pltpu.VMEM((D, 1024), BF),
            pltpu.VMEM((4, 4, 1024, 128), BF),
            pltpu.VMEM((ROWS, D), BF),
            pltpu.VMEM((ROWS, 1024), BF),
            pltpu.VMEM((G, 2, 4, ROWS, 256), BF),
            pltpu.VMEM((G, 4, ROWS, 256), BF),
            pltpu.VMEM((G, 4, ROWS, 256), BF),
            pltpu.VMEM((G, ROWS // 2, 256), BF),
            pltpu.VMEM((G, ROWS // 2, 256), BF),
            pltpu.VMEM((G, ROWS, 256), BF),
            pltpu.VMEM((G, ROWS, 256), BF),
            DMA((7,)), DMA((16,)), DMA((16,)), DMA((4,)), DMA((4,)),
            DMA((9, G)), DMA((9, G)), DMA((7, G)), DMA((7, G)),
        ],
        compiler_params=pltpu.CompilerParams(
            has_side_effects=True, collective_id=1, vmem_limit_bytes=56 * 1024 * 1024
        ),
        cost_estimate=pl.CostEstimate(flops=20_000_000_000, bytes_accessed=8_000_000, transcendentals=0),
        name="tail",
    )(att, wo, res, gain, *ups, *downs)


def shifted(value, axis, step):
    def index(z, y):
        return (z % 4) * 4 + y % 4

    pairs = [
        (index(z, y), index(z + step, y) if axis == "z" else index(z, y + step)) for z in range(4) for y in range(4)
    ]
    return lax.ppermute(value, "sp", pairs)


def body(queries, keys, values, cum_gates, doc_ids, residual, w_out, norm_gain, w_up, w_down):
    qin, kvall, woall, resin, gain, u0, d0 = exchange(
        queries, keys, values, jnp.transpose(cum_gates), doc_ids.reshape(1, T), norm_gain, w_out, residual, w_up, w_down
    )
    um, upl = shifted(u0, "z", 1), shifted(u0, "z", -1)
    dm, dpl = shifted(d0, "y", 1), shifted(d0, "y", -1)
    att = attend(qin, kvall)
    ups = [u.reshape(512, 1024) for u in (u0, um, upl)]
    return tail(att, woall, resin, gain, ups, (d0, dm, dpl))


def solution(mesh):
    in_specs = (
        P("sp", "tp"),
        P("sp", "tp"),
        P("sp", "tp"),
        P("sp", "tp"),
        P("sp"),
        P("sp", "tp"),
        P("tp", None),
        P("tp"),
        P("sp", "tp"),
        P("tp", "sp"),
    )
    return jax.shard_map(body, mesh=mesh, in_specs=in_specs, out_specs=P("sp", "tp"), check_vma=False)
```

```python
import functools

import jax
import jax.numpy as jnp
from jax import lax
from jax.experimental import pallas as pl
from jax.experimental.pallas import tpu as pltpu
from jax.sharding import PartitionSpec as P

D = 2048
HD = 64
T = 1024
HALF = 512
ITEM = 528
eps = 1e-06
far_below = -1e30
BIG = 8192.0
MESH = pl.DeviceIdType.MESH
BF = jnp.bfloat16
F32 = jnp.float32
VM = pl.BlockSpec(memory_space=pltpu.VMEM)
HB = pl.BlockSpec(memory_space=pl.ANY)
DMA = pltpu.SemaphoreType.DMA


def sds(shape, dtype):
    return jax.ShapeDtypeStruct(shape, dtype)


def place():
    sp, tp = lax.axis_index("sp"), lax.axis_index("tp")
    return lax.div(sp, 4), lax.rem(sp, 4), lax.div(tp, 2), lax.rem(tp, 2)


def dev(z, y, x, c):
    return (z * 4 + y, x * 2 + c)


def send(src, dst, ssem, rsem, device):
    return pltpu.make_async_remote_copy(
        src_ref=src, dst_ref=dst, send_sem=ssem, recv_sem=rsem, device_id=device, device_id_type=MESH
    )


def up(v, k):
    return lax.rem(v + k, 4)


def signal(barrier, device):
    pl.semaphore_signal(barrier, inc=1, device_id=device, device_id_type=MESH)


class Ring:
    def __init__(self, go, me, slot, right, left, s_r, s_l, r, sib=None, s_sib=None, r_sib=None):
        self.go, self.me, self.slot, self.right, self.left = go, me, slot, right, left
        self.s_r, self.s_l, self.r = s_r, s_l, r
        self.sib, self.s_sib, self.r_sib = sib, s_sib, r_sib

    def start(self, src, order=(0, 1)):
        for half in order:
            n, dst = 2 * self.me + half, self.slot(self.me, half)
            self.go(send(src(half), dst, self.s_r.at[n], self.r.at[n], self.right))
            self.go(send(src(half), dst, self.s_l.at[n], self.r.at[n], self.left))
            if self.s_sib is not None:
                self.go(send(src(half), dst, self.s_sib.at[n], self.r_sib.at[n], self.sib))

    def take(self, i, half, forward=0):
        n, at = 2 * i + half, self.slot(i, half)
        send(at, at, self.s_r.at[n], self.r.at[n], self.right).wait_recv()
        if forward > 0:
            self.go(send(at, at, self.s_r.at[n], self.r.at[n], self.right))
        if forward < 0:
            self.go(send(at, at, self.s_l.at[n], self.r.at[n], self.left))
        if self.s_sib is not None:
            self.go(send(at, at, self.s_sib.at[n], self.r_sib.at[n], self.sib))

    def middle(self, half):
        lo, hi = up(self.me, 3), up(self.me, 1)
        if half == 0:
            self.take(lo, 0, 1)
            self.take(hi, 0)
        else:
            self.take(hi, 1, -1)
            self.take(lo, 1)

    def last(self):
        self.take(up(self.me, 2), 0)
        self.take(up(self.me, 2), 1)


def pack_kernel(q_ref, k_ref, v_ref, g_ref, d_ref, n_ref, qt_ref, kv_ref, gain_ref):
    gain_ref[...] = jnp.broadcast_to(n_ref[...].astype(F32)[None], (8, 256))
    qt = (q_ref[...].astype(F32) * (HD ** -0.5)).T.astype(BF)
    qt_ref[0] = qt[:HD]
    qt_ref[1] = qt[HD:]
    k_lo, k_hi = k_ref[:HALF].astype(F32), k_ref[HALF:].astype(F32)
    first = lax.broadcasted_iota(jnp.int32, (HALF, 128), 1) < HD
    kv_ref[0, 0, :HALF] = jnp.where(first, k_lo, pltpu.roll(k_hi, HD, 1)).astype(BF)
    kv_ref[0, 1, :HALF] = jnp.where(first, pltpu.roll(k_lo, HD, 1), k_hi).astype(BF)
    vt = v_ref[...].astype(F32).T.astype(BF)
    row = lax.broadcasted_iota(jnp.int32, (8, T), 0)
    kind = lax.rem(row, 4)
    doc0 = 1.0 - d_ref[...].astype(F32)
    for j in range(2):
        g = g_ref[j:j + 1, :]
        hi = g.astype(BF).astype(F32)
        mid = (g - hi).astype(BF).astype(F32)
        lo = (g - hi) - mid
        aux = jnp.where(kind == 0, hi, jnp.where(kind == 1, mid, jnp.where(kind == 2, lo, doc0)))
        aux = jnp.where(row < 4, aux, pltpu.roll(aux, T - 128, 1))
        for n in range(8):
            kv_ref[1, j, n * 64:(n + 1) * 64] = vt[j * HD:(j + 1) * HD, n * 128:(n + 1) * 128]
        for t in range(2):
            at = t * 512
            two = jnp.concatenate([aux[:, at:at + 128], aux[:, at + 256:at + 384]], axis=0)
            kv_ref[t, j, HALF:] = two.astype(BF)


def exchange_kernel(
    q_h, k_h, v_h, g_h, d_h, n_h, wo_h, res_h, wu_h, wd_h, qin, kvall, woall, resin, gainall, wu4, wd4,
    q_v, k_v, v_v, g_v, d_v, n_v, wo, res, wu, wd, qt, kv, gain, in_sem,
    qs, qr, ks, rr, s_sib, r_sib, s_r, s_l,
    wl, w_sib, wr_sib, w_s_r, w_s_l, w_r, es, er, gs, gr,
    u_s_r, u_s_l, u_r, d_s_r, d_s_l, d_r, ul,
):
    z, y, x, c = place()
    sp, tp = z * 4 + y, x * 2 + c
    sib = dev(z, y, x, 1 - c)
    yp, ym, y2 = up(y, 1), up(y, 3), up(y, 2)
    xp, xm, x2 = up(x, 1), up(x, 3), up(x, 2)

    loads = [
        pltpu.make_async_copy(src, dst, in_sem.at[n])
        for n, (src, dst) in enumerate(
            zip((k_h, v_h, g_h, d_h, n_h, q_h, wo_h, res_h, wu_h, wd_h), (k_v, v_v, g_v, d_v, n_v, q_v, wo, res, wu, wd))
        )
    ]
    for load in loads:
        load.start()
    barrier = pltpu.get_barrier_semaphore()
    cs = lax.div(z, 2)
    for zs in range(4):
        @pl.when(jnp.logical_not((z == zs) & (c == cs)))
        def _():
            signal(barrier, dev(zs, y, x, cs))

    for k in range(1, 8):
        signal(barrier, (sp, lax.rem(tp + k, 8)))
    signal(barrier, dev(z, yp, x, c))
    signal(barrier, dev(z, ym, x, c))
    zp, zm = up(z, 1), up(z, 3)
    signal(barrier, dev(zp, y, x, c))
    signal(barrier, dev(zm, y, x, c))
    for load in loads:
        load.wait()
    pack_kernel(q_v, k_v, v_v, g_v, d_v, n_v, qt, kv, gain)
    pl.semaphore_wait(barrier, jnp.where(c == cs, 14, 15))

    def guarded(is_self, local, remote):
        @pl.when(is_self)
        def _():
            local.start()

        @pl.when(jnp.logical_not(is_self))
        def _():
            remote.start()

    pending = []
    for j in range(2):
        zt = 2 * c + j
        for t in range(2):
            mine = (zt == z) & (c == t)
            src, dst = kv.at[t, j], kvall.at[t, sp]
            remote = send(src, dst, ks.at[2 * t + j], rr.at[sp], dev(zt, y, x, t))
            guarded(mine, pltpu.make_async_copy(src, dst, rr.at[sp]), remote)
            pending.append((mine, remote))
    for j in range(2):
        zt = 2 * c + j
        for hf in range(2):
            ct = lax.rem(hf + z, 2)
            mine = (zt == z) & (ct == c)
            src, dst = qt.at[j, :, pl.ds(hf * HALF, HALF)], qin.at[z]
            remote = send(src, dst, qs.at[2 * j + hf], qr.at[z], dev(zt, y, x, ct))
            guarded(mine, pltpu.make_async_copy(src, dst, qr.at[z]), remote)
            pending.append((mine, remote))

    done = []

    def wrows(xs, half):
        return pl.ds((2 * xs + c) * 128 + half * 64, 64)

    def go(copy):
        copy.start()
        done.append(copy)

    ring_w = Ring(go, x, lambda i, half: woall.at[wrows(i, half)], dev(z, y, xp, c), dev(z, y, xm, c),
                  w_s_r, w_s_l, w_r, sib, w_sib, wr_sib)
    ring_u = Ring(go, y, lambda i, half: wu4.at[i, pl.ds(half * 64, 64)], dev(z, yp, x, c), dev(z, ym, x, c),
                  u_s_r, u_s_l, u_r)
    ring_d = Ring(go, z, lambda i, half: wd4.at[i, pl.ds(half * HALF, HALF)], dev(zp, y, x, c), dev(zm, y, x, c),
                  d_s_r, d_s_l, d_r)
    own_w = [
        pltpu.make_async_copy(wo, woall.at[pl.ds(pl.multiple_of(tp * 128, 128), 128)], wl.at[0]),
        pltpu.make_async_copy(wu, wu4.at[y], ul.at[0]),
        pltpu.make_async_copy(wd, wd4.at[z], ul.at[1]),
    ]
    for loc in own_w:
        loc.start()
    ring_w.start(lambda half: wo.at[pl.ds(half * 64, 64)])

    own_e = pltpu.make_async_copy(res.at[pl.ds(pl.multiple_of(tp * 128, 128), 128)],
                                  resin.at[:, pl.ds(pl.multiple_of(tp * 256, 256), 256)], er.at[tp])
    own_e.start()
    own_g = pltpu.make_async_copy(gain, gainall.at[:, pl.ds(pl.multiple_of(tp * 256, 256), 256)], gr.at[tp])
    own_g.start()
    for k in range(1, 8):
        to = lax.rem(tp + k, 8)
        cols = pl.ds(pl.multiple_of(tp * 256, 256), 256)
        go(send(res.at[pl.ds(pl.multiple_of(to * 128, 128), 128)], resin.at[:, cols], es.at[k], er.at[tp], (sp, to)))
        go(send(gain, gainall.at[:, cols], gs.at[k], gr.at[tp], (sp, to)))

    def arrived(b):
        send(kvall.at[c, b], kvall.at[c, b], s_sib.at[b], rr.at[b], sib).wait_recv()
        go(send(kvall.at[c, b], kvall.at[c, b], s_sib.at[b], r_sib.at[b], sib))

    def right(b):
        go(send(kvall.at[c, b], kvall.at[c, b], s_r.at[b], rr.at[b], dev(z, yp, x, c)))

    def left(b):
        go(send(kvall.at[c, b], kvall.at[c, b], s_l.at[b], rr.at[b], dev(z, ym, x, c)))

    zs = [z, up(z, 1), up(z, 3), up(z, 2)]

    def near(r):
        b = zs[r] * 4 + y
        arrived(b)
        right(b)
        left(b)

    def next_to(r):
        b = zs[r] * 4 + ym
        arrived(b)
        if r in (0, 2):
            right(b)
        b = zs[r] * 4 + yp
        arrived(b)
        if r in (1, 3):
            left(b)

    near(0)
    ring_d.start(lambda half: wd.at[pl.ds(half * HALF, HALF)])
    ring_u.start(lambda half: wu.at[pl.ds(half * 64, 64)])
    near(1)
    near(2)
    next_to(0)
    ring_w.middle(0)
    near(3)
    ring_u.middle(0)
    ring_d.middle(0)
    next_to(1)
    next_to(2)
    ring_w.middle(1)
    ring_u.middle(1)
    ring_d.middle(1)
    next_to(3)
    for r in range(4):
        arrived(zs[r] * 4 + y2)
    ring_w.last()
    ring_u.last()
    ring_d.last()

    for b in range(16):
        send(kvall.at[1 - c, b], kvall.at[1 - c, b], s_sib.at[b], r_sib.at[b], sib).wait_recv()
    for n in range(8):
        rows = pl.ds((2 * (n // 2) + (1 - c)) * 128 + (n % 2) * 64, 64)
        send(woall.at[rows], woall.at[rows], w_sib.at[n], wr_sib.at[n], sib).wait_recv()
    for i in range(4):
        send(qin.at[i], qin.at[i], qs.at[0], qr.at[i], sib).wait_recv()
    for n in range(8):
        cols = pl.ds(n * 256, 256)
        send(resin.at[:, cols], resin.at[:, cols], es.at[0], er.at[n], sib).wait_recv()
        send(gainall.at[:, cols], gainall.at[:, cols], gs.at[0], gr.at[n], sib).wait_recv()
    for loc in own_w:
        loc.wait()
    for mine, remote in pending:
        @pl.when(jnp.logical_not(mine))
        def _():
            remote.wait_send()
    for copy in done:
        copy.wait_send()


def exchange(*args):
    return pl.pallas_call(
        exchange_kernel,
        out_shape=(
            sds((4, HD, HALF), BF),
            sds((2, 16, ITEM, 128), BF),
            sds((1024, D), BF),
            sds((128, D), BF),
            sds((8, D), F32),
            sds((4, 128, 1024), BF),
            sds((4, T, 128), BF),
        ),
        in_specs=[HB] * 10,
        out_specs=(HB,) * 7,
        scratch_shapes=[
            pltpu.VMEM((T, 128), BF),
            pltpu.VMEM((T, 128), BF),
            pltpu.VMEM((T, 128), BF),
            pltpu.VMEM((2, T), F32),
            pltpu.VMEM((1, T), jnp.int32),
            pltpu.VMEM((256,), BF),
            pltpu.VMEM((128, D), BF),
            pltpu.VMEM((T, 256), BF),
            pltpu.VMEM((128, 1024), BF),
            pltpu.VMEM((1024, 128), BF),
            pltpu.VMEM((2, HD, T), BF),
            pltpu.VMEM((2, 2, ITEM, 128), BF),
            pltpu.VMEM((8, 256), F32),
            DMA((10,)),
            DMA((4,)), DMA((4,)), DMA((4,)), DMA((16,)), DMA((16,)), DMA((16,)), DMA((16,)), DMA((16,)),
            DMA((2,)), DMA((8,)), DMA((8,)), DMA((8,)), DMA((8,)), DMA((8,)),
            DMA((8,)), DMA((8,)), DMA((8,)), DMA((8,)),
            DMA((8,)), DMA((8,)), DMA((8,)), DMA((8,)), DMA((8,)), DMA((8,)), DMA((2,)),
        ],
        compiler_params=pltpu.CompilerParams(has_side_effects=True, collective_id=0),
        cost_estimate=pl.CostEstimate(flops=20_000_000_000, bytes_accessed=16_000_000, transcendentals=0),
        name="exchange",
    )(*args)


QW = 256
NS = HALF // QW
PARTS = (slice(0, 256), slice(256, 512))


def in_turn(*streams):
    streams = list(streams)
    while streams:
        for stream in list(streams):
            if next(stream, streams) is streams:
                streams.remove(stream)


def attend_kernel(q_h, kv_h, o_ref, q_ref, kv_ref, aux_ref, in_sem, kv_sem, pieces, gmat, w_ref, *scr):
    z, y, x, c = place()
    main = pl.ds(0, HALF)
    loads = [
        pltpu.make_async_copy(kv_h.at[0, :, pl.ds(HALF, 16)], aux_ref.at[0], in_sem.at[0]),
        pltpu.make_async_copy(kv_h.at[1, :, pl.ds(HALF, 16)], aux_ref.at[1], in_sem.at[2]),
        pltpu.make_async_copy(q_h, q_ref, in_sem.at[1]),
    ]

    def blocks(t, i):
        four = pl.ds(4 * i, 4)
        return pltpu.make_async_copy(kv_h.at[t, four, main], kv_ref.at[t, four], kv_sem.at[t, i])

    for load in loads:
        load.start()
    for i in range(4):
        for t in range(2):
            blocks(t, i).start()
    loads[0].wait()
    loads[1].wait()
    s_refs, accs, tops, shrinks = scr[:NS], scr[NS:2 * NS], scr[2 * NS:3 * NS], scr[3 * NS:]
    ones = jnp.ones((16, HALF), BF)
    count = jnp.zeros((1, 128), F32)
    for b in range(16):
        for t in range(2):
            a = aux_ref[t, b].astype(F32)
            for k in range(4):
                hf, at = t, k * 128
                count = count + a[k * 4 + 3:k * 4 + 4]
                pieces[b * 8 + hf * 4:b * 8 + hf * 4 + 4, at:at + 128] = a[k * 4:k * 4 + 4]
    docs0 = jnp.sum(count).astype(jnp.int32)
    gmat[...] = pieces[...].T.astype(BF)
    loads[2].wait()
    row = lax.broadcasted_iota(jnp.int32, (128, QW), 0)
    unit_of_row, piece_of_row = row // 4, row % 4

    def tile(i, carry):
        for t in range(2):
            blocks(t, i).wait()
        hq = 2 * (4 * i + y) + lax.rem(c + i, 2)
        start = jnp.where(hq * HALF >= docs0, lax.div(docs0, HALF), 0)
        q_pos = hq * HALF + lax.broadcasted_iota(jnp.int32, (1, HALF), 1)
        doc1 = jnp.where(q_pos >= docs0, -BIG, 0.0)
        for k in range(NS):
            cols = slice(k * QW, (k + 1) * QW)
            w_ref[:, cols] = jnp.where(piece_of_row == 3, doc1[:, cols], -1.0)

        def scores(k, u, first):
            cols = slice(k * QW, (k + 1) * QW)
            q = q_ref[i, :, cols]
            none = jnp.zeros_like(q)
            b, low = lax.div(u, 2), lax.rem(u, 2) == 0
            sel = jnp.where(unit_of_row == u, w_ref[:, cols], 0.0).astype(BF)
            rhs = jnp.concatenate([jnp.where(low, q, none), jnp.where(low, none, q), sel], axis=0)
            largest = []
            for rows in PARTS:
                lhs = jnp.concatenate([kv_ref[0, b, rows, :], gmat[rows, :]], axis=1)
                s = jnp.dot(lhs, rhs, preferred_element_type=F32)
                if first:
                    key = rows.start + lax.broadcasted_iota(jnp.int32, s.shape, 0)
                    s = jnp.where(key <= k * QW + lax.broadcasted_iota(jnp.int32, s.shape, 1), s, far_below)
                s_refs[k][rows, :] = s
                largest.append(jnp.max(s, axis=0, keepdims=True))
                yield
            new = functools.reduce(jnp.maximum, largest)
            if not first:
                old = tops[k][...]
                new = jnp.maximum(old, new)
                shrinks[k][...] = jnp.exp(old - new)
            tops[k][...] = new

        def weigh(k, u, first):
            b, hf = lax.div(u, 2), lax.rem(u, 2)
            vt = jnp.concatenate(
                [kv_ref[1, b, pl.ds(pl.multiple_of(hf * 256 + n * 64, 64), 64), :] for n in range(4)], axis=1
            )
            vt = jnp.concatenate([vt, ones], axis=0)
            most = tops[k][...]
            product = None
            for rows in PARTS:
                p = jnp.exp(s_refs[k][rows, :] - most).astype(BF)
                term = jnp.dot(vt[:, rows], p, preferred_element_type=F32)
                product = term if product is None else product + term
                yield
            accs[k][...] = product if first else accs[k][...] * shrinks[k][...] + product

        ahead = jnp.maximum(hq - 1, 0)
        in_turn(scores(0, hq, True))
        in_turn(scores(1, hq, True), weigh(0, hq, True))
        in_turn(scores(0, jnp.minimum(start, ahead), False), weigh(1, hq, True))

        def step(u, carry):
            in_turn(scores(1, u, False), weigh(0, u, False))
            in_turn(scores(0, jnp.minimum(u + 1, ahead), False), weigh(1, u, False))
            return carry

        lax.fori_loop(start, hq, step, 0)
        for k in range(NS):
            total = accs[k][...]
            o_ref[i, :, k * QW:(k + 1) * QW] = (total[:HD] / total[HD:HD + 1]).astype(BF)
        return carry

    lax.fori_loop(0, 4, tile, 0)


def attend(q, kv):
    return pl.pallas_call(
        attend_kernel,
        out_shape=sds((4, HD, HALF), BF),
        in_specs=[HB, HB],
        out_specs=VM,
        scratch_shapes=[
            pltpu.VMEM((4, HD, HALF), BF),
            pltpu.VMEM((2, 16, HALF, 128), BF),
            pltpu.VMEM((2, 16, 16, 128), BF),
            DMA((3,)),
            DMA((2, 4)),
            pltpu.VMEM((128, HALF), F32),
            pltpu.VMEM((HALF, 128), BF),
            pltpu.VMEM((128, HALF), F32),
        ]
        + [pltpu.VMEM((HALF, QW), F32)] * NS
        + [pltpu.VMEM((80, QW), F32)] * NS
        + [pltpu.VMEM((1, QW), F32)] * (2 * NS),
        compiler_params=pltpu.CompilerParams(vmem_limit_bytes=66_500_000),
        cost_estimate=pl.CostEstimate(flops=20_000_000_000, bytes_accessed=8_000_000, transcendentals=0),
        name="attend",
    )(q, kv)


G = 4
ROWS = T // G
PIECE = 128 // G
A, B = pl.ds(0, ROWS // 2), pl.ds(ROWS // 2, ROWS // 2)


def tail_kernel(
    att_any, wo_any, res_any, gain_any, u0, um, upl, d0, dm, dpl, out,
    att, res, gain, a_in, wo, own, midb, wu, wd, normed, hidden, part, sibbuf, stage, hop_a, hop_b, from_l, from_r,
    w_sem, a_s, a_r, o_s, o_r, g_s, g_r, t_s, t_r,
):
    z, y, x, c = place()
    sp, tp = z * 4 + y, x * 2 + c
    sib = dev(z, y, x, 1 - c)
    xp, xm, x2 = up(x, 1), up(x, 3), up(x, 2)
    right, left = dev(z, y, xp, c), dev(z, y, xm, c)
    z_next, z_prev, y_next, y_prev = up(z, 1), up(z, 3), up(y, 1), up(y, 3)
    head = 4 * x + z

    barrier = pltpu.get_barrier_semaphore()
    cs = lax.rem(lax.div(tp, 4) + z, 2)
    for zs in range(4):
        for xs in range(4):
            @pl.when(jnp.logical_not((z == zs) & (x == xs) & (c == cs)))
            def _():
                signal(barrier, dev(zs, y, xs, cs))

    to_z = dev(z_next, y, x, c), dev(z_prev, y, x, c)
    to_y = dev(z, y_next, x, c), dev(z, y_prev, x, c)
    for device in (sib, right, left, *to_z, *to_y):
        signal(barrier, device)
    def wu_rows(zz, lo, n):
        return wu.at[pl.ds(pl.multiple_of(zz * 512 + lo, 256), n)]

    loads = [
        pltpu.make_async_copy(att_any, att, w_sem.at[7]),
        pltpu.make_async_copy(wo_any, wo, w_sem.at[0]),
        pltpu.make_async_copy(res_any, res, w_sem.at[8]),
        pltpu.make_async_copy(gain_any, gain, w_sem.at[9]),
        pltpu.make_async_copy(u0, wu_rows(z, 0, 512), w_sem.at[1]),
        pltpu.make_async_copy(um, wu_rows(z_prev, 0, 512), w_sem.at[2]),
        pltpu.make_async_copy(upl, wu_rows(z_next, 0, 512), w_sem.at[3]),
        pltpu.make_async_copy(d0, wd.at[y], w_sem.at[4]),
        pltpu.make_async_copy(dm, wd.at[y_prev], w_sem.at[5]),
        pltpu.make_async_copy(dpl, wd.at[y_next], w_sem.at[6]),
    ]
    for load in loads:
        load.start()
    pl.semaphore_wait(barrier, jnp.where(lax.div(x, 2) == lax.rem(c + z, 2), 22, 23))
    loads[0].wait()

    done = []

    def go(copy):
        copy.start()
        done.append(copy)

    pending = []
    for i in range(4):
        hf = lax.rem(c + i, 2)
        for k in range(4):
            to = 4 * hf + k
            mine = (z == i) & (to == tp)
            src = att.at[i, :, pl.ds(k * 128, 128)]
            dst = a_in.at[pl.ds(pl.multiple_of(head * HD, HD), HD)]
            remote = send(src, dst, a_s.at[4 * i + k], a_r.at[head], (i * 4 + y, to))
            local = pltpu.make_async_copy(src, dst, a_r.at[head])

            @pl.when(mine)
            def _():
                local.start()

            @pl.when(jnp.logical_not(mine))
            def _():
                remote.start()

            pending.append((mine, remote))

    go(send(um.at[pl.ds(0, 256)], wu_rows(z_prev, 0, 256), o_s.at[0], o_r.at[0], to_z[0]))
    go(send(upl.at[pl.ds(256, 256)], wu_rows(z_next, 256, 256), o_s.at[1], o_r.at[1], to_z[1]))
    go(send(dm.at[pl.ds(0, 2)], wd.at[y_prev, pl.ds(0, 2)], o_s.at[2], o_r.at[2], to_y[0]))
    go(send(dpl.at[pl.ds(2, 2)], wd.at[y_next, pl.ds(2, 2)], o_s.at[3], o_r.at[3], to_y[1]))

    for h in range(16):
        rows = pl.ds(h * HD, HD)
        send(a_in.at[rows], a_in.at[rows], a_s.at[0], a_r.at[h], sib).wait_recv()
    loads[1].wait()
    loads[2].wait()
    a = a_in[...].astype(F32).T.astype(BF)
    for n in range(4):
        cols = slice(n * 512, (n + 1) * 512)
        mixed = jnp.dot(a, wo[:, cols], preferred_element_type=F32)
        own[:, cols] = (res[:, cols].astype(F32) + mixed).astype(BF)

    def piece(g, xs, cc, lo=0, n=PIECE):
        return midb.at[g, pl.ds(pl.multiple_of((2 * xs + cc) * PIECE + lo, PIECE // 2), n)]

    def pass_on(g, at, k, device, kr=None):
        go(send(at, at, g_s.at[k, g], g_r.at[k if kr is None else kr, g], device))

    def came(g, at, k):
        send(at, at, g_s.at[k, g], g_r.at[k, g], sib).wait_recv()

    def gather_own(g):
        src, dst = own.at[pl.ds(g * PIECE, PIECE)], piece(g, x, c)
        go(send(src, dst, g_s.at[0, g], g_r.at[0, g], right))
        go(send(src, dst, g_s.at[1, g], g_r.at[1, g], left))
        go(send(src, dst, g_s.at[4, g], g_r.at[4, g], sib))
        midb[g, pl.ds(pl.multiple_of(tp * PIECE, PIECE), PIECE), :] = own[g * PIECE:(g + 1) * PIECE, :]

    def gather_near(g):
        came(g, piece(g, xm, c), 0)
        pass_on(g, piece(g, xm, c, 0, PIECE // 2), 2, right)
        pass_on(g, piece(g, xm, c), 5, sib)
        came(g, piece(g, xp, c), 1)
        pass_on(g, piece(g, xp, c, PIECE // 2, PIECE // 2), 3, left)
        pass_on(g, piece(g, xp, c), 6, sib)

    def gather_far(g):
        for k in (0, 1):
            at = piece(g, x2, c, k * (PIECE // 2), PIECE // 2)
            came(g, at, 2 + k)
            pass_on(g, at, 7 + k, sib)

    def gather_rest(g):
        came(g, piece(g, x, 1 - c), 4)
        came(g, piece(g, xm, 1 - c), 5)
        came(g, piece(g, xp, 1 - c), 6)
        came(g, piece(g, x2, 1 - c, 0, PIECE // 2), 7)
        came(g, piece(g, x2, 1 - c, PIECE // 2, PIECE // 2), 8)

    def feed(g):
        wide = midb[g].astype(F32)
        inv = lax.rsqrt(jnp.mean(wide * wide, axis=-1, keepdims=True) + eps)
        normed[...] = (wide * inv * gain[0:1, :]).astype(BF)

        def lift(n, carry):
            cols = pl.ds(pl.multiple_of(n * 256, 256), 256)
            h = jnp.dot(normed[...], wu[:, cols], preferred_element_type=F32)
            hidden[:, cols] = jnp.square(jnp.maximum(h, 0.0)).astype(BF)
            return carry

        lax.fori_loop(0, 4, lift, 0)

        def drop(core):
            def one(k, carry):
                yy = 2 * core + k
                cols = pl.multiple_of(k * 128, 128)
                for zp in (0, 2):
                    rhs = jnp.concatenate([wd[yy, zp], wd[yy, zp + 1]], axis=1)
                    term = jnp.dot(hidden[...], rhs, preferred_element_type=F32).astype(BF)
                    part[g, core, zp, :, pl.ds(cols, 128)] = term[:, :128]
                    part[g, core, zp + 1, :, pl.ds(cols, 128)] = term[:, 128:]
                return carry

            lax.fori_loop(0, 2, one, 0)

        drop(1 - c)
        go(send(part.at[g, 1 - c], sibbuf.at[g], t_s.at[0, g], t_r.at[0, g], sib))
        drop(c)

    def both(g, rel, rows):
        xt = up(x, rel)
        return part[g, c, xt, rows, :].astype(F32) + sibbuf[g, xt, rows, :].astype(F32)

    def scatter_first(g):
        send(sibbuf.at[g], sibbuf.at[g], t_s.at[0, g], t_r.at[0, g], sib).wait_recv()
        stage[g, 2] = both(g, 2, pl.ds(0, ROWS)).astype(BF)
        go(send(stage.at[g, 2, A], hop_a.at[g], t_s.at[1, g], t_r.at[1, g], right))
        go(send(stage.at[g, 2, B], hop_b.at[g], t_s.at[2, g], t_r.at[2, g], left))
        stage[g, 1, B, :] = both(g, 1, B).astype(BF)
        go(send(stage.at[g, 1, B], from_l.at[g, B], t_s.at[3, g], t_r.at[3, g], right))
        stage[g, 3, A, :] = both(g, 3, A).astype(BF)
        go(send(stage.at[g, 3, A], from_r.at[g, A], t_s.at[4, g], t_r.at[4, g], left))

    def scatter_second(g):
        send(hop_a.at[g], hop_a.at[g], t_s.at[1, g], t_r.at[1, g], sib).wait_recv()
        stage[g, 1, A, :] = (both(g, 1, A) + hop_a[g].astype(F32)).astype(BF)
        go(send(stage.at[g, 1, A], from_l.at[g, A], t_s.at[5, g], t_r.at[5, g], right))
        send(hop_b.at[g], hop_b.at[g], t_s.at[2, g], t_r.at[2, g], sib).wait_recv()
        stage[g, 3, B, :] = (both(g, 3, B) + hop_b[g].astype(F32)).astype(BF)
        go(send(stage.at[g, 3, B], from_r.at[g, B], t_s.at[6, g], t_r.at[6, g], left))

    def scatter_third(g):
        for k, buf, rows in ((3, from_l, B), (4, from_r, A), (5, from_l, A), (6, from_r, B)):
            send(buf.at[g, rows], buf.at[g, rows], t_s.at[k, g], t_r.at[k, g], sib).wait_recv()
        for n in range(8):
            rows = pl.ds(n * PIECE, PIECE)
            total = both(g, 0, rows) + from_l[g, rows, :].astype(F32) + from_r[g, rows, :].astype(F32)
            mid = midb[g, rows, pl.ds(pl.multiple_of(tp * 256, 256), 256)].astype(F32)
            out[n * 128 + g * PIECE:n * 128 + (g + 1) * PIECE, :] = (mid + total).astype(BF)

    gather_own(0)
    gather_own(1)
    gather_near(0)
    gather_own(2)
    gather_near(1)
    gather_own(3)
    gather_far(0)
    gather_rest(0)
    for load in loads[3:]:
        load.wait()
    for k, at in ((0, wu_rows(up(z, 2), 0, 256)), (1, wu_rows(up(z, 2), 256, 256)),
                  (2, wd.at[up(y, 2), pl.ds(0, 2)]), (3, wd.at[up(y, 2), pl.ds(2, 2)])):
        send(at, at, o_s.at[k], o_r.at[k], sib).wait_recv()
    feed(0)
    gather_near(2)
    gather_far(1)
    gather_rest(1)
    gather_near(3)
    scatter_first(0)
    feed(1)
    gather_far(2)
    gather_rest(2)
    gather_far(3)
    scatter_first(1)
    scatter_second(0)
    feed(2)
    gather_rest(3)
    scatter_first(2)
    scatter_second(1)
    feed(3)
    scatter_second(2)
    scatter_first(3)
    scatter_third(0)
    scatter_third(1)
    scatter_second(3)
    scatter_third(2)
    scatter_third(3)
    for mine, remote in pending:
        @pl.when(jnp.logical_not(mine))
        def _():
            remote.wait_send()
    for copy in done:
        copy.wait_send()


def tail(att, wo, res, gain, ups, downs):
    return pl.pallas_call(
        tail_kernel,
        out_shape=sds((T, 256), BF),
        in_specs=[HB] * 10,
        out_specs=VM,
        scratch_shapes=[
            pltpu.VMEM((4, HD, HALF), BF),
            pltpu.VMEM((128, D), BF),
            pltpu.VMEM((8, D), F32),
            pltpu.VMEM((1024, 128), BF),
            pltpu.VMEM((1024, D), BF),
            pltpu.VMEM((128, D), BF),
            pltpu.VMEM((G, ROWS, D), BF),
            pltpu.VMEM((D, 1024), BF),
            pltpu.VMEM((4, 4, 1024, 128), BF),
            pltpu.VMEM((ROWS, D), BF),
            pltpu.VMEM((ROWS, 1024), BF),
            pltpu.VMEM((G, 2, 4, ROWS, 256), BF),
            pltpu.VMEM((G, 4, ROWS, 256), BF),
            pltpu.VMEM((G, 4, ROWS, 256), BF),
            pltpu.VMEM((G, ROWS // 2, 256), BF),
            pltpu.VMEM((G, ROWS // 2, 256), BF),
            pltpu.VMEM((G, ROWS, 256), BF),
            pltpu.VMEM((G, ROWS, 256), BF),
            DMA((10,)), DMA((16,)), DMA((16,)), DMA((4,)), DMA((4,)),
            DMA((9, G)), DMA((9, G)), DMA((7, G)), DMA((7, G)),
        ],
        compiler_params=pltpu.CompilerParams(
            has_side_effects=True, collective_id=1, vmem_limit_bytes=56 * 1024 * 1024
        ),
        cost_estimate=pl.CostEstimate(flops=20_000_000_000, bytes_accessed=8_000_000, transcendentals=0),
        name="tail",
    )(att, wo, res, gain, *ups, *downs)


def shifted(value, axis, step):
    def index(z, y):
        return (z % 4) * 4 + y % 4

    pairs = [
        (index(z, y), index(z + step, y) if axis == "z" else index(z, y + step)) for z in range(4) for y in range(4)
    ]
    return lax.ppermute(value, "sp", pairs)


def body(queries, keys, values, cum_gates, doc_ids, residual, w_out, norm_gain, w_up, w_down):
    qin, kvall, woall, resin, gain, u0, d0 = exchange(
        queries, keys, values, jnp.transpose(cum_gates), doc_ids.reshape(1, T), norm_gain, w_out, residual, w_up, w_down
    )
    um, upl = shifted(u0, "z", 1), shifted(u0, "z", -1)
    dm, dpl = shifted(d0, "y", 1), shifted(d0, "y", -1)
    att = attend(qin, kvall)
    ups = [u.reshape(512, 1024) for u in (u0, um, upl)]
    return tail(att, woall, resin, gain, ups, (d0, dm, dpl))


def solution(mesh):
    in_specs = (
        P("sp", "tp"),
        P("sp", "tp"),
        P("sp", "tp"),
        P("sp", "tp"),
        P("sp"),
        P("sp", "tp"),
        P("tp", None),
        P("tp"),
        P("sp", "tp"),
        P("tp", "sp"),
    )
    return jax.shard_map(body, mesh=mesh, in_specs=in_specs, out_specs=P("sp", "tp"), check_vma=False)
```

```python
import functools

import jax
import jax.numpy as jnp
from jax import lax
from jax.experimental import pallas as pl
from jax.experimental.pallas import tpu as pltpu
from jax.sharding import PartitionSpec as P

D = 2048
HD = 64
T = 1024
HALF = 512
ITEM = 528
eps = 1e-06
far_below = -1e30
BIG = 8192.0
MESH = pl.DeviceIdType.MESH
BF = jnp.bfloat16
F32 = jnp.float32
VM = pl.BlockSpec(memory_space=pltpu.VMEM)
HB = pl.BlockSpec(memory_space=pl.ANY)
DMA = pltpu.SemaphoreType.DMA


def sds(shape, dtype):
    return jax.ShapeDtypeStruct(shape, dtype)


def place():
    sp, tp = lax.axis_index("sp"), lax.axis_index("tp")
    return lax.div(sp, 4), lax.rem(sp, 4), lax.div(tp, 2), lax.rem(tp, 2)


def dev(z, y, x, c):
    return (z * 4 + y, x * 2 + c)


def send(src, dst, ssem, rsem, device):
    return pltpu.make_async_remote_copy(
        src_ref=src, dst_ref=dst, send_sem=ssem, recv_sem=rsem, device_id=device, device_id_type=MESH
    )


def up(v, k):
    return lax.rem(v + k, 4)


def signal(barrier, device):
    pl.semaphore_signal(barrier, inc=1, device_id=device, device_id_type=MESH)


class Ring:
    def __init__(self, go, me, slot, right, left, s_r, s_l, r, sib=None, s_sib=None, r_sib=None):
        self.go, self.me, self.slot, self.right, self.left = go, me, slot, right, left
        self.s_r, self.s_l, self.r = s_r, s_l, r
        self.sib, self.s_sib, self.r_sib = sib, s_sib, r_sib

    def start(self, src, order=(0, 1)):
        for half in order:
            n, dst = 2 * self.me + half, self.slot(self.me, half)
            self.go(send(src(half), dst, self.s_r.at[n], self.r.at[n], self.right))
            self.go(send(src(half), dst, self.s_l.at[n], self.r.at[n], self.left))
            if self.s_sib is not None:
                self.go(send(src(half), dst, self.s_sib.at[n], self.r_sib.at[n], self.sib))

    def take(self, i, half, forward=0):
        n, at = 2 * i + half, self.slot(i, half)
        send(at, at, self.s_r.at[n], self.r.at[n], self.right).wait_recv()
        if forward > 0:
            self.go(send(at, at, self.s_r.at[n], self.r.at[n], self.right))
        if forward < 0:
            self.go(send(at, at, self.s_l.at[n], self.r.at[n], self.left))
        if self.s_sib is not None:
            self.go(send(at, at, self.s_sib.at[n], self.r_sib.at[n], self.sib))

    def middle(self, half):
        lo, hi = up(self.me, 3), up(self.me, 1)
        if half == 0:
            self.take(lo, 0, 1)
            self.take(hi, 0)
        else:
            self.take(hi, 1, -1)
            self.take(lo, 1)

    def last(self):
        self.take(up(self.me, 2), 0)
        self.take(up(self.me, 2), 1)


def pack_kernel(q_ref, k_ref, v_ref, g_ref, d_ref, n_ref, qt_ref, kv_ref, gain_ref):
    gain_ref[...] = jnp.broadcast_to(n_ref[...].astype(F32)[None], (8, 256))
    qt = (q_ref[...].astype(F32) * (HD ** -0.5)).T.astype(BF)
    qt_ref[0] = qt[:HD]
    qt_ref[1] = qt[HD:]
    k_lo, k_hi = k_ref[:HALF].astype(F32), k_ref[HALF:].astype(F32)
    first = lax.broadcasted_iota(jnp.int32, (HALF, 128), 1) < HD
    kv_ref[0, 0, :HALF] = jnp.where(first, k_lo, pltpu.roll(k_hi, HD, 1)).astype(BF)
    kv_ref[0, 1, :HALF] = jnp.where(first, pltpu.roll(k_lo, HD, 1), k_hi).astype(BF)
    vt = v_ref[...].astype(F32).T.astype(BF)
    row = lax.broadcasted_iota(jnp.int32, (8, T), 0)
    kind = lax.rem(row, 4)
    doc0 = 1.0 - d_ref[...].astype(F32)
    for j in range(2):
        g = g_ref[j:j + 1, :]
        hi = g.astype(BF).astype(F32)
        mid = (g - hi).astype(BF).astype(F32)
        lo = (g - hi) - mid
        aux = jnp.where(kind == 0, hi, jnp.where(kind == 1, mid, jnp.where(kind == 2, lo, doc0)))
        aux = jnp.where(row < 4, aux, pltpu.roll(aux, T - 128, 1))
        for n in range(8):
            kv_ref[1, j, n * 64:(n + 1) * 64] = vt[j * HD:(j + 1) * HD, n * 128:(n + 1) * 128]
        for t in range(2):
            at = t * 512
            two = jnp.concatenate([aux[:, at:at + 128], aux[:, at + 256:at + 384]], axis=0)
            kv_ref[t, j, HALF:] = two.astype(BF)


def exchange_kernel(
    q_h, k_h, v_h, g_h, d_h, n_h, wo_h, res_h, wu_h, wd_h, qin, kv_out, woall, resin, gainall, wu4, wd4,
    q_v, k_v, v_v, g_v, d_v, n_v, wo, res, wu, wd, qt, kv, gain, kvall, in_sem, out_sem,
    qs, qr, ks, rr, s_sib, r_sib, s_r, s_l,
    wl, w_sib, wr_sib, w_s_r, w_s_l, w_r, es, er, gs, gr,
    u_s_r, u_s_l, u_r, d_s_r, d_s_l, d_r, ul,
):
    z, y, x, c = place()
    sp, tp = z * 4 + y, x * 2 + c
    sib = dev(z, y, x, 1 - c)
    yp, ym, y2 = up(y, 1), up(y, 3), up(y, 2)
    xp, xm, x2 = up(x, 1), up(x, 3), up(x, 2)

    loads = [
        pltpu.make_async_copy(src, dst, in_sem.at[n])
        for n, (src, dst) in enumerate(
            zip((k_h, v_h, g_h, d_h, n_h, q_h, wo_h, res_h, wu_h, wd_h), (k_v, v_v, g_v, d_v, n_v, q_v, wo, res, wu, wd))
        )
    ]
    for load in loads:
        load.start()
    barrier = pltpu.get_barrier_semaphore()
    cs = lax.div(z, 2)
    for zs in range(4):
        @pl.when(jnp.logical_not((z == zs) & (c == cs)))
        def _():
            signal(barrier, dev(zs, y, x, cs))

    for k in range(1, 8):
        signal(barrier, (sp, lax.rem(tp + k, 8)))
    signal(barrier, dev(z, yp, x, c))
    signal(barrier, dev(z, ym, x, c))
    zp, zm = up(z, 1), up(z, 3)
    signal(barrier, dev(zp, y, x, c))
    signal(barrier, dev(zm, y, x, c))
    for load in loads:
        load.wait()
    pack_kernel(q_v, k_v, v_v, g_v, d_v, n_v, qt, kv, gain)
    pl.semaphore_wait(barrier, jnp.where(c == cs, 14, 15))

    def guarded(is_self, local, remote):
        @pl.when(is_self)
        def _():
            local.start()

        @pl.when(jnp.logical_not(is_self))
        def _():
            remote.start()

    pending = []
    for j in range(2):
        zt = 2 * c + j
        for t in range(2):
            mine = (zt == z) & (c == t)
            src, dst = kv.at[t, j], kvall.at[t, sp]
            remote = send(src, dst, ks.at[2 * t + j], rr.at[sp], dev(zt, y, x, t))
            guarded(mine, pltpu.make_async_copy(src, dst, rr.at[sp]), remote)
            pending.append((mine, remote))
    for j in range(2):
        zt = 2 * c + j
        for hf in range(2):
            ct = lax.rem(hf + z, 2)
            mine = (zt == z) & (ct == c)
            src, dst = qt.at[j, :, pl.ds(hf * HALF, HALF)], qin.at[z]
            remote = send(src, dst, qs.at[2 * j + hf], qr.at[z], dev(zt, y, x, ct))
            guarded(mine, pltpu.make_async_copy(src, dst, qr.at[z]), remote)
            pending.append((mine, remote))

    done = []

    def wrows(xs, half):
        return pl.ds((2 * xs + c) * 128 + half * 64, 64)

    def go(copy):
        copy.start()
        done.append(copy)

    ring_w = Ring(go, x, lambda i, half: woall.at[wrows(i, half)], dev(z, y, xp, c), dev(z, y, xm, c),
                  w_s_r, w_s_l, w_r, sib, w_sib, wr_sib)
    ring_u = Ring(go, y, lambda i, half: wu4.at[i, pl.ds(half * 64, 64)], dev(z, yp, x, c), dev(z, ym, x, c),
                  u_s_r, u_s_l, u_r)
    ring_d = Ring(go, z, lambda i, half: wd4.at[i, pl.ds(half * HALF, HALF)], dev(zp, y, x, c), dev(zm, y, x, c),
                  d_s_r, d_s_l, d_r)
    own_w = [
        pltpu.make_async_copy(wo, woall.at[pl.ds(pl.multiple_of(tp * 128, 128), 128)], wl.at[0]),
        pltpu.make_async_copy(wu, wu4.at[y], ul.at[0]),
        pltpu.make_async_copy(wd, wd4.at[z], ul.at[1]),
    ]
    for loc in own_w:
        loc.start()
    ring_w.start(lambda half: wo.at[pl.ds(half * 64, 64)])

    own_e = pltpu.make_async_copy(res.at[pl.ds(pl.multiple_of(tp * 128, 128), 128)],
                                  resin.at[:, pl.ds(pl.multiple_of(tp * 256, 256), 256)], er.at[tp])
    own_e.start()
    own_g = pltpu.make_async_copy(gain, gainall.at[:, pl.ds(pl.multiple_of(tp * 256, 256), 256)], gr.at[tp])
    own_g.start()
    for k in range(1, 8):
        to = lax.rem(tp + k, 8)
        cols = pl.ds(pl.multiple_of(tp * 256, 256), 256)
        go(send(res.at[pl.ds(pl.multiple_of(to * 128, 128), 128)], resin.at[:, cols], es.at[k], er.at[tp], (sp, to)))
        go(send(gain, gainall.at[:, cols], gs.at[k], gr.at[tp], (sp, to)))

    def drain(t, b):
        return pltpu.make_async_copy(kvall.at[t, b], kv_out.at[t, b], out_sem.at[t, b])

    def arrived(b):
        send(kvall.at[c, b], kvall.at[c, b], s_sib.at[b], rr.at[b], sib).wait_recv()
        drain(c, b).start()
        go(send(kvall.at[c, b], kvall.at[c, b], s_sib.at[b], r_sib.at[b], sib))

    def right(b):
        go(send(kvall.at[c, b], kvall.at[c, b], s_r.at[b], rr.at[b], dev(z, yp, x, c)))

    def left(b):
        go(send(kvall.at[c, b], kvall.at[c, b], s_l.at[b], rr.at[b], dev(z, ym, x, c)))

    zs = [z, up(z, 1), up(z, 3), up(z, 2)]

    def near(r):
        b = zs[r] * 4 + y
        arrived(b)
        right(b)
        left(b)

    def next_to(r):
        b = zs[r] * 4 + ym
        arrived(b)
        if r in (0, 2):
            right(b)
        b = zs[r] * 4 + yp
        arrived(b)
        if r in (1, 3):
            left(b)

    near(0)
    ring_d.start(lambda half: wd.at[pl.ds(half * HALF, HALF)])
    ring_u.start(lambda half: wu.at[pl.ds(half * 64, 64)])
    near(1)
    near(2)
    next_to(0)
    ring_w.middle(0)
    near(3)
    ring_u.middle(0)
    ring_d.middle(0)
    next_to(1)
    next_to(2)
    ring_w.middle(1)
    ring_u.middle(1)
    ring_d.middle(1)
    next_to(3)
    for r in range(4):
        arrived(zs[r] * 4 + y2)
    ring_w.last()
    ring_u.last()
    ring_d.last()

    for b in range(16):
        send(kvall.at[1 - c, b], kvall.at[1 - c, b], s_sib.at[b], r_sib.at[b], sib).wait_recv()
        drain(1 - c, b).start()
    for n in range(8):
        rows = pl.ds((2 * (n // 2) + (1 - c)) * 128 + (n % 2) * 64, 64)
        send(woall.at[rows], woall.at[rows], w_sib.at[n], wr_sib.at[n], sib).wait_recv()
    for i in range(4):
        send(qin.at[i], qin.at[i], qs.at[0], qr.at[i], sib).wait_recv()
    for n in range(8):
        cols = pl.ds(n * 256, 256)
        send(resin.at[:, cols], resin.at[:, cols], es.at[0], er.at[n], sib).wait_recv()
        send(gainall.at[:, cols], gainall.at[:, cols], gs.at[0], gr.at[n], sib).wait_recv()
    for loc in own_w:
        loc.wait()
    for b in range(16):
        drain(c, b).wait()
        drain(1 - c, b).wait()
    for mine, remote in pending:
        @pl.when(jnp.logical_not(mine))
        def _():
            remote.wait_send()
    for copy in done:
        copy.wait_send()


def exchange(*args):
    return pl.pallas_call(
        exchange_kernel,
        out_shape=(
            sds((4, HD, HALF), BF),
            sds((2, 16, ITEM, 128), BF),
            sds((1024, D), BF),
            sds((128, D), BF),
            sds((8, D), F32),
            sds((4, 128, 1024), BF),
            sds((4, T, 128), BF),
        ),
        in_specs=[HB] * 10,
        out_specs=(HB,) * 7,
        scratch_shapes=[
            pltpu.VMEM((T, 128), BF),
            pltpu.VMEM((T, 128), BF),
            pltpu.VMEM((T, 128), BF),
            pltpu.VMEM((2, T), F32),
            pltpu.VMEM((1, T), jnp.int32),
            pltpu.VMEM((256,), BF),
            pltpu.VMEM((128, D), BF),
            pltpu.VMEM((T, 256), BF),
            pltpu.VMEM((128, 1024), BF),
            pltpu.VMEM((1024, 128), BF),
            pltpu.VMEM((2, HD, T), BF),
            pltpu.VMEM((2, 2, ITEM, 128), BF),
            pltpu.VMEM((8, 256), F32),
            pltpu.VMEM((2, 16, ITEM, 128), BF),
            DMA((10,)),
            DMA((2, 16)),
            DMA((4,)), DMA((4,)), DMA((4,)), DMA((16,)), DMA((16,)), DMA((16,)), DMA((16,)), DMA((16,)),
            DMA((2,)), DMA((8,)), DMA((8,)), DMA((8,)), DMA((8,)), DMA((8,)),
            DMA((8,)), DMA((8,)), DMA((8,)), DMA((8,)),
            DMA((8,)), DMA((8,)), DMA((8,)), DMA((8,)), DMA((8,)), DMA((8,)), DMA((2,)),
        ],
        compiler_params=pltpu.CompilerParams(has_side_effects=True, collective_id=0),
        cost_estimate=pl.CostEstimate(flops=20_000_000_000, bytes_accessed=16_000_000, transcendentals=0),
        name="exchange",
    )(*args)


QW = 256
NS = HALF // QW
PARTS = (slice(0, 256), slice(256, 512))


def in_turn(*streams):
    streams = list(streams)
    while streams:
        for stream in list(streams):
            if next(stream, streams) is streams:
                streams.remove(stream)


def attend_kernel(q_h, kv_h, o_ref, q_ref, kv_ref, aux_ref, in_sem, kv_sem, pieces, gmat, w_ref, *scr):
    z, y, x, c = place()
    main = pl.ds(0, HALF)
    loads = [
        pltpu.make_async_copy(kv_h.at[0, :, pl.ds(HALF, 16)], aux_ref.at[0], in_sem.at[0]),
        pltpu.make_async_copy(kv_h.at[1, :, pl.ds(HALF, 16)], aux_ref.at[1], in_sem.at[2]),
        pltpu.make_async_copy(q_h, q_ref, in_sem.at[1]),
    ]

    def blocks(t, i):
        four = pl.ds(4 * i, 4)
        return pltpu.make_async_copy(kv_h.at[t, four, main], kv_ref.at[t, four], kv_sem.at[t, i])

    for load in loads:
        load.start()
    for i in range(4):
        for t in range(2):
            blocks(t, i).start()
    loads[0].wait()
    loads[1].wait()
    s_refs, accs, tops, shrinks = scr[:NS], scr[NS:2 * NS], scr[2 * NS:3 * NS], scr[3 * NS:]
    ones = jnp.ones((16, HALF), BF)
    count = jnp.zeros((1, 128), F32)
    for b in range(16):
        for t in range(2):
            a = aux_ref[t, b].astype(F32)
            for k in range(4):
                hf, at = t, k * 128
                count = count + a[k * 4 + 3:k * 4 + 4]
                pieces[b * 8 + hf * 4:b * 8 + hf * 4 + 4, at:at + 128] = a[k * 4:k * 4 + 4]
    docs0 = jnp.sum(count).astype(jnp.int32)
    gmat[...] = pieces[...].T.astype(BF)
    loads[2].wait()
    row = lax.broadcasted_iota(jnp.int32, (128, QW), 0)
    unit_of_row, piece_of_row = row // 4, row % 4

    def tile(i, carry):
        for t in range(2):
            blocks(t, i).wait()
        hq = 2 * (4 * i + y) + lax.rem(c + i, 2)
        start = jnp.where(hq * HALF >= docs0, lax.div(docs0, HALF), 0)
        q_pos = hq * HALF + lax.broadcasted_iota(jnp.int32, (1, HALF), 1)
        doc1 = jnp.where(q_pos >= docs0, -BIG, 0.0)
        for k in range(NS):
            cols = slice(k * QW, (k + 1) * QW)
            w_ref[:, cols] = jnp.where(piece_of_row == 3, doc1[:, cols], -1.0)

        def scores(k, u, first):
            cols = slice(k * QW, (k + 1) * QW)
            q = q_ref[i, :, cols]
            none = jnp.zeros_like(q)
            b, low = lax.div(u, 2), lax.rem(u, 2) == 0
            sel = jnp.where(unit_of_row == u, w_ref[:, cols], 0.0).astype(BF)
            rhs = jnp.concatenate([jnp.where(low, q, none), jnp.where(low, none, q), sel], axis=0)
            largest = []
            for rows in PARTS:
                lhs = jnp.concatenate([kv_ref[0, b, rows, :], gmat[rows, :]], axis=1)
                s = jnp.dot(lhs, rhs, preferred_element_type=F32)
                if first:
                    key = rows.start + lax.broadcasted_iota(jnp.int32, s.shape, 0)
                    s = jnp.where(key <= k * QW + lax.broadcasted_iota(jnp.int32, s.shape, 1), s, far_below)
                s_refs[k][rows, :] = s
                largest.append(jnp.max(s, axis=0, keepdims=True))
                yield
            new = functools.reduce(jnp.maximum, largest)
            if not first:
                old = tops[k][...]
                new = jnp.maximum(old, new)
                shrinks[k][...] = jnp.exp(old - new)
            tops[k][...] = new

        def weigh(k, u, first):
            b, hf = lax.div(u, 2), lax.rem(u, 2)
            vt = jnp.concatenate(
                [kv_ref[1, b, pl.ds(pl.multiple_of(hf * 256 + n * 64, 64), 64), :] for n in range(4)], axis=1
            )
            vt = jnp.concatenate([vt, ones], axis=0)
            most = tops[k][...]
            product = None
            for rows in PARTS:
                p = jnp.exp(s_refs[k][rows, :] - most).astype(BF)
                term = jnp.dot(vt[:, rows], p, preferred_element_type=F32)
                product = term if product is None else product + term
                yield
            accs[k][...] = product if first else accs[k][...] * shrinks[k][...] + product

        ahead = jnp.maximum(hq - 1, 0)
        in_turn(scores(0, hq, True))
        in_turn(scores(1, hq, True), weigh(0, hq, True))
        in_turn(scores(0, jnp.minimum(start, ahead), False), weigh(1, hq, True))

        def step(u, carry):
            in_turn(scores(1, u, False), weigh(0, u, False))
            in_turn(scores(0, jnp.minimum(u + 1, ahead), False), weigh(1, u, False))
            return carry

        lax.fori_loop(start, hq, step, 0)
        for k in range(NS):
            total = accs[k][...]
            o_ref[i, :, k * QW:(k + 1) * QW] = (total[:HD] / total[HD:HD + 1]).astype(BF)
        return carry

    lax.fori_loop(0, 4, tile, 0)


def attend(q, kv):
    return pl.pallas_call(
        attend_kernel,
        out_shape=sds((4, HD, HALF), BF),
        in_specs=[HB, HB],
        out_specs=VM,
        scratch_shapes=[
            pltpu.VMEM((4, HD, HALF), BF),
            pltpu.VMEM((2, 16, HALF, 128), BF),
            pltpu.VMEM((2, 16, 16, 128), BF),
            DMA((3,)),
            DMA((2, 4)),
            pltpu.VMEM((128, HALF), F32),
            pltpu.VMEM((HALF, 128), BF),
            pltpu.VMEM((128, HALF), F32),
        ]
        + [pltpu.VMEM((HALF, QW), F32)] * NS
        + [pltpu.VMEM((80, QW), F32)] * NS
        + [pltpu.VMEM((1, QW), F32)] * (2 * NS),
        compiler_params=pltpu.CompilerParams(vmem_limit_bytes=66_500_000),
        cost_estimate=pl.CostEstimate(flops=20_000_000_000, bytes_accessed=8_000_000, transcendentals=0),
        name="attend",
    )(q, kv)


G = 4
ROWS = T // G
PIECE = 128 // G
A, B = pl.ds(0, ROWS // 2), pl.ds(ROWS // 2, ROWS // 2)


def tail_kernel(
    att_any, wo_any, res_any, gain_any, u0, um, upl, d0, dm, dpl, out,
    att, res, gain, a_in, wo, own, midb, wu, wd, normed, hidden, part, sibbuf, stage, hop_a, hop_b, from_l, from_r,
    w_sem, a_s, a_r, o_s, o_r, g_s, g_r, t_s, t_r,
):
    z, y, x, c = place()
    sp, tp = z * 4 + y, x * 2 + c
    sib = dev(z, y, x, 1 - c)
    xp, xm, x2 = up(x, 1), up(x, 3), up(x, 2)
    right, left = dev(z, y, xp, c), dev(z, y, xm, c)
    z_next, z_prev, y_next, y_prev = up(z, 1), up(z, 3), up(y, 1), up(y, 3)
    head = 4 * x + z

    barrier = pltpu.get_barrier_semaphore()
    cs = lax.rem(lax.div(tp, 4) + z, 2)
    for zs in range(4):
        for xs in range(4):
            @pl.when(jnp.logical_not((z == zs) & (x == xs) & (c == cs)))
            def _():
                signal(barrier, dev(zs, y, xs, cs))

    to_z = dev(z_next, y, x, c), dev(z_prev, y, x, c)
    to_y = dev(z, y_next, x, c), dev(z, y_prev, x, c)
    for device in (sib, right, left, *to_z, *to_y):
        signal(barrier, device)
    def wu_rows(zz, lo, n):
        return wu.at[pl.ds(pl.multiple_of(zz * 512 + lo, 256), n)]

    loads = [
        pltpu.make_async_copy(att_any, att, w_sem.at[7]),
        pltpu.make_async_copy(wo_any, wo, w_sem.at[0]),
        pltpu.make_async_copy(res_any, res, w_sem.at[8]),
        pltpu.make_async_copy(gain_any, gain, w_sem.at[9]),
        pltpu.make_async_copy(u0, wu_rows(z, 0, 512), w_sem.at[1]),
        pltpu.make_async_copy(um, wu_rows(z_prev, 0, 512), w_sem.at[2]),
        pltpu.make_async_copy(upl, wu_rows(z_next, 0, 512), w_sem.at[3]),
        pltpu.make_async_copy(d0, wd.at[y], w_sem.at[4]),
        pltpu.make_async_copy(dm, wd.at[y_prev], w_sem.at[5]),
        pltpu.make_async_copy(dpl, wd.at[y_next], w_sem.at[6]),
    ]
    for load in loads:
        load.start()
    pl.semaphore_wait(barrier, jnp.where(lax.div(x, 2) == lax.rem(c + z, 2), 22, 23))
    loads[0].wait()

    done = []

    def go(copy):
        copy.start()
        done.append(copy)

    pending = []
    for i in range(4):
        hf = lax.rem(c + i, 2)
        for k in range(4):
            to = 4 * hf + k
            mine = (z == i) & (to == tp)
            src = att.at[i, :, pl.ds(k * 128, 128)]
            dst = a_in.at[pl.ds(pl.multiple_of(head * HD, HD), HD)]
            remote = send(src, dst, a_s.at[4 * i + k], a_r.at[head], (i * 4 + y, to))
            local = pltpu.make_async_copy(src, dst, a_r.at[head])

            @pl.when(mine)
            def _():
                local.start()

            @pl.when(jnp.logical_not(mine))
            def _():
                remote.start()

            pending.append((mine, remote))

    go(send(um.at[pl.ds(0, 256)], wu_rows(z_prev, 0, 256), o_s.at[0], o_r.at[0], to_z[0]))
    go(send(upl.at[pl.ds(256, 256)], wu_rows(z_next, 256, 256), o_s.at[1], o_r.at[1], to_z[1]))
    go(send(dm.at[pl.ds(0, 2)], wd.at[y_prev, pl.ds(0, 2)], o_s.at[2], o_r.at[2], to_y[0]))
    go(send(dpl.at[pl.ds(2, 2)], wd.at[y_next, pl.ds(2, 2)], o_s.at[3], o_r.at[3], to_y[1]))

    for h in range(16):
        rows = pl.ds(h * HD, HD)
        send(a_in.at[rows], a_in.at[rows], a_s.at[0], a_r.at[h], sib).wait_recv()
    loads[1].wait()
    loads[2].wait()
    a = a_in[...].astype(F32).T.astype(BF)
    for n in range(4):
        cols = slice(n * 512, (n + 1) * 512)
        mixed = jnp.dot(a, wo[:, cols], preferred_element_type=F32)
        own[:, cols] = (res[:, cols].astype(F32) + mixed).astype(BF)

    def piece(g, xs, cc, lo=0, n=PIECE):
        return midb.at[g, pl.ds(pl.multiple_of((2 * xs + cc) * PIECE + lo, PIECE // 2), n)]

    def pass_on(g, at, k, device, kr=None):
        go(send(at, at, g_s.at[k, g], g_r.at[k if kr is None else kr, g], device))

    def came(g, at, k):
        send(at, at, g_s.at[k, g], g_r.at[k, g], sib).wait_recv()

    def gather_own(g):
        src, dst = own.at[pl.ds(g * PIECE, PIECE)], piece(g, x, c)
        go(send(src, dst, g_s.at[0, g], g_r.at[0, g], right))
        go(send(src, dst, g_s.at[1, g], g_r.at[1, g], left))
        go(send(src, dst, g_s.at[4, g], g_r.at[4, g], sib))
        midb[g, pl.ds(pl.multiple_of(tp * PIECE, PIECE), PIECE), :] = own[g * PIECE:(g + 1) * PIECE, :]

    def gather_near(g):
        came(g, piece(g, xm, c), 0)
        pass_on(g, piece(g, xm, c, 0, PIECE // 2), 2, right)
        pass_on(g, piece(g, xm, c), 5, sib)
        came(g, piece(g, xp, c), 1)
        pass_on(g, piece(g, xp, c, PIECE // 2, PIECE // 2), 3, left)
        pass_on(g, piece(g, xp, c), 6, sib)

    def gather_far(g):
        for k in (0, 1):
            at = piece(g, x2, c, k * (PIECE // 2), PIECE // 2)
            came(g, at, 2 + k)
            pass_on(g, at, 7 + k, sib)

    def gather_rest(g):
        came(g, piece(g, x, 1 - c), 4)
        came(g, piece(g, xm, 1 - c), 5)
        came(g, piece(g, xp, 1 - c), 6)
        came(g, piece(g, x2, 1 - c, 0, PIECE // 2), 7)
        came(g, piece(g, x2, 1 - c, PIECE // 2, PIECE // 2), 8)

    def feed(g):
        wide = midb[g].astype(F32)
        inv = lax.rsqrt(jnp.mean(wide * wide, axis=-1, keepdims=True) + eps)
        normed[...] = (wide * inv * gain[0:1, :]).astype(BF)

        def lift(n, carry):
            cols = pl.ds(pl.multiple_of(n * 256, 256), 256)
            h = jnp.dot(normed[...], wu[:, cols], preferred_element_type=F32)
            hidden[:, cols] = jnp.square(jnp.maximum(h, 0.0)).astype(BF)
            return carry

        lax.fori_loop(0, 4, lift, 0)

        def drop(core):
            def one(k, carry):
                yy = 2 * core + k
                cols = pl.multiple_of(k * 128, 128)
                for zp in (0, 2):
                    rhs = jnp.concatenate([wd[yy, zp], wd[yy, zp + 1]], axis=1)
                    term = jnp.dot(hidden[...], rhs, preferred_element_type=F32).astype(BF)
                    part[g, core, zp, :, pl.ds(cols, 128)] = term[:, :128]
                    part[g, core, zp + 1, :, pl.ds(cols, 128)] = term[:, 128:]
                return carry

            lax.fori_loop(0, 2, one, 0)

        drop(1 - c)
        go(send(part.at[g, 1 - c], sibbuf.at[g], t_s.at[0, g], t_r.at[0, g], sib))
        drop(c)

    def both(g, rel, rows):
        xt = up(x, rel)
        return part[g, c, xt, rows, :].astype(F32) + sibbuf[g, xt, rows, :].astype(F32)

    def scatter_first(g):
        send(sibbuf.at[g], sibbuf.at[g], t_s.at[0, g], t_r.at[0, g], sib).wait_recv()
        stage[g, 2] = both(g, 2, pl.ds(0, ROWS)).astype(BF)
        go(send(stage.at[g, 2, A], hop_a.at[g], t_s.at[1, g], t_r.at[1, g], right))
        go(send(stage.at[g, 2, B], hop_b.at[g], t_s.at[2, g], t_r.at[2, g], left))
        stage[g, 1, B, :] = both(g, 1, B).astype(BF)
        go(send(stage.at[g, 1, B], from_l.at[g, B], t_s.at[3, g], t_r.at[3, g], right))
        stage[g, 3, A, :] = both(g, 3, A).astype(BF)
        go(send(stage.at[g, 3, A], from_r.at[g, A], t_s.at[4, g], t_r.at[4, g], left))

    def scatter_second(g):
        send(hop_a.at[g], hop_a.at[g], t_s.at[1, g], t_r.at[1, g], sib).wait_recv()
        stage[g, 1, A, :] = (both(g, 1, A) + hop_a[g].astype(F32)).astype(BF)
        go(send(stage.at[g, 1, A], from_l.at[g, A], t_s.at[5, g], t_r.at[5, g], right))
        send(hop_b.at[g], hop_b.at[g], t_s.at[2, g], t_r.at[2, g], sib).wait_recv()
        stage[g, 3, B, :] = (both(g, 3, B) + hop_b[g].astype(F32)).astype(BF)
        go(send(stage.at[g, 3, B], from_r.at[g, B], t_s.at[6, g], t_r.at[6, g], left))

    def scatter_third(g):
        for k, buf, rows in ((3, from_l, B), (4, from_r, A), (5, from_l, A), (6, from_r, B)):
            send(buf.at[g, rows], buf.at[g, rows], t_s.at[k, g], t_r.at[k, g], sib).wait_recv()
        for n in range(8):
            rows = pl.ds(n * PIECE, PIECE)
            total = both(g, 0, rows) + from_l[g, rows, :].astype(F32) + from_r[g, rows, :].astype(F32)
            mid = midb[g, rows, pl.ds(pl.multiple_of(tp * 256, 256), 256)].astype(F32)
            out[n * 128 + g * PIECE:n * 128 + (g + 1) * PIECE, :] = (mid + total).astype(BF)

    gather_own(0)
    gather_own(1)
    gather_near(0)
    gather_own(2)
    gather_near(1)
    gather_own(3)
    gather_far(0)
    gather_rest(0)
    for load in loads[3:]:
        load.wait()
    for k, at in ((0, wu_rows(up(z, 2), 0, 256)), (1, wu_rows(up(z, 2), 256, 256)),
                  (2, wd.at[up(y, 2), pl.ds(0, 2)]), (3, wd.at[up(y, 2), pl.ds(2, 2)])):
        send(at, at, o_s.at[k], o_r.at[k], sib).wait_recv()
    feed(0)
    gather_near(2)
    gather_far(1)
    gather_rest(1)
    gather_near(3)
    scatter_first(0)
    feed(1)
    gather_far(2)
    gather_rest(2)
    gather_far(3)
    scatter_first(1)
    scatter_second(0)
    feed(2)
    gather_rest(3)
    scatter_first(2)
    scatter_second(1)
    feed(3)
    scatter_second(2)
    scatter_first(3)
    scatter_third(0)
    scatter_third(1)
    scatter_second(3)
    scatter_third(2)
    scatter_third(3)
    for mine, remote in pending:
        @pl.when(jnp.logical_not(mine))
        def _():
            remote.wait_send()
    for copy in done:
        copy.wait_send()


def tail(att, wo, res, gain, ups, downs):
    return pl.pallas_call(
        tail_kernel,
        out_shape=sds((T, 256), BF),
        in_specs=[HB] * 10,
        out_specs=VM,
        scratch_shapes=[
            pltpu.VMEM((4, HD, HALF), BF),
            pltpu.VMEM((128, D), BF),
            pltpu.VMEM((8, D), F32),
            pltpu.VMEM((1024, 128), BF),
            pltpu.VMEM((1024, D), BF),
            pltpu.VMEM((128, D), BF),
            pltpu.VMEM((G, ROWS, D), BF),
            pltpu.VMEM((D, 1024), BF),
            pltpu.VMEM((4, 4, 1024, 128), BF),
            pltpu.VMEM((ROWS, D), BF),
            pltpu.VMEM((ROWS, 1024), BF),
            pltpu.VMEM((G, 2, 4, ROWS, 256), BF),
            pltpu.VMEM((G, 4, ROWS, 256), BF),
            pltpu.VMEM((G, 4, ROWS, 256), BF),
            pltpu.VMEM((G, ROWS // 2, 256), BF),
            pltpu.VMEM((G, ROWS // 2, 256), BF),
            pltpu.VMEM((G, ROWS, 256), BF),
            pltpu.VMEM((G, ROWS, 256), BF),
            DMA((10,)), DMA((16,)), DMA((16,)), DMA((4,)), DMA((4,)),
            DMA((9, G)), DMA((9, G)), DMA((7, G)), DMA((7, G)),
        ],
        compiler_params=pltpu.CompilerParams(
            has_side_effects=True, collective_id=1, vmem_limit_bytes=56 * 1024 * 1024
        ),
        cost_estimate=pl.CostEstimate(flops=20_000_000_000, bytes_accessed=8_000_000, transcendentals=0),
        name="tail",
    )(att, wo, res, gain, *ups, *downs)


def shifted(value, axis, step):
    def index(z, y):
        return (z % 4) * 4 + y % 4

    pairs = [
        (index(z, y), index(z + step, y) if axis == "z" else index(z, y + step)) for z in range(4) for y in range(4)
    ]
    return lax.ppermute(value, "sp", pairs)


def body(queries, keys, values, cum_gates, doc_ids, residual, w_out, norm_gain, w_up, w_down):
    qin, kvall, woall, resin, gain, u0, d0 = exchange(
        queries, keys, values, jnp.transpose(cum_gates), doc_ids.reshape(1, T), norm_gain, w_out, residual, w_up, w_down
    )
    um, upl = shifted(u0, "z", 1), shifted(u0, "z", -1)
    dm, dpl = shifted(d0, "y", 1), shifted(d0, "y", -1)
    att = attend(qin, kvall)
    ups = [u.reshape(512, 1024) for u in (u0, um, upl)]
    return tail(att, woall, resin, gain, ups, (d0, dm, dpl))


def solution(mesh):
    in_specs = (
        P("sp", "tp"),
        P("sp", "tp"),
        P("sp", "tp"),
        P("sp", "tp"),
        P("sp"),
        P("sp", "tp"),
        P("tp", None),
        P("tp"),
        P("sp", "tp"),
        P("tp", "sp"),
    )
    return jax.shard_map(body, mesh=mesh, in_specs=in_specs, out_specs=P("sp", "tp"), check_vma=False)
```

```python
import functools

import jax
import jax.numpy as jnp
from jax import lax
from jax.experimental import pallas as pl
from jax.experimental.pallas import tpu as pltpu
from jax.sharding import PartitionSpec as P

D = 2048
HD = 64
T = 1024
HALF = 512
ITEM = 528
eps = 1e-06
far_below = -1e30
BIG = 8192.0
MESH = pl.DeviceIdType.MESH
BF = jnp.bfloat16
F32 = jnp.float32
VM = pl.BlockSpec(memory_space=pltpu.VMEM)
HB = pl.BlockSpec(memory_space=pl.ANY)
DMA = pltpu.SemaphoreType.DMA


def sds(shape, dtype):
    return jax.ShapeDtypeStruct(shape, dtype)


def place():
    sp, tp = lax.axis_index("sp"), lax.axis_index("tp")
    return lax.div(sp, 4), lax.rem(sp, 4), lax.div(tp, 2), lax.rem(tp, 2)


def dev(z, y, x, c):
    return (z * 4 + y, x * 2 + c)


def send(src, dst, ssem, rsem, device):
    return pltpu.make_async_remote_copy(
        src_ref=src, dst_ref=dst, send_sem=ssem, recv_sem=rsem, device_id=device, device_id_type=MESH
    )


def up(v, k):
    return lax.rem(v + k, 4)


def signal(barrier, device):
    pl.semaphore_signal(barrier, inc=1, device_id=device, device_id_type=MESH)


class Ring:
    def __init__(self, go, me, slot, right, left, s_r, s_l, r, sib=None, s_sib=None, r_sib=None):
        self.go, self.me, self.slot, self.right, self.left = go, me, slot, right, left
        self.s_r, self.s_l, self.r = s_r, s_l, r
        self.sib, self.s_sib, self.r_sib = sib, s_sib, r_sib

    def start(self, src, order=(0, 1)):
        for half in order:
            n, dst = 2 * self.me + half, self.slot(self.me, half)
            self.go(send(src(half), dst, self.s_r.at[n], self.r.at[n], self.right))
            self.go(send(src(half), dst, self.s_l.at[n], self.r.at[n], self.left))
            if self.s_sib is not None:
                self.go(send(src(half), dst, self.s_sib.at[n], self.r_sib.at[n], self.sib))

    def take(self, i, half, forward=0):
        n, at = 2 * i + half, self.slot(i, half)
        send(at, at, self.s_r.at[n], self.r.at[n], self.right).wait_recv()
        if forward > 0:
            self.go(send(at, at, self.s_r.at[n], self.r.at[n], self.right))
        if forward < 0:
            self.go(send(at, at, self.s_l.at[n], self.r.at[n], self.left))
        if self.s_sib is not None:
            self.go(send(at, at, self.s_sib.at[n], self.r_sib.at[n], self.sib))

    def middle(self, half):
        lo, hi = up(self.me, 3), up(self.me, 1)
        if half == 0:
            self.take(lo, 0, 1)
            self.take(hi, 0)
        else:
            self.take(hi, 1, -1)
            self.take(lo, 1)

    def last(self):
        self.take(up(self.me, 2), 0)
        self.take(up(self.me, 2), 1)


def pack_kernel(q_ref, k_ref, v_ref, g_ref, d_ref, n_ref, qt_ref, kv_ref, gain_ref):
    gain_ref[...] = jnp.broadcast_to(n_ref[...].astype(F32)[None], (8, 256))
    qt = (q_ref[...].astype(F32) * (HD ** -0.5)).T.astype(BF)
    qt_ref[0] = qt[:HD]
    qt_ref[1] = qt[HD:]
    k_lo, k_hi = k_ref[:HALF].astype(F32), k_ref[HALF:].astype(F32)
    first = lax.broadcasted_iota(jnp.int32, (HALF, 128), 1) < HD
    kv_ref[0, 0, :HALF] = jnp.where(first, k_lo, pltpu.roll(k_hi, HD, 1)).astype(BF)
    kv_ref[0, 1, :HALF] = jnp.where(first, pltpu.roll(k_lo, HD, 1), k_hi).astype(BF)
    vt = v_ref[...].astype(F32).T.astype(BF)
    row = lax.broadcasted_iota(jnp.int32, (8, T), 0)
    kind = lax.rem(row, 4)
    doc0 = 1.0 - d_ref[...].astype(F32)
    for j in range(2):
        g = g_ref[j:j + 1, :]
        hi = g.astype(BF).astype(F32)
        mid = (g - hi).astype(BF).astype(F32)
        lo = (g - hi) - mid
        aux = jnp.where(kind == 0, hi, jnp.where(kind == 1, mid, jnp.where(kind == 2, lo, doc0)))
        aux = jnp.where(row < 4, aux, pltpu.roll(aux, T - 128, 1))
        for n in range(8):
            kv_ref[1, j, n * 64:(n + 1) * 64] = vt[j * HD:(j + 1) * HD, n * 128:(n + 1) * 128]
        for t in range(2):
            at = t * 512
            two = jnp.concatenate([aux[:, at:at + 128], aux[:, at + 256:at + 384]], axis=0)
            kv_ref[t, j, HALF:] = two.astype(BF)


def exchange_kernel(
    q_h, k_h, v_h, g_h, d_h, n_h, wo_h, res_h, wu_h, wd_h, qin, kv_out, woall, resin, gainall, wu4, wd4,
    q_v, k_v, v_v, g_v, d_v, n_v, wo, res, wu, wd, qt, kv, gain, kvall, in_sem, out_sem,
    qs, qr, ks, rr, s_sib, r_sib, s_r, s_l,
    wl, w_sib, wr_sib, w_s_r, w_s_l, w_r, es, er, gs, gr,
    u_s_r, u_s_l, u_r, d_s_r, d_s_l, d_r, ul,
):
    z, y, x, c = place()
    sp, tp = z * 4 + y, x * 2 + c
    sib = dev(z, y, x, 1 - c)
    yp, ym, y2 = up(y, 1), up(y, 3), up(y, 2)
    xp, xm, x2 = up(x, 1), up(x, 3), up(x, 2)

    loads = [
        pltpu.make_async_copy(src, dst, in_sem.at[n])
        for n, (src, dst) in enumerate(
            zip((k_h, v_h, g_h, d_h, n_h, q_h, wo_h, res_h, wu_h, wd_h), (k_v, v_v, g_v, d_v, n_v, q_v, wo, res, wu, wd))
        )
    ]
    for load in loads:
        load.start()
    barrier = pltpu.get_barrier_semaphore()
    cs = lax.div(z, 2)
    for zs in range(4):
        @pl.when(jnp.logical_not((z == zs) & (c == cs)))
        def _():
            signal(barrier, dev(zs, y, x, cs))

    for k in range(1, 8):
        signal(barrier, (sp, lax.rem(tp + k, 8)))
    signal(barrier, dev(z, yp, x, c))
    signal(barrier, dev(z, ym, x, c))
    zp, zm = up(z, 1), up(z, 3)
    signal(barrier, dev(zp, y, x, c))
    signal(barrier, dev(zm, y, x, c))
    for load in loads:
        load.wait()
    pack_kernel(q_v, k_v, v_v, g_v, d_v, n_v, qt, kv, gain)
    pl.semaphore_wait(barrier, jnp.where(c == cs, 14, 15))

    def guarded(is_self, local, remote):
        @pl.when(is_self)
        def _():
            local.start()

        @pl.when(jnp.logical_not(is_self))
        def _():
            remote.start()

    pending = []
    for j in range(2):
        zt = 2 * c + j
        for t in range(2):
            mine = (zt == z) & (c == t)
            src, dst = kv.at[t, j], kvall.at[t, sp]
            remote = send(src, dst, ks.at[2 * t + j], rr.at[sp], dev(zt, y, x, t))
            guarded(mine, pltpu.make_async_copy(src, dst, rr.at[sp]), remote)
            pending.append((mine, remote))
    for j in range(2):
        zt = 2 * c + j
        for hf in range(2):
            ct = lax.rem(hf + z, 2)
            mine = (zt == z) & (ct == c)
            src, dst = qt.at[j, :, pl.ds(hf * HALF, HALF)], qin.at[z]
            remote = send(src, dst, qs.at[2 * j + hf], qr.at[z], dev(zt, y, x, ct))
            guarded(mine, pltpu.make_async_copy(src, dst, qr.at[z]), remote)
            pending.append((mine, remote))

    done = []

    def wrows(xs, half):
        return pl.ds((2 * xs + c) * 128 + half * 64, 64)

    def go(copy):
        copy.start()
        done.append(copy)

    ring_w = Ring(go, x, lambda i, half: woall.at[wrows(i, half)], dev(z, y, xp, c), dev(z, y, xm, c),
                  w_s_r, w_s_l, w_r, sib, w_sib, wr_sib)
    ring_u = Ring(go, y, lambda i, half: wu4.at[i, pl.ds(half * 64, 64)], dev(z, yp, x, c), dev(z, ym, x, c),
                  u_s_r, u_s_l, u_r)
    ring_d = Ring(go, z, lambda i, half: wd4.at[i, pl.ds(half * HALF, HALF)], dev(zp, y, x, c), dev(zm, y, x, c),
                  d_s_r, d_s_l, d_r)
    own_w = [
        pltpu.make_async_copy(wo, woall.at[pl.ds(pl.multiple_of(tp * 128, 128), 128)], wl.at[0]),
        pltpu.make_async_copy(wu, wu4.at[y], ul.at[0]),
        pltpu.make_async_copy(wd, wd4.at[z], ul.at[1]),
    ]
    for loc in own_w:
        loc.start()
    ring_w.start(lambda half: wo.at[pl.ds(half * 64, 64)])

    own_e = pltpu.make_async_copy(res.at[pl.ds(pl.multiple_of(tp * 128, 128), 128)],
                                  resin.at[:, pl.ds(pl.multiple_of(tp * 256, 256), 256)], er.at[tp])
    own_e.start()
    own_g = pltpu.make_async_copy(gain, gainall.at[:, pl.ds(pl.multiple_of(tp * 256, 256), 256)], gr.at[tp])
    own_g.start()
    for k in range(1, 8):
        to = lax.rem(tp + k, 8)
        cols = pl.ds(pl.multiple_of(tp * 256, 256), 256)
        go(send(res.at[pl.ds(pl.multiple_of(to * 128, 128), 128)], resin.at[:, cols], es.at[k], er.at[tp], (sp, to)))
        go(send(gain, gainall.at[:, cols], gs.at[k], gr.at[tp], (sp, to)))

    def drain(t, b):
        return pltpu.make_async_copy(kvall.at[t, b], kv_out.at[t, b], out_sem.at[t, b])

    def arrived(b):
        send(kvall.at[c, b], kvall.at[c, b], s_sib.at[b], rr.at[b], sib).wait_recv()
        drain(c, b).start()
        go(send(kvall.at[c, b], kvall.at[c, b], s_sib.at[b], r_sib.at[b], sib))

    def right(b):
        go(send(kvall.at[c, b], kvall.at[c, b], s_r.at[b], rr.at[b], dev(z, yp, x, c)))

    def left(b):
        go(send(kvall.at[c, b], kvall.at[c, b], s_l.at[b], rr.at[b], dev(z, ym, x, c)))

    zs = [z, up(z, 1), up(z, 3), up(z, 2)]

    def near(r):
        b = zs[r] * 4 + y
        arrived(b)
        right(b)
        left(b)

    def next_to(r):
        b = zs[r] * 4 + ym
        arrived(b)
        if r in (0, 2):
            right(b)
        b = zs[r] * 4 + yp
        arrived(b)
        if r in (1, 3):
            left(b)

    near(0)
    ring_d.start(lambda half: wd.at[pl.ds(half * HALF, HALF)])
    ring_u.start(lambda half: wu.at[pl.ds(half * 64, 64)])
    near(1)
    near(2)
    next_to(0)
    ring_w.middle(0)
    near(3)
    ring_u.middle(0)
    ring_d.middle(0)
    next_to(1)
    next_to(2)
    ring_w.middle(1)
    ring_u.middle(1)
    ring_d.middle(1)
    next_to(3)
    for r in range(4):
        arrived(zs[r] * 4 + y2)
    ring_w.last()
    ring_u.last()
    ring_d.last()

    for b in range(16):
        send(kvall.at[1 - c, b], kvall.at[1 - c, b], s_sib.at[b], r_sib.at[b], sib).wait_recv()
        drain(1 - c, b).start()
    for n in range(8):
        rows = pl.ds((2 * (n // 2) + (1 - c)) * 128 + (n % 2) * 64, 64)
        send(woall.at[rows], woall.at[rows], w_sib.at[n], wr_sib.at[n], sib).wait_recv()
    for i in range(4):
        send(qin.at[i], qin.at[i], qs.at[0], qr.at[i], sib).wait_recv()
    for n in range(8):
        cols = pl.ds(n * 256, 256)
        send(resin.at[:, cols], resin.at[:, cols], es.at[0], er.at[n], sib).wait_recv()
        send(gainall.at[:, cols], gainall.at[:, cols], gs.at[0], gr.at[n], sib).wait_recv()
    for loc in own_w:
        loc.wait()
    for b in range(16):
        drain(c, b).wait()
        drain(1 - c, b).wait()
    for mine, remote in pending:
        @pl.when(jnp.logical_not(mine))
        def _():
            remote.wait_send()
    for copy in done:
        copy.wait_send()


def exchange(*args):
    return pl.pallas_call(
        exchange_kernel,
        out_shape=(
            sds((4, HD, HALF), BF),
            sds((2, 16, ITEM, 128), BF),
            sds((1024, D), BF),
            sds((128, D), BF),
            sds((8, D), F32),
            sds((4, 128, 1024), BF),
            sds((4, T, 128), BF),
        ),
        in_specs=[HB] * 10,
        out_specs=(HB,) * 7,
        scratch_shapes=[
            pltpu.VMEM((T, 128), BF),
            pltpu.VMEM((T, 128), BF),
            pltpu.VMEM((T, 128), BF),
            pltpu.VMEM((2, T), F32),
            pltpu.VMEM((1, T), jnp.int32),
            pltpu.VMEM((256,), BF),
            pltpu.VMEM((128, D), BF),
            pltpu.VMEM((T, 256), BF),
            pltpu.VMEM((128, 1024), BF),
            pltpu.VMEM((1024, 128), BF),
            pltpu.VMEM((2, HD, T), BF),
            pltpu.VMEM((2, 2, ITEM, 128), BF),
            pltpu.VMEM((8, 256), F32),
            pltpu.VMEM((2, 16, ITEM, 128), BF),
            DMA((10,)),
            DMA((2, 16)),
            DMA((4,)), DMA((4,)), DMA((4,)), DMA((16,)), DMA((16,)), DMA((16,)), DMA((16,)), DMA((16,)),
            DMA((2,)), DMA((8,)), DMA((8,)), DMA((8,)), DMA((8,)), DMA((8,)),
            DMA((8,)), DMA((8,)), DMA((8,)), DMA((8,)),
            DMA((8,)), DMA((8,)), DMA((8,)), DMA((8,)), DMA((8,)), DMA((8,)), DMA((2,)),
        ],
        compiler_params=pltpu.CompilerParams(has_side_effects=True, collective_id=0),
        cost_estimate=pl.CostEstimate(flops=20_000_000_000, bytes_accessed=16_000_000, transcendentals=0),
        name="exchange",
    )(*args)


QW = 256
NS = HALF // QW
PARTS = (slice(0, 256), slice(256, 512))


def in_turn(*streams):
    streams = list(streams)
    while streams:
        for stream in list(streams):
            if next(stream, streams) is streams:
                streams.remove(stream)


def attend_kernel(q_h, kv_h, o_ref, q_ref, kv_ref, aux_ref, in_sem, kv_sem, pieces, gmat, w_ref, *scr):
    z, y, x, c = place()
    main = pl.ds(0, HALF)
    loads = [
        pltpu.make_async_copy(kv_h.at[0, :, pl.ds(HALF, 16)], aux_ref.at[0], in_sem.at[0]),
        pltpu.make_async_copy(kv_h.at[1, :, pl.ds(HALF, 16)], aux_ref.at[1], in_sem.at[2]),
        pltpu.make_async_copy(q_h, q_ref, in_sem.at[1]),
    ]

    def blocks(t, i):
        four = pl.ds(4 * i, 4)
        return pltpu.make_async_copy(kv_h.at[t, four, main], kv_ref.at[t, four], kv_sem.at[t, i])

    for load in loads:
        load.start()
    for i in range(4):
        for t in range(2):
            blocks(t, i).start()
    loads[0].wait()
    loads[1].wait()
    s_refs, accs, tops, shrinks = scr[:NS], scr[NS:2 * NS], scr[2 * NS:3 * NS], scr[3 * NS:]
    ones = jnp.ones((16, HALF), BF)
    count = jnp.zeros((1, 128), F32)
    for b in range(16):
        for t in range(2):
            a = aux_ref[t, b].astype(F32)
            for k in range(4):
                hf, at = t, k * 128
                count = count + a[k * 4 + 3:k * 4 + 4]
                pieces[b * 8 + hf * 4:b * 8 + hf * 4 + 4, at:at + 128] = a[k * 4:k * 4 + 4]
    docs0 = jnp.sum(count).astype(jnp.int32)
    gmat[...] = pieces[...].T.astype(BF)
    loads[2].wait()
    row = lax.broadcasted_iota(jnp.int32, (128, QW), 0)
    unit_of_row, piece_of_row = row // 4, row % 4

    def tile(i, carry):
        for t in range(2):
            blocks(t, i).wait()
        hq = 2 * (4 * i + y) + lax.rem(c + i, 2)
        start = jnp.where(hq * HALF >= docs0, lax.div(docs0, HALF), 0)
        q_pos = hq * HALF + lax.broadcasted_iota(jnp.int32, (1, HALF), 1)
        doc1 = jnp.where(q_pos >= docs0, -BIG, 0.0)
        for k in range(NS):
            cols = slice(k * QW, (k + 1) * QW)
            w_ref[:, cols] = jnp.where(piece_of_row == 3, doc1[:, cols], -1.0)

        def scores(k, u, first):
            cols = slice(k * QW, (k + 1) * QW)
            q = q_ref[i, :, cols]
            none = jnp.zeros_like(q)
            b, low = lax.div(u, 2), lax.rem(u, 2) == 0
            sel = jnp.where(unit_of_row == u, w_ref[:, cols], 0.0).astype(BF)
            rhs = jnp.concatenate([jnp.where(low, q, none), jnp.where(low, none, q), sel], axis=0)
            largest = []
            for rows in PARTS:
                lhs = jnp.concatenate([kv_ref[0, b, rows, :], gmat[rows, :]], axis=1)
                s = jnp.dot(lhs, rhs, preferred_element_type=F32)
                if first:
                    key = rows.start + lax.broadcasted_iota(jnp.int32, s.shape, 0)
                    s = jnp.where(key <= k * QW + lax.broadcasted_iota(jnp.int32, s.shape, 1), s, far_below)
                s_refs[k][rows, :] = s
                largest.append(jnp.max(s, axis=0, keepdims=True))
                yield
            new = functools.reduce(jnp.maximum, largest)
            if not first:
                old = tops[k][...]
                new = jnp.maximum(old, new)
                shrinks[k][...] = jnp.exp(old - new)
            tops[k][...] = new

        def weigh(k, u, first):
            b, hf = lax.div(u, 2), lax.rem(u, 2)
            vt = jnp.concatenate(
                [kv_ref[1, b, pl.ds(pl.multiple_of(hf * 256 + n * 64, 64), 64), :] for n in range(4)], axis=1
            )
            vt = jnp.concatenate([vt, ones], axis=0)
            most = tops[k][...]
            product = None
            for rows in PARTS:
                p = jnp.exp(s_refs[k][rows, :] - most).astype(BF)
                term = jnp.dot(vt[:, rows], p, preferred_element_type=F32)
                product = term if product is None else product + term
                yield
            accs[k][...] = product if first else accs[k][...] * shrinks[k][...] + product

        ahead = jnp.maximum(hq - 1, 0)
        in_turn(scores(0, hq, True))
        in_turn(scores(1, hq, True), weigh(0, hq, True))
        in_turn(scores(0, jnp.minimum(start, ahead), False), weigh(1, hq, True))

        def step(u, carry):
            in_turn(scores(1, u, False), weigh(0, u, False))
            in_turn(scores(0, jnp.minimum(u + 1, ahead), False), weigh(1, u, False))
            return carry

        lax.fori_loop(start, hq - 1, step, 0)

        @pl.when(start < hq)
        def _():
            in_turn(scores(1, hq - 1, False), weigh(0, hq - 1, False))
            in_turn(weigh(1, hq - 1, False))

        for k in range(NS):
            total = accs[k][...]
            o_ref[i, :, k * QW:(k + 1) * QW] = (total[:HD] / total[HD:HD + 1]).astype(BF)
        return carry

    lax.fori_loop(0, 4, tile, 0)


def attend(q, kv):
    return pl.pallas_call(
        attend_kernel,
        out_shape=sds((4, HD, HALF), BF),
        in_specs=[HB, HB],
        out_specs=VM,
        scratch_shapes=[
            pltpu.VMEM((4, HD, HALF), BF),
            pltpu.VMEM((2, 16, HALF, 128), BF),
            pltpu.VMEM((2, 16, 16, 128), BF),
            DMA((3,)),
            DMA((2, 4)),
            pltpu.VMEM((128, HALF), F32),
            pltpu.VMEM((HALF, 128), BF),
            pltpu.VMEM((128, HALF), F32),
        ]
        + [pltpu.VMEM((HALF, QW), F32)] * NS
        + [pltpu.VMEM((80, QW), F32)] * NS
        + [pltpu.VMEM((1, QW), F32)] * (2 * NS),
        compiler_params=pltpu.CompilerParams(vmem_limit_bytes=66_500_000),
        cost_estimate=pl.CostEstimate(flops=20_000_000_000, bytes_accessed=8_000_000, transcendentals=0),
        name="attend",
    )(q, kv)


G = 4
ROWS = T // G
PIECE = 128 // G
A, B = pl.ds(0, ROWS // 2), pl.ds(ROWS // 2, ROWS // 2)


def tail_kernel(
    att_any, wo_any, res_any, gain_any, u0, um, upl, d0, dm, dpl, out,
    att, res, gain, a_in, wo, own, midb, wu, wd, normed, hidden, part, sibbuf, stage, hop_a, hop_b, from_l, from_r,
    w_sem, a_s, a_r, o_s, o_r, g_s, g_r, t_s, t_r,
):
    z, y, x, c = place()
    sp, tp = z * 4 + y, x * 2 + c
    sib = dev(z, y, x, 1 - c)
    xp, xm, x2 = up(x, 1), up(x, 3), up(x, 2)
    right, left = dev(z, y, xp, c), dev(z, y, xm, c)
    z_next, z_prev, y_next, y_prev = up(z, 1), up(z, 3), up(y, 1), up(y, 3)
    head = 4 * x + z

    barrier = pltpu.get_barrier_semaphore()
    cs = lax.rem(lax.div(tp, 4) + z, 2)
    for zs in range(4):
        for xs in range(4):
            @pl.when(jnp.logical_not((z == zs) & (x == xs) & (c == cs)))
            def _():
                signal(barrier, dev(zs, y, xs, cs))

    to_z = dev(z_next, y, x, c), dev(z_prev, y, x, c)
    to_y = dev(z, y_next, x, c), dev(z, y_prev, x, c)
    for device in (sib, right, left, *to_z, *to_y):
        signal(barrier, device)
    def wu_rows(zz, lo, n):
        return wu.at[pl.ds(pl.multiple_of(zz * 512 + lo, 256), n)]

    loads = [
        pltpu.make_async_copy(att_any, att, w_sem.at[7]),
        pltpu.make_async_copy(wo_any, wo, w_sem.at[0]),
        pltpu.make_async_copy(res_any, res, w_sem.at[8]),
        pltpu.make_async_copy(gain_any, gain, w_sem.at[9]),
        pltpu.make_async_copy(u0, wu_rows(z, 0, 512), w_sem.at[1]),
        pltpu.make_async_copy(um, wu_rows(z_prev, 0, 512), w_sem.at[2]),
        pltpu.make_async_copy(upl, wu_rows(z_next, 0, 512), w_sem.at[3]),
        pltpu.make_async_copy(d0, wd.at[y], w_sem.at[4]),
        pltpu.make_async_copy(dm, wd.at[y_prev], w_sem.at[5]),
        pltpu.make_async_copy(dpl, wd.at[y_next], w_sem.at[6]),
    ]
    for load in loads:
        load.start()
    pl.semaphore_wait(barrier, jnp.where(lax.div(x, 2) == lax.rem(c + z, 2), 22, 23))
    loads[0].wait()

    done = []

    def go(copy):
        copy.start()
        done.append(copy)

    pending = []
    for i in range(4):
        hf = lax.rem(c + i, 2)
        for k in range(4):
            to = 4 * hf + k
            mine = (z == i) & (to == tp)
            src = att.at[i, :, pl.ds(k * 128, 128)]
            dst = a_in.at[pl.ds(pl.multiple_of(head * HD, HD), HD)]
            remote = send(src, dst, a_s.at[4 * i + k], a_r.at[head], (i * 4 + y, to))
            local = pltpu.make_async_copy(src, dst, a_r.at[head])

            @pl.when(mine)
            def _():
                local.start()

            @pl.when(jnp.logical_not(mine))
            def _():
                remote.start()

            pending.append((mine, remote))

    go(send(um.at[pl.ds(0, 256)], wu_rows(z_prev, 0, 256), o_s.at[0], o_r.at[0], to_z[0]))
    go(send(upl.at[pl.ds(256, 256)], wu_rows(z_next, 256, 256), o_s.at[1], o_r.at[1], to_z[1]))
    go(send(dm.at[pl.ds(0, 2)], wd.at[y_prev, pl.ds(0, 2)], o_s.at[2], o_r.at[2], to_y[0]))
    go(send(dpl.at[pl.ds(2, 2)], wd.at[y_next, pl.ds(2, 2)], o_s.at[3], o_r.at[3], to_y[1]))

    for h in range(16):
        rows = pl.ds(h * HD, HD)
        send(a_in.at[rows], a_in.at[rows], a_s.at[0], a_r.at[h], sib).wait_recv()
    loads[1].wait()
    loads[2].wait()
    a = a_in[...].astype(F32).T.astype(BF)
    for n in range(4):
        cols = slice(n * 512, (n + 1) * 512)
        mixed = jnp.dot(a, wo[:, cols], preferred_element_type=F32)
        own[:, cols] = (res[:, cols].astype(F32) + mixed).astype(BF)

    def piece(g, xs, cc, lo=0, n=PIECE):
        return midb.at[g, pl.ds(pl.multiple_of((2 * xs + cc) * PIECE + lo, PIECE // 2), n)]

    def pass_on(g, at, k, device, kr=None):
        go(send(at, at, g_s.at[k, g], g_r.at[k if kr is None else kr, g], device))

    def came(g, at, k):
        send(at, at, g_s.at[k, g], g_r.at[k, g], sib).wait_recv()

    def gather_own(g):
        src, dst = own.at[pl.ds(g * PIECE, PIECE)], piece(g, x, c)
        go(send(src, dst, g_s.at[0, g], g_r.at[0, g], right))
        go(send(src, dst, g_s.at[1, g], g_r.at[1, g], left))
        go(send(src, dst, g_s.at[4, g], g_r.at[4, g], sib))
        midb[g, pl.ds(pl.multiple_of(tp * PIECE, PIECE), PIECE), :] = own[g * PIECE:(g + 1) * PIECE, :]

    def gather_near(g):
        came(g, piece(g, xm, c), 0)
        pass_on(g, piece(g, xm, c, 0, PIECE // 2), 2, right)
        pass_on(g, piece(g, xm, c), 5, sib)
        came(g, piece(g, xp, c), 1)
        pass_on(g, piece(g, xp, c, PIECE // 2, PIECE // 2), 3, left)
        pass_on(g, piece(g, xp, c), 6, sib)

    def gather_far(g):
        for k in (0, 1):
            at = piece(g, x2, c, k * (PIECE // 2), PIECE // 2)
            came(g, at, 2 + k)
            pass_on(g, at, 7 + k, sib)

    def gather_rest(g):
        came(g, piece(g, x, 1 - c), 4)
        came(g, piece(g, xm, 1 - c), 5)
        came(g, piece(g, xp, 1 - c), 6)
        came(g, piece(g, x2, 1 - c, 0, PIECE // 2), 7)
        came(g, piece(g, x2, 1 - c, PIECE // 2, PIECE // 2), 8)

    def feed(g):
        wide = midb[g].astype(F32)
        inv = lax.rsqrt(jnp.mean(wide * wide, axis=-1, keepdims=True) + eps)
        normed[...] = (wide * inv * gain[0:1, :]).astype(BF)

        def lift(n, carry):
            cols = pl.ds(pl.multiple_of(n * 256, 256), 256)
            h = jnp.dot(normed[...], wu[:, cols], preferred_element_type=F32)
            hidden[:, cols] = jnp.square(jnp.maximum(h, 0.0)).astype(BF)
            return carry

        lax.fori_loop(0, 4, lift, 0)

        def drop(core):
            def one(k, carry):
                yy = 2 * core + k
                cols = pl.multiple_of(k * 128, 128)
                for zp in (0, 2):
                    rhs = jnp.concatenate([wd[yy, zp], wd[yy, zp + 1]], axis=1)
                    term = jnp.dot(hidden[...], rhs, preferred_element_type=F32).astype(BF)
                    part[g, core, zp, :, pl.ds(cols, 128)] = term[:, :128]
                    part[g, core, zp + 1, :, pl.ds(cols, 128)] = term[:, 128:]
                return carry

            lax.fori_loop(0, 2, one, 0)

        drop(1 - c)
        go(send(part.at[g, 1 - c], sibbuf.at[g], t_s.at[0, g], t_r.at[0, g], sib))
        drop(c)

    def both(g, rel, rows):
        xt = up(x, rel)
        return part[g, c, xt, rows, :].astype(F32) + sibbuf[g, xt, rows, :].astype(F32)

    def scatter_first(g):
        send(sibbuf.at[g], sibbuf.at[g], t_s.at[0, g], t_r.at[0, g], sib).wait_recv()
        stage[g, 2] = both(g, 2, pl.ds(0, ROWS)).astype(BF)
        go(send(stage.at[g, 2, A], hop_a.at[g], t_s.at[1, g], t_r.at[1, g], right))
        go(send(stage.at[g, 2, B], hop_b.at[g], t_s.at[2, g], t_r.at[2, g], left))
        stage[g, 1, B, :] = both(g, 1, B).astype(BF)
        go(send(stage.at[g, 1, B], from_l.at[g, B], t_s.at[3, g], t_r.at[3, g], right))
        stage[g, 3, A, :] = both(g, 3, A).astype(BF)
        go(send(stage.at[g, 3, A], from_r.at[g, A], t_s.at[4, g], t_r.at[4, g], left))

    def scatter_second(g):
        send(hop_a.at[g], hop_a.at[g], t_s.at[1, g], t_r.at[1, g], sib).wait_recv()
        stage[g, 1, A, :] = (both(g, 1, A) + hop_a[g].astype(F32)).astype(BF)
        go(send(stage.at[g, 1, A], from_l.at[g, A], t_s.at[5, g], t_r.at[5, g], right))
        send(hop_b.at[g], hop_b.at[g], t_s.at[2, g], t_r.at[2, g], sib).wait_recv()
        stage[g, 3, B, :] = (both(g, 3, B) + hop_b[g].astype(F32)).astype(BF)
        go(send(stage.at[g, 3, B], from_r.at[g, B], t_s.at[6, g], t_r.at[6, g], left))

    def scatter_third(g):
        for k, buf, rows in ((3, from_l, B), (4, from_r, A), (5, from_l, A), (6, from_r, B)):
            send(buf.at[g, rows], buf.at[g, rows], t_s.at[k, g], t_r.at[k, g], sib).wait_recv()
        for n in range(8):
            rows = pl.ds(n * PIECE, PIECE)
            total = both(g, 0, rows) + from_l[g, rows, :].astype(F32) + from_r[g, rows, :].astype(F32)
            mid = midb[g, rows, pl.ds(pl.multiple_of(tp * 256, 256), 256)].astype(F32)
            out[n * 128 + g * PIECE:n * 128 + (g + 1) * PIECE, :] = (mid + total).astype(BF)

    gather_own(0)
    gather_own(1)
    gather_near(0)
    gather_own(2)
    gather_near(1)
    gather_own(3)
    gather_far(0)
    gather_rest(0)
    for load in loads[3:]:
        load.wait()
    for k, at in ((0, wu_rows(up(z, 2), 0, 256)), (1, wu_rows(up(z, 2), 256, 256)),
                  (2, wd.at[up(y, 2), pl.ds(0, 2)]), (3, wd.at[up(y, 2), pl.ds(2, 2)])):
        send(at, at, o_s.at[k], o_r.at[k], sib).wait_recv()
    feed(0)
    gather_near(2)
    gather_far(1)
    gather_rest(1)
    gather_near(3)
    scatter_first(0)
    feed(1)
    gather_far(2)
    gather_rest(2)
    gather_far(3)
    scatter_first(1)
    scatter_second(0)
    feed(2)
    gather_rest(3)
    scatter_first(2)
    scatter_second(1)
    feed(3)
    scatter_second(2)
    scatter_first(3)
    scatter_third(0)
    scatter_third(1)
    scatter_second(3)
    scatter_third(2)
    scatter_third(3)
    for mine, remote in pending:
        @pl.when(jnp.logical_not(mine))
        def _():
            remote.wait_send()
    for copy in done:
        copy.wait_send()


def tail(att, wo, res, gain, ups, downs):
    return pl.pallas_call(
        tail_kernel,
        out_shape=sds((T, 256), BF),
        in_specs=[HB] * 10,
        out_specs=VM,
        scratch_shapes=[
            pltpu.VMEM((4, HD, HALF), BF),
            pltpu.VMEM((128, D), BF),
            pltpu.VMEM((8, D), F32),
            pltpu.VMEM((1024, 128), BF),
            pltpu.VMEM((1024, D), BF),
            pltpu.VMEM((128, D), BF),
            pltpu.VMEM((G, ROWS, D), BF),
            pltpu.VMEM((D, 1024), BF),
            pltpu.VMEM((4, 4, 1024, 128), BF),
            pltpu.VMEM((ROWS, D), BF),
            pltpu.VMEM((ROWS, 1024), BF),
            pltpu.VMEM((G, 2, 4, ROWS, 256), BF),
            pltpu.VMEM((G, 4, ROWS, 256), BF),
            pltpu.VMEM((G, 4, ROWS, 256), BF),
            pltpu.VMEM((G, ROWS // 2, 256), BF),
            pltpu.VMEM((G, ROWS // 2, 256), BF),
            pltpu.VMEM((G, ROWS, 256), BF),
            pltpu.VMEM((G, ROWS, 256), BF),
            DMA((10,)), DMA((16,)), DMA((16,)), DMA((4,)), DMA((4,)),
            DMA((9, G)), DMA((9, G)), DMA((7, G)), DMA((7, G)),
        ],
        compiler_params=pltpu.CompilerParams(
            has_side_effects=True, collective_id=1, vmem_limit_bytes=56 * 1024 * 1024
        ),
        cost_estimate=pl.CostEstimate(flops=20_000_000_000, bytes_accessed=8_000_000, transcendentals=0),
        name="tail",
    )(att, wo, res, gain, *ups, *downs)


def shifted(value, axis, step):
    def index(z, y):
        return (z % 4) * 4 + y % 4

    pairs = [
        (index(z, y), index(z + step, y) if axis == "z" else index(z, y + step)) for z in range(4) for y in range(4)
    ]
    return lax.ppermute(value, "sp", pairs)


def body(queries, keys, values, cum_gates, doc_ids, residual, w_out, norm_gain, w_up, w_down):
    qin, kvall, woall, resin, gain, u0, d0 = exchange(
        queries, keys, values, jnp.transpose(cum_gates), doc_ids.reshape(1, T), norm_gain, w_out, residual, w_up, w_down
    )
    um, upl = shifted(u0, "z", 1), shifted(u0, "z", -1)
    dm, dpl = shifted(d0, "y", 1), shifted(d0, "y", -1)
    att = attend(qin, kvall)
    ups = [u.reshape(512, 1024) for u in (u0, um, upl)]
    return tail(att, woall, resin, gain, ups, (d0, dm, dpl))


def solution(mesh):
    in_specs = (
        P("sp", "tp"),
        P("sp", "tp"),
        P("sp", "tp"),
        P("sp", "tp"),
        P("sp"),
        P("sp", "tp"),
        P("tp", None),
        P("tp"),
        P("sp", "tp"),
        P("tp", "sp"),
    )
    return jax.shard_map(body, mesh=mesh, in_specs=in_specs, out_specs=P("sp", "tp"), check_vma=False)
```
